128 devices in a mesh: sp: 64 (over z, y, x), tp: 2 (over core).
Axes of the slice: x: 4, y: 4, z: 4, core: 2. Of those that a mesh axis runs over, the one named last changes fastest.
Arguments:
- stream: bfloat16 [16384, 2048], P('sp', 'tp'), may hold values from -6 to 6
- out_grad: bfloat16 [16384, 2048], P('sp', 'tp'), may hold values from -16 to 16
- gate_in: bfloat16 [16384, 1024], P('sp', 'tp'), may hold values from -6 to 6
- conv_gate: bfloat16 [16384, 1024], P('sp', 'tp'), may hold values from -6 to 6
- conv_value: bfloat16 [16384, 1024], P('sp', 'tp'), may hold values from -6 to 6
- taps: float32 [3, 1024], P(None, 'tp'), may hold values from -3.5 to 3.5
- w_out: bfloat16 [2048, 1024], P(None, 'tp'), may hold values from -0.1875 to 0.1875
- route_ids: int32 [16384, 2], P('sp'), may hold values from 0 to 63, all different within a row; in each aligned block of 256 rows (0 to 255, 256 to 511, ...) at most 16 rows name the same one
- route_weights: float32 [16384, 2], P('sp'), may hold values from 0.1 to 1
- w_gate: bfloat16 [64, 2048, 1024], P('sp', None, 'tp'), may hold values from -0.125 to 0.125
- w_up: bfloat16 [64, 2048, 1024], P('sp', None, 'tp'), may hold values from -0.125 to 0.125
- w_down: bfloat16 [64, 1024, 2048], P('sp', 'tp'), may hold values from -0.1875 to 0.1875
Outputs:
- stream_grad: bfloat16 [16384, 2048], P('sp', 'tp')
- gate_in_grad: bfloat16 [16384, 1024], P('sp', 'tp')
- conv_gate_grad: bfloat16 [16384, 1024], P('sp', 'tp')
- conv_value_grad: bfloat16 [16384, 1024], P('sp', 'tp')
- w_out_grad: float32 [2048, 1024], P('sp', 'tp')
- w_gate_grad: float32 [64, 2048, 1024], P('sp', None, 'tp')
- w_up_grad: float32 [64, 2048, 1024], P('sp', None, 'tp')
- w_down_grad: float32 [64, 1024, 2048], P('sp', 'tp')
The draws below stay inside these ranges and needn't reach their ends.
Inputs may be any that keep to these rules, and one draw needn't show every extreme that they name: `route_ids`: the ids of one token differ. Within each aligned block of 256 tokens (the rows of one index of sp), no expert is named by more than 16 routes, and in every draw some expert is named by exactly 16 routes of some block.
All inputs are finite; a program needn't handle non-finite values.
Results may differ from the reference program's by a relative error of at most 0.009.
Values may be sent and summed in bfloat16 or wider, within the bound.
A program may use at most 128 MiB of HBM per device.

```python
import math
import jax
import jax.numpy as jnp
import numpy as np
from jax import lax

D = 2048
CW = 1024
FF = 1024
TOP = 2
TAPS = 3
EXPERTS = 64
TOK_DEV = 256
TOKENS = 16384
CAP = 16
EXPERT_ROWS = 1024
N_SP = 64
N_TP = 2


def strengthened(drawn, rng, source, target, parts, factor):
    owner, partner = [(jnp.arange(drawn.shape[position]) // (drawn.shape[position] // parts)).reshape([-1 if axis == position else 1 for axis in range(drawn.ndim)]) for position in (source, target)]
    chosen = jax.random.permutation(rng, parts)[partner]
    strong = (owner == chosen) | (owner == (partner + parts // 2) % parts)
    return jnp.where(strong, factor * drawn, drawn)


def level_of(own_key, dims, pieces, smallest, high):
    def one(position, blocks):
        steps = jax.random.uniform(jax.random.fold_in(jax.random.fold_in(own_key, 6), position), (blocks,), jnp.float32, smallest / len(pieces), high / len(pieces))
        return jnp.repeat(jnp.exp(steps), dims[position] // blocks).reshape((-1,) + (1,) * (len(dims) - position - 1))

    factor_of = one(*pieces[0])
    for cut in pieces[1:]:
        factor_of = factor_of * one(*cut)
    return factor_of


def deal_out(stream_key, own, number, rows, count, top, bound, lean):
    ranking = jax.random.permutation(stream_key, count)
    packed, usual = shares(count, rows * top, bound, lean, True), shares(count, rows * top, bound, lean, False)
    places = jnp.arange(count)

    def named(sizes, turn):
        used = int((sizes > 0).sum())
        fixed = max(1, used // 4)
        passed = fixed + (places - fixed + turn * (used - fixed)) % max(1, count - fixed)
        return jnp.zeros((count,), jnp.int32).at[ranking[jnp.where(places < fixed, places, passed)]].set(jnp.asarray(sizes, jnp.int32))

    sizes = jnp.where(number % 4 == 0, named(packed, number // 4), named(usual, number - number // 4 - 1))
    mixed = jax.random.permutation(jax.random.fold_in(own, 3), count)
    giver, taker = mixed[0:count // 2 * 2:2], mixed[1:count // 2 * 2:2]
    room = jnp.minimum(sizes[giver] - 1, bound - sizes[taker]) // 2
    room = jnp.where((giver == ranking[0]) | (taker == ranking[0]) | (sizes[taker] == 0), 0, jnp.maximum(room, 0))
    passed = jax.random.randint(jax.random.fold_in(own, 4), (count // 2,), 0, 1 << 20) % (room + 1)
    sizes = sizes.at[giver].add(-passed).at[taker].add(passed)
    items = jnp.searchsorted(jnp.cumsum(sizes), jnp.arange(rows * top), side="right").astype(jnp.int32)
    listing = items.reshape(top, rows).T
    listing = listing[jax.random.permutation(jax.random.fold_in(own, 1), rows)]
    turn = jax.random.randint(jax.random.fold_in(own, 2), (rows, 1), 0, top)
    return jnp.take_along_axis(listing, (jnp.arange(top)[None, :] + turn) % top, axis=1)


def shares(amount, total, most, skew, full):
    loads = [(1 << 20) // math.isqrt(grade ** skew) + 1 for grade in range(1, amount + 1)]
    largest = most if full else min(most, max(-(-total // amount), total * loads[0] // sum(loads)))
    least = 1 if total - largest >= amount - 1 else 0
    given, rest = [largest] + [least] * (amount - 1), total - largest - least * (amount - 1)
    while rest > 0:
        free = [i for i in range(1, amount) if given[i] < largest] or [i for i in range(1, amount) if given[i] < most]
        whole, left = sum([loads[i] for i in free]), rest
        for i in free:
            addition = min(most - given[i], max(1, left * loads[i] // whole), rest)
            given[i] = given[i] + addition
            rest = rest - addition
    return np.array(given)


def scatter_about(own_key, dims, scale, limit, split=(), kind=jnp.bfloat16):
    array = scale * jax.random.normal(own_key, dims, jnp.float32)
    if split:
        array = array * level_of(own_key, dims, split, -0.22, 0.18)
    return jnp.clip(array, -limit, limit).astype(kind)


def gaussian_with(rng, extent, width, most, pieces, heavy, held_as=jnp.bfloat16):
    result = width * jax.random.normal(rng, extent, jnp.float32)
    if pieces:
        result = result * level_of(rng, extent, pieces, -0.22, 0.18)
    return jnp.clip(strengthened(result, jax.random.fold_in(rng, 3), *heavy), -most, most).astype(held_as)


def setup_inputs(seed: int = 0) -> dict:
    key_list = jax.random.split(jax.random.key(seed), 13)
    stream = scatter_about(key_list[0], (TOKENS, D), 1.0, 6.0, ((0, 64), (1, 2)))
    out_grad = gaussian_with(key_list[1], (TOKENS, D), 1.0, 16.0, ((0, 64), (1, 2)), (0, 1, 64, 4.0))
    gate_in = scatter_about(key_list[2], (TOKENS, CW), 1.0, 6.0, ((0, 64), (1, 2)))
    conv_gate = scatter_about(key_list[3], (TOKENS, CW), 1.0, 6.0, ((0, 64), (1, 2)))
    conv_value = scatter_about(key_list[4], (TOKENS, CW), 1.0, 6.0, ((0, 64), (1, 2)))
    taps = scatter_about(key_list[5], (TAPS, CW), TAPS ** -0.5, 3.5, ((1, 2),), jnp.float32)
    w_out = scatter_about(key_list[6], (D, CW), CW ** -0.5, 0.1875, ((1, 2),))
    route_ids_keys = jax.random.split(jax.random.fold_in(key_list[7], 1), TOKENS // TOK_DEV)
    route_ids_turns = jax.random.permutation(jax.random.fold_in(key_list[7], 3), TOKENS // TOK_DEV)
    route_ids = jax.vmap(lambda own, number: deal_out(jax.random.fold_in(key_list[7], 2), own, number, TOK_DEV, EXPERTS, TOP, CAP, 2))(route_ids_keys, route_ids_turns).reshape((TOKENS, TOP))
    route_weights = jnp.clip(0.1 + 0.9 * jax.random.uniform(key_list[8], (TOKENS, TOP), jnp.float32) ** level_of(key_list[8], (TOKENS, TOP), ((0, 64),), -0.2, 0.2), 0.1, 1.0)
    w_gate = scatter_about(key_list[9], (EXPERTS, D, FF), D ** -0.5, 0.125, ((0, 64), (2, 2)))
    w_up = scatter_about(key_list[10], (EXPERTS, D, FF), D ** -0.5, 0.125, ((0, 64), (2, 2)))
    w_down = scatter_about(key_list[11], (EXPERTS, FF, D), FF ** -0.5, 0.1875, ((0, 64), (1, 2)))
    return {"stream": stream, "out_grad": out_grad, "gate_in": gate_in, "conv_gate": conv_gate, "conv_value": conv_value, "taps": taps, "w_out": w_out, "route_ids": route_ids, "route_weights": route_weights, "w_gate": w_gate, "w_up": w_up, "w_down": w_down}


def expert_step(carry_rows, stream_pad, cot_pad):
    table_row, gate_weight, up_weight, down_weight = carry_rows
    routes_total = TOKENS * TOP
    token_index = jnp.where(table_row < routes_total, table_row // TOP, TOKENS).astype(jnp.int32)
    expert_in = stream_pad[token_index]
    expert_cot = cot_pad[table_row]
    pre_gate = jnp.dot(expert_in, gate_weight, preferred_element_type=jnp.float32)
    pre_up = jnp.dot(expert_in, up_weight, preferred_element_type=jnp.float32)
    sigmoid_gate = jax.nn.sigmoid(pre_gate)
    silu_gate = pre_gate * sigmoid_gate
    hidden = (silu_gate * pre_up).astype(jnp.bfloat16)
    hidden_grad = jnp.dot(expert_cot, down_weight.T, preferred_element_type=jnp.float32)
    down_grad = jnp.dot(hidden.T, expert_cot, preferred_element_type=jnp.float32)
    up_grad = (hidden_grad * silu_gate).astype(jnp.bfloat16)
    gate_grad = (hidden_grad * pre_up * sigmoid_gate * (1.0 + pre_gate * (1.0 - sigmoid_gate))).astype(jnp.bfloat16)
    gate_w_grad = jnp.dot(expert_in.T, gate_grad, preferred_element_type=jnp.float32)
    up_w_grad = jnp.dot(expert_in.T, up_grad, preferred_element_type=jnp.float32)
    block_width = FF // N_TP
    running = jnp.zeros((EXPERT_ROWS, D), jnp.float32)
    for block_index in range(N_TP):
        lower = block_index * block_width
        upper = lower + block_width
        partial_term = jnp.dot(gate_grad[:, lower:upper], gate_weight[:, lower:upper].T, preferred_element_type=jnp.float32)
        partial_term = partial_term + jnp.dot(up_grad[:, lower:upper], up_weight[:, lower:upper].T, preferred_element_type=jnp.float32)
        rounded = lax.optimization_barrier(partial_term.astype(jnp.bfloat16))
        running = running + rounded.astype(jnp.float32)
    return gate_w_grad, up_w_grad, down_grad, running.astype(jnp.bfloat16)


def reference(stream, out_grad, gate_in, conv_gate, conv_value, taps, w_out, route_ids, route_weights, w_gate, w_up, w_down):
    prod_rows = conv_gate.astype(jnp.float32) * conv_value.astype(jnp.float32)
    padded = jnp.concatenate([jnp.zeros((TAPS - 1, CW), jnp.float32), prod_rows], axis=0)
    conv_sum = jnp.zeros((TOKENS, CW), jnp.float32)
    for tap_index in range(TAPS):
        conv_sum = conv_sum + taps[tap_index][None, :] * padded[tap_index:tap_index + TOKENS]
    mixer_out = (gate_in.astype(jnp.float32) * conv_sum).astype(jnp.bfloat16)

    routes_dev = TOK_DEV * TOP
    route_block = route_ids.reshape(N_SP, routes_dev)
    one_hot = (route_block[:, :, None] == jnp.arange(EXPERTS, dtype=jnp.int32)[None, None, :]).astype(jnp.int32)
    slot_pos = jnp.sum(jnp.cumsum(one_hot, axis=1) * one_hot, axis=2) - 1
    source_index = jnp.arange(N_SP, dtype=jnp.int32)[:, None]
    flat_slot = (route_block * EXPERT_ROWS + source_index * CAP + slot_pos).reshape(-1).astype(jnp.int32)
    routes_total = TOKENS * TOP
    table = jnp.full((EXPERTS * EXPERT_ROWS,), routes_total, jnp.int32)
    table = table.at[flat_slot].set(jnp.arange(routes_total, dtype=jnp.int32))
    table = table.reshape(EXPERTS, EXPERT_ROWS)

    stream_pad = jnp.concatenate([stream, jnp.zeros((1, D), jnp.bfloat16)], axis=0)
    scaled = (route_weights[:, :, None] * out_grad[:, None, :].astype(jnp.float32)).astype(jnp.bfloat16)
    cot_pad = jnp.concatenate([scaled.reshape(routes_total, D), jnp.zeros((1, D), jnp.bfloat16)], axis=0)

    def per_expert(carry_rows):
        return expert_step(carry_rows, stream_pad, cot_pad)

    w_gate_grad, w_up_grad, w_down_grad, row_grad = lax.map(per_expert, (table, w_gate, w_up, w_down))
    row_flat = row_grad.reshape(EXPERTS * EXPERT_ROWS, D)
    route_rows = row_flat[flat_slot].astype(jnp.float32).reshape(TOKENS, TOP, D)
    input_grad = jnp.sum(route_rows, axis=1)
    stream_grad = (out_grad.astype(jnp.float32) + input_grad).astype(jnp.bfloat16)

    w_out_grad = jnp.dot(stream_grad.T, mixer_out, preferred_element_type=jnp.float32)
    mixer_grad = jnp.dot(stream_grad, w_out, preferred_element_type=jnp.float32).astype(jnp.bfloat16)
    gate_in_grad = (mixer_grad.astype(jnp.float32) * conv_sum).astype(jnp.bfloat16)
    conv_inner = mixer_grad.astype(jnp.float32) * gate_in.astype(jnp.float32)
    padded_back = jnp.concatenate([conv_inner, jnp.zeros((TAPS - 1, CW), jnp.float32)], axis=0)
    prod_grad = jnp.zeros((TOKENS, CW), jnp.float32)
    for tap_index in range(TAPS):
        offset = TAPS - 1 - tap_index
        prod_grad = prod_grad + taps[tap_index][None, :] * padded_back[offset:offset + TOKENS]
    conv_gate_grad = (prod_grad * conv_value.astype(jnp.float32)).astype(jnp.bfloat16)
    conv_value_grad = (prod_grad * conv_gate.astype(jnp.float32)).astype(jnp.bfloat16)
    return (stream_grad, gate_in_grad, conv_gate_grad, conv_value_grad, w_out_grad, w_gate_grad, w_up_grad, w_down_grad)
```

```python
import functools

import jax
import jax.numpy as jnp
from jax import lax
from jax.experimental import pallas as pl
from jax.experimental.pallas import tpu as pltpu
from jax.sharding import PartitionSpec as P

MESH = pl.DeviceIdType.MESH
BF = jnp.bfloat16
F32 = jnp.float32
SIDE = 4
SLOTS = 16
STRIDE = (16, 4, 1)
ORDERS = ((2, 1, 0), (1, 0, 2), (0, 2, 1))
X_CUTS = ((0, 384), (384, 384), (768, 256))
G_CUTS = ((0, 256), (256, 384), (640, 384))


def coordinate(dim):
    return (lax.axis_index("sp") // STRIDE[dim]) % SIDE


def peer_of(dim, by):
    here = coordinate(dim)
    return lax.axis_index("sp") + ((here + by) % SIDE - here) * STRIDE[dim]


def greet_all():
    barrier = pltpu.get_barrier_semaphore()
    tp = lax.axis_index("tp")
    for dim in range(3):
        for by in range(1, SIDE):
            pl.semaphore_signal(
                barrier, inc=1, device_id=(peer_of(dim, by), tp), device_id_type=MESH
            )
    pl.semaphore_signal(
        barrier, inc=1, device_id=(lax.axis_index("sp"), 1 - tp), device_id_type=MESH
    )


def all_greeted():
    pl.semaphore_wait(pltpu.get_barrier_semaphore(), 10)


def piece(ref, dim, at, cut):
    index = [slice(None)] * 3
    index[dim] = at
    return ref.at[(*index, slice(None), pl.ds(cut[0], cut[1]))]


def phase_copies(source, target, dim, cut, send_sem, recv_sem, local_sem):
    here = coordinate(dim)
    tp = lax.axis_index("tp")
    copies = []
    for by in (2, 1, 3):
        copies.append(
            pltpu.make_async_remote_copy(
                src_ref=piece(source, dim, (here + by) % SIDE, cut),
                dst_ref=piece(target, dim, here, cut),
                send_sem=send_sem.at[by - 1],
                recv_sem=recv_sem.at[by - 1],
                device_id=(peer_of(dim, by), tp),
                device_id_type=MESH,
            )
        )
    copies.append(
        pltpu.make_async_copy(
            piece(source, dim, here, cut), piece(target, dim, here, cut), local_sem
        )
    )
    return copies


def start_all(copies):
    for copy in copies:
        copy.start()


def arrive_all(copies):
    for copy in copies[:-1]:
        copy.wait_recv()
    copies[-1].wait()


def slots_in_lanes(ids):
    tokens = ids.shape[1]
    expert = lax.broadcasted_iota(jnp.int32, (64, tokens), 0)
    first, second = ids[0:1, :], ids[1:2, :]
    named = jnp.where((expert == first) | (expert == second), 1.0, 0.0)
    before = (
        lax.broadcasted_iota(jnp.int32, (tokens, tokens), 0)
        < lax.broadcasted_iota(jnp.int32, (tokens, tokens), 1)
    )
    earlier = jnp.dot(
        named.astype(BF), jnp.where(before, 1.0, 0.0).astype(BF), preferred_element_type=F32
    )
    position = [
        jnp.sum(jnp.where(expert == which, earlier, 0.0), axis=0, keepdims=True).astype(jnp.int32)
        for which in (first, second)
    ]
    return first * SLOTS + position[0], second * SLOTS + position[1]


def dispatch_kernel(
    ids_ref,
    weights_ref,
    stream_ref,
    cot_ref,
    full_x,
    full_g,
    hot_ref,
    send,
    middle,
    send_sems,
    recv_sems,
    local_sems,
    tp_send,
    tp_recv,
):
    tp = lax.axis_index("tp")
    greet_all()
    slot0, slot1 = slots_in_lanes(ids_ref[...])
    weight0, weight1 = weights_ref[0:1, :], weights_ref[1:2, :]
    for z in range(SIDE):
        rows = 256
        row = lax.broadcasted_iota(jnp.int32, (rows, 256), 0) + z * rows
        is0, is1 = row == slot0, row == slot1
        hot = jnp.where(is0 | is1, 1.0, 0.0).astype(BF)
        hot_ref[pl.ds(z * rows, rows), :] = hot
        send[0, z] = (
            jnp.dot(hot, stream_ref[...], preferred_element_type=F32)
            .astype(BF)
            .reshape(4, 4, SLOTS, 1024)
        )
        scale = jnp.sum(
            jnp.where(is0, weight0, 0.0) + jnp.where(is1, weight1, 0.0), axis=1, keepdims=True
        )
        send[1, z] = (
            (scale * jnp.dot(hot, cot_ref[...], preferred_element_type=F32))
            .astype(BF)
            .reshape(4, 4, SLOTS, 1024)
        )
    all_greeted()
    full = (full_x, full_g)
    portions = []
    for tensor, cuts in enumerate((X_CUTS, G_CUTS)):
        stages = (send.at[tensor], middle.at[0, tensor], middle.at[1, tensor], full[tensor].at[tp])
        for which, cut in enumerate(cuts):
            number = tensor * 3 + which
            portions.append(
                [
                    phase_copies(
                        stages[phase],
                        stages[phase + 1],
                        ORDERS[which][phase],
                        cut,
                        send_sems.at[number, phase],
                        recv_sems.at[number, phase],
                        local_sems.at[number, phase],
                    )
                    for phase in range(3)
                ]
            )
    for portion in portions:
        start_all(portion[0])
    for phase in range(1, 3):
        for portion in portions:
            arrive_all(portion[phase - 1])
            start_all(portion[phase])
    crossings = []
    for number, portion in enumerate(portions):
        arrive_all(portion[2])
        tensor, which = divmod(number, 3)
        cut = (X_CUTS, G_CUTS)[tensor][which]
        half = full[tensor].at[tp, :, :, :, :, pl.ds(cut[0], cut[1])]
        crossing = pltpu.make_async_remote_copy(
            src_ref=half,
            dst_ref=half,
            send_sem=tp_send.at[number],
            recv_sem=tp_recv.at[number],
            device_id=(lax.axis_index("sp"), 1 - tp),
            device_id_type=MESH,
        )
        crossing.start()
        crossings.append(crossing)
    for crossing in crossings:
        crossing.wait()
    for portion in portions:
        for copies in portion:
            for copy in copies[:-1]:
                copy.wait_send()


def dispatched(ids, weights, stream, cot):
    vmem = pl.BlockSpec(memory_space=pltpu.VMEM)
    return pl.pallas_call(
        dispatch_kernel,
        out_shape=(
            jax.ShapeDtypeStruct((2, 4, 4, 4, SLOTS, 1024), BF),
            jax.ShapeDtypeStruct((2, 4, 4, 4, SLOTS, 1024), BF),
            jax.ShapeDtypeStruct((1024, 256), BF),
        ),
        in_specs=[vmem] * 4,
        out_specs=(vmem,) * 3,
        scratch_shapes=[
            pltpu.VMEM((2, 4, 4, 4, SLOTS, 1024), BF),
            pltpu.VMEM((2, 2, 4, 4, 4, SLOTS, 1024), BF),
            pltpu.SemaphoreType.DMA((6, 3, 3)),
            pltpu.SemaphoreType.DMA((6, 3, 3)),
            pltpu.SemaphoreType.DMA((6, 3)),
            pltpu.SemaphoreType.DMA((6,)),
            pltpu.SemaphoreType.DMA((6,)),
        ],
        compiler_params=pltpu.CompilerParams(
            collective_id=0, has_side_effects=True, vmem_limit_bytes=60 << 20
        ),
    )(ids, weights, stream, cot)


def return_kernel(
    rows_ref,
    hot_ref,
    cot_ref,
    half_ref,
    whole_ref,
    middle,
    send_sems,
    recv_sems,
    local_sems,
    tp_send,
    tp_recv,
):
    tp = lax.axis_index("tp")
    greet_all()
    all_greeted()
    stages = (rows_ref, middle.at[0], middle.at[1], middle.at[2])
    portions = [
        [
            phase_copies(
                stages[phase],
                stages[phase + 1],
                ORDERS[which][phase],
                cut,
                send_sems.at[which, phase],
                recv_sems.at[which, phase],
                local_sems.at[which, phase],
            )
            for phase in range(3)
        ]
        for which, cut in enumerate(X_CUTS)
    ]
    for portion in portions:
        start_all(portion[0])
    for phase in range(1, 3):
        for portion in portions:
            arrive_all(portion[phase - 1])
            start_all(portion[phase])
    crossings = []
    for which, portion in enumerate(portions):
        arrive_all(portion[2])
        start, width = X_CUTS[which]
        columns = pl.ds(start, width)
        arrived = middle[2, :, :, :, :, columns].reshape(1024, width)
        added = lax.dot_general(
            hot_ref[...], arrived, (((0,), (0,)), ((), ())), preferred_element_type=F32
        )
        total = (cot_ref[:, columns].astype(F32) + added).astype(BF)
        half_ref[:, columns] = total
        whole_ref[tp, :, columns] = total
        crossing = pltpu.make_async_remote_copy(
            src_ref=whole_ref.at[tp, :, columns],
            dst_ref=whole_ref.at[tp, :, columns],
            send_sem=tp_send.at[which],
            recv_sem=tp_recv.at[which],
            device_id=(lax.axis_index("sp"), 1 - tp),
            device_id_type=MESH,
        )
        crossing.start()
        crossings.append(crossing)
    for crossing in crossings:
        crossing.wait()
    for portion in portions:
        for copies in portion:
            for copy in copies[:-1]:
                copy.wait_send()


def returned(rows, hot, cot):
    vmem = pl.BlockSpec(memory_space=pltpu.VMEM)
    return pl.pallas_call(
        return_kernel,
        out_shape=(
            jax.ShapeDtypeStruct((256, 1024), BF),
            jax.ShapeDtypeStruct((2, 256, 1024), BF),
        ),
        in_specs=[vmem] * 3,
        out_specs=(vmem,) * 2,
        scratch_shapes=[
            pltpu.VMEM((3, 4, 4, 4, SLOTS, 1024), BF),
            pltpu.SemaphoreType.DMA((3, 3, 3)),
            pltpu.SemaphoreType.DMA((3, 3, 3)),
            pltpu.SemaphoreType.DMA((3, 3)),
            pltpu.SemaphoreType.DMA((3,)),
            pltpu.SemaphoreType.DMA((3,)),
        ],
        compiler_params=pltpu.CompilerParams(
            collective_id=1, has_side_effects=True, vmem_limit_bytes=40 << 20
        ),
    )(rows, hot, cot)


def passed_along(shard, axis, by):
    count = lax.axis_size(axis)
    pairs = [(i, i + by) for i in range(count) if 0 <= i + by < count]
    return lax.ppermute(shard, axis, pairs)


def dot(a, b):
    return jnp.dot(a, b, preferred_element_type=F32)


def dot_tn(a, b):
    return lax.dot_general(a, b, (((0,), (0,)), ((), ())), preferred_element_type=F32)


def dot_nt(a, b):
    return lax.dot_general(a, b, (((1,), (1,)), ((), ())), preferred_element_type=F32)


def shards(
    stream,
    out_grad,
    gate_in,
    conv_gate,
    conv_value,
    taps,
    w_out,
    route_ids,
    route_weights,
    w_gate,
    w_up,
    w_down,
):
    tok_rows, half_width = stream.shape
    tp = lax.axis_index("tp")
    full_x, full_g, hot = dispatched(route_ids.T, route_weights.T, stream, out_grad)
    full_x = full_x.reshape(2, 1024, half_width)
    full_g = full_g.reshape(2, 1024, half_width)
    wg, wu, wd = w_gate[0], w_up[0], w_down[0]
    lo, hi = slice(0, half_width), slice(half_width, 2 * half_width)
    pre_gate = dot(full_x[0], wg[lo]) + dot(full_x[1], wg[hi])
    pre_up = dot(full_x[0], wu[lo]) + dot(full_x[1], wu[hi])
    sigmoid_gate = jax.nn.sigmoid(pre_gate)
    silu_gate = pre_gate * sigmoid_gate
    hidden = (silu_gate * pre_up).astype(BF)
    hidden_grad = dot_nt(full_g[0], wd[:, lo]) + dot_nt(full_g[1], wd[:, hi])
    up_grad = (hidden_grad * silu_gate).astype(BF)
    gate_grad = (
        hidden_grad * pre_up * sigmoid_gate * (1.0 + pre_gate * (1.0 - sigmoid_gate))
    ).astype(BF)

    def partial_of(side):
        at = side * half_width
        gate_part = lax.dynamic_slice_in_dim(wg, at, half_width, 0)
        up_part = lax.dynamic_slice_in_dim(wu, at, half_width, 0)
        return (dot_nt(gate_grad, gate_part) + dot_nt(up_grad, up_part)).astype(BF)

    theirs = partial_of(1 - tp)
    arrived = lax.ppermute(theirs, "tp", [(0, 1), (1, 0)])
    mine = partial_of(tp)
    row_grad = (mine.astype(F32) + arrived.astype(F32)).astype(BF)
    stream_half, whole = returned(row_grad.reshape(4, 4, 4, SLOTS, half_width), hot, out_grad)
    mixer_grad = (dot(whole[0], w_out[lo]) + dot(whole[1], w_out[hi])).astype(BF)

    depth = taps.shape[0]
    channels = conv_gate.shape[1]
    prod_rows = conv_gate.astype(F32) * conv_value.astype(F32)
    left_rows = passed_along(prod_rows[tok_rows - depth + 1 :], "sp", 1)
    padded = jnp.concatenate([left_rows, prod_rows], axis=0)
    conv_sum = jnp.zeros((tok_rows, channels), F32)
    for tap_index in range(depth):
        conv_sum = conv_sum + taps[tap_index][None, :] * padded[tap_index : tap_index + tok_rows]
    mixer_out = (gate_in.astype(F32) * conv_sum).astype(BF)
    out_blocks = jnp.concatenate(
        [dot_tn(whole[0], mixer_out), dot_tn(whole[1], mixer_out)], axis=0
    ).astype(BF)
    exchanged = lax.all_to_all(
        out_blocks.reshape(64, 32, channels), "sp", split_axis=0, concat_axis=0, tiled=True
    )
    out_proj_grad = exchanged.astype(F32).sum(axis=0)
    mixer_wide = mixer_grad.astype(F32)
    gate_in_grad = (mixer_wide * conv_sum).astype(BF)
    conv_inner = mixer_wide * gate_in.astype(F32)
    right_rows = passed_along(conv_inner[: depth - 1], "sp", -1)
    padded_back = jnp.concatenate([conv_inner, right_rows], axis=0)
    prod_grad = jnp.zeros((tok_rows, channels), F32)
    for tap_index in range(depth):
        offset = depth - 1 - tap_index
        prod_grad = prod_grad + taps[tap_index][None, :] * padded_back[offset : offset + tok_rows]
    conv_gate_grad = (prod_grad * conv_value.astype(F32)).astype(BF)
    conv_value_grad = (prod_grad * conv_gate.astype(F32)).astype(BF)
    gate_w_grad = jnp.concatenate([dot_tn(full_x[0], gate_grad), dot_tn(full_x[1], gate_grad)], 0)
    up_w_grad = jnp.concatenate([dot_tn(full_x[0], up_grad), dot_tn(full_x[1], up_grad)], 0)
    down_w_grad = jnp.concatenate([dot_tn(hidden, full_g[0]), dot_tn(hidden, full_g[1])], 1)
    return (
        stream_half,
        gate_in_grad,
        conv_gate_grad,
        conv_value_grad,
        out_proj_grad,
        gate_w_grad[None],
        up_w_grad[None],
        down_w_grad[None],
    )


def solution(mesh):
    placed = (
        P("sp", "tp"),
        P("sp", "tp"),
        P("sp", "tp"),
        P("sp", "tp"),
        P("sp", "tp"),
        P(None, "tp"),
        P(None, "tp"),
        P("sp", None),
        P("sp", None),
        P("sp", None, "tp"),
        P("sp", None, "tp"),
        P("sp", "tp", None),
    )
    return jax.shard_map(
        shards,
        mesh=mesh,
        in_specs=placed,
        out_specs=(
            P("sp", "tp"),
            P("sp", "tp"),
            P("sp", "tp"),
            P("sp", "tp"),
            P("sp", "tp"),
            P("sp", None, "tp"),
            P("sp", None, "tp"),
            P("sp", "tp", None),
        ),
        check_vma=False,
    )
```

```python
import functools

import jax
import jax.numpy as jnp
from jax import lax
from jax.experimental import pallas as pl
from jax.experimental.pallas import tpu as pltpu
from jax.sharding import PartitionSpec as P

MESH = pl.DeviceIdType.MESH
BF = jnp.bfloat16
F32 = jnp.float32
SIDE = 4
SLOTS = 16
STRIDE = (16, 4, 1)
ORDERS = ((2, 1, 0), (1, 0, 2), (0, 2, 1))
X_CUTS = ((0, 384), (384, 384), (768, 256))
G_CUTS = ((0, 256), (256, 384), (640, 384))


def coordinate(dim):
    return (lax.axis_index("sp") // STRIDE[dim]) % SIDE


def peer_of(dim, by):
    here = coordinate(dim)
    return lax.axis_index("sp") + ((here + by) % SIDE - here) * STRIDE[dim]


def piece(spot, dim, at, width):
    ref, start = spot
    index = [slice(None)] * 3
    index[dim] = at
    return ref.at[(*index, slice(None), pl.ds(start, width))]


def phase_copies(source, target, dim, width, send_sem, recv_sem, local_sem):
    here = coordinate(dim)
    tp = lax.axis_index("tp")
    copies = []
    for by in (2, 1, 3):
        copies.append(
            pltpu.make_async_remote_copy(
                src_ref=piece(source, dim, (here + by) % SIDE, width),
                dst_ref=piece(target, dim, here, width),
                send_sem=send_sem.at[by - 1],
                recv_sem=recv_sem.at[by - 1],
                device_id=(peer_of(dim, by), tp),
                device_id_type=MESH,
            )
        )
    copies.append(
        pltpu.make_async_copy(
            piece(source, dim, here, width), piece(target, dim, here, width), local_sem
        )
    )
    return copies


def start_all(copies):
    for copy in copies:
        copy.start()


def arrive_all(copies):
    for copy in copies[:-1]:
        copy.wait_recv()
    copies[-1].wait()


def slots_in_lanes(ids):
    tokens = ids.shape[1]
    expert = lax.broadcasted_iota(jnp.int32, (64, tokens), 0)
    first, second = ids[0:1, :], ids[1:2, :]
    named = jnp.where((expert == first) | (expert == second), 1.0, 0.0)
    before = (
        lax.broadcasted_iota(jnp.int32, (tokens, tokens), 0)
        < lax.broadcasted_iota(jnp.int32, (tokens, tokens), 1)
    )
    earlier = jnp.dot(
        named.astype(BF), jnp.where(before, 1.0, 0.0).astype(BF), preferred_element_type=F32
    )
    position = [
        jnp.sum(jnp.where(expert == which, earlier, 0.0), axis=0, keepdims=True).astype(jnp.int32)
        for which in (first, second)
    ]
    return first * SLOTS + position[0], second * SLOTS + position[1]


UNIT_CUTS = ((0, 3), (3, 3), (6, 2))


def greet_all():
    barrier = pltpu.get_barrier_semaphore()
    tp = lax.axis_index("tp")
    sp = lax.axis_index("sp")
    for dim in range(3):
        for by in range(1, SIDE):
            pl.semaphore_signal(
                barrier, inc=1, device_id=(peer_of(dim, by), tp), device_id_type=MESH
            )
    for other in ((sp, 1 - tp), ((sp + 1) % 64, tp), ((sp + 63) % 64, tp)):
        pl.semaphore_signal(barrier, inc=1, device_id=other, device_id_type=MESH)


def all_greeted():
    pl.semaphore_wait(pltpu.get_barrier_semaphore(), 12)


def remote(source, target, send_sem, recv_sem, device):
    return pltpu.make_async_remote_copy(
        src_ref=source,
        dst_ref=target,
        send_sem=send_sem,
        recv_sem=recv_sem,
        device_id=device,
        device_id_type=MESH,
    )


def dot(a, b):
    return jnp.dot(a, b, preferred_element_type=F32)


def dot_tn(a, b):
    return lax.dot_general(a, b, (((0,), (0,)), ((), ())), preferred_element_type=F32)


def dot_nt(a, b):
    return lax.dot_general(a, b, (((1,), (1,)), ((), ())), preferred_element_type=F32)


def main_kernel(
    ids_ref,
    weights_ref,
    stream_ref,
    cot_ref,
    gate_in_ref,
    conv_gate_ref,
    conv_value_ref,
    taps_ref,
    w_out_hbm,
    w_gate_hbm,
    w_up_hbm,
    w_down_hbm,
    half_ref,
    gate_in_grad_ref,
    conv_gate_grad_ref,
    conv_value_grad_ref,
    out_block_ref,
    x_hbm,
    g_hbm,
    hidden_hbm,
    gate_hbm,
    up_hbm,
    send,
    middle,
    full_x,
    full_g,
    wg,
    wu,
    wd,
    w_out,
    silu_keep,
    slope_keep,
    hidden,
    gate_grad,
    up_grad,
    arrived,
    back,
    hot_ref,
    whole,
    blocks,
    got1,
    sum1,
    got2,
    sum2,
    got3,
    pad_left,
    pad_right,
    halo,
    conv_sum_ref,
    mixer_out,
    load_sems,
    save_sems,
    send_sems,
    recv_sems,
    local_sems,
    tp_send,
    tp_recv,
    halo_send,
    halo_recv,
    fold_send,
    fold_recv,
):
    tp = lax.axis_index("tp")
    sp = lax.axis_index("sp")
    partner = (sp, 1 - tp)
    greet_all()
    loads = [
        pltpu.make_async_copy(source, target, load_sems.at[k])
        for k, (source, target) in enumerate(
            ((w_gate_hbm.at[0], wg), (w_up_hbm.at[0], wu), (w_down_hbm.at[0], wd), (w_out_hbm, w_out))
        )
    ]
    start_all(loads)

    slot0, slot1 = slots_in_lanes(ids_ref[...])
    weight0, weight1 = weights_ref[0:1, :], weights_ref[1:2, :]
    for z in range(SIDE):
        row = lax.broadcasted_iota(jnp.int32, (256, 256), 0) + z * 256
        hot = jnp.where((row == slot0) | (row == slot1), 1.0, 0.0).astype(BF)
        hot_ref[pl.ds(z * 256, 256), :] = hot
        send[0, z] = dot(hot, stream_ref[...]).astype(BF).reshape(4, 4, SLOTS, 1024)

    def own_half(ref, cut):
        start = pl.multiple_of(tp * 1024 + cut[0], 128)
        return ref.at[:, :, :, :, pl.ds(start, cut[1])]

    full = (full_x, full_g)
    portions = []
    for tensor, cuts in enumerate((X_CUTS, G_CUTS)):
        for which, cut in enumerate(cuts):
            number = tensor * 3 + which
            spots = [
                (send.at[tensor], cut[0]),
                (middle.at[0, tensor], cut[0]),
                (middle.at[1, tensor], cut[0]),
                (full[tensor], pl.multiple_of(tp * 1024 + cut[0], 128)),
            ]
            portions.append(
                [
                    phase_copies(
                        spots[phase],
                        spots[phase + 1],
                        ORDERS[which][phase],
                        cut[1],
                        send_sems.at[number, phase],
                        recv_sems.at[number, phase],
                        local_sems.at[number, phase],
                    )
                    for phase in range(3)
                ]
            )
    all_greeted()
    for portion in portions[:3]:
        start_all(portion[0])
    for z in range(SIDE):
        row = lax.broadcasted_iota(jnp.int32, (256, 256), 0) + z * 256
        scale = jnp.sum(
            jnp.where(row == slot0, weight0, 0.0) + jnp.where(row == slot1, weight1, 0.0),
            axis=1,
            keepdims=True,
        )
        hot = hot_ref[pl.ds(z * 256, 256), :]
        send[1, z] = (scale * dot(hot, cot_ref[...])).astype(BF).reshape(4, 4, SLOTS, 1024)
    for portion in portions[3:]:
        start_all(portion[0])

    pad_left[pl.ds(8, 256), :] = conv_gate_ref[...].astype(F32) * conv_value_ref[...].astype(F32)
    left = remote(
        pad_left.at[pl.ds(256, 8)],
        halo.at[0],
        halo_send.at[0],
        halo_recv.at[0],
        ((sp + 1) % 64, tp),
    )
    left.start()
    for portion in portions:
        arrive_all(portion[0])
        start_all(portion[1])
    left.wait()
    pad_left[pl.ds(0, 8), :] = jnp.where(sp == 0, 0.0, halo[0])
    conv_sum = jnp.zeros((256, 512), F32)
    for tap in range(3):
        conv_sum = conv_sum + taps_ref[tap : tap + 1, :] * pad_left[pl.ds(6 + tap, 256), :]
    conv_sum_ref[...] = conv_sum
    mixer_out[...] = (gate_in_ref[...].astype(F32) * conv_sum).astype(BF)
    for portion in portions:
        arrive_all(portion[1])
        start_all(portion[2])

    crossings = []
    saves = []

    def cross(tensor):
        for which, cut in enumerate((X_CUTS, G_CUTS)[tensor]):
            number = tensor * 3 + which
            arrive_all(portions[number][2])
            part = own_half(full[tensor], cut)
            crossing = remote(part, part, tp_send.at[number], tp_recv.at[number], partner)
            crossing.start()
            crossings.append(crossing)

    def save(source, target):
        copy = pltpu.make_async_copy(source, target, save_sems.at[len(saves)])
        copy.start()
        saves.append(copy)

    cross(0)
    for load in loads:
        load.wait()
    for crossing in crossings[:3]:
        crossing.wait()

    def activate(step, carry):
        rows = full_x[pl.ds(step * 2, 2)].reshape(512, 2048)
        at = pl.ds(pl.multiple_of(step * 512, 512), 512)
        pre_gate = dot(rows, wg[...])
        pre_up = dot(rows, wu[...])
        sigmoid = jax.nn.sigmoid(pre_gate)
        silu = pre_gate * sigmoid
        silu_keep[at, :] = silu
        slope_keep[at, :] = pre_up * sigmoid * (1.0 + pre_gate * (1.0 - sigmoid))
        hidden[at, :] = (silu * pre_up).astype(BF)
        return carry

    lax.fori_loop(0, 2, activate, 0)
    save(full_x, x_hbm)
    save(hidden, hidden_hbm)
    cross(1)
    for crossing in crossings[3:]:
        crossing.wait()

    def differentiate(step, carry):
        rows = full_g[pl.ds(step * 2, 2)].reshape(512, 2048)
        at = pl.ds(pl.multiple_of(step * 512, 512), 512)
        hidden_grad = dot_nt(rows, wd[...])
        up_grad[at, :] = (hidden_grad * silu_keep[at, :]).astype(BF)
        gate_grad[at, :] = (hidden_grad * slope_keep[at, :]).astype(BF)
        return carry

    lax.fori_loop(0, 2, differentiate, 0)
    save(full_g, g_hbm)
    save(gate_grad, gate_hbm)
    save(up_grad, up_hbm)
    for portion in portions:
        for copy in portion[0][:-1]:
            copy.wait_send()

    def partial_of(side, cut):
        at = pl.ds(pl.multiple_of(side * 1024 + cut[0], 128), cut[1])
        return dot_nt(gate_grad[...], wg[at, :]) + dot_nt(up_grad[...], wu[at, :])

    back_stages = (send.at[1], back.at[0], back.at[1], back.at[2])
    returns = [
        [
            phase_copies(
                (back_stages[phase], cut[0]),
                (back_stages[phase + 1], cut[0]),
                ORDERS[which][phase],
                cut[1],
                send_sems.at[6 + which, phase],
                recv_sems.at[6 + which, phase],
                local_sems.at[6 + which, phase],
            )
            for phase in range(3)
        ]
        for which, cut in enumerate(X_CUTS)
    ]
    shares = []
    for which, cut in enumerate(X_CUTS):
        columns = pl.ds(cut[0], cut[1])
        send[0, :, :, :, :, columns] = (
            partial_of(1 - tp, cut).astype(BF).reshape(4, 4, 4, SLOTS, cut[1])
        )
        share = remote(
            send.at[0, :, :, :, :, columns],
            arrived.at[:, :, :, :, columns],
            tp_send.at[6 + which],
            tp_recv.at[6 + which],
            partner,
        )
        share.start()
        shares.append(share)
    for which, cut in enumerate(X_CUTS):
        columns = pl.ds(cut[0], cut[1])
        mine = partial_of(tp, cut).astype(BF).astype(F32)
        shares[which].wait_recv()
        theirs = arrived[:, :, :, :, columns].reshape(1024, cut[1]).astype(F32)
        send[1, :, :, :, :, columns] = (mine + theirs).astype(BF).reshape(4, 4, 4, SLOTS, cut[1])
        start_all(returns[which][0])
    for phase in range(1, 3):
        for portion in returns:
            arrive_all(portion[phase - 1])
            start_all(portion[phase])

    swaps = []
    for which, portion in enumerate(returns):
        arrive_all(portion[2])
        cut = X_CUTS[which]
        columns = pl.ds(cut[0], cut[1])
        added = dot_tn(hot_ref[...], back[2, :, :, :, :, columns].reshape(1024, cut[1]))
        total = (cot_ref[:, columns].astype(F32) + added).astype(BF)
        half_ref[:, columns] = total
        whole[tp, :, columns] = total
        swap = remote(
            whole.at[tp, :, columns],
            whole.at[tp, :, columns],
            tp_send.at[9 + which],
            tp_recv.at[9 + which],
            partner,
        )
        swap.start()
        swaps.append(swap)

    def block_of(half):
        for part in range(2):
            product = dot_tn(whole[half, :, pl.ds(part * 512, 512)], mixer_out[...])
            for tile in range(4):
                blocks[half * 2 + part, :, :, pl.ds(tile * 2, 2)] = (
                    product[:, tile * 128 : (tile + 1) * 128].astype(BF).reshape(4, 4, 2, 16, 128)
                )

    block_of(tp)
    for swap in swaps:
        swap.wait()
    block_of(1 - tp)

    def fold_copies(which, phase):
        start, count = UNIT_CUTS[which]
        dim = ORDERS[which][phase]
        here = coordinate(dim)
        left_dims = sorted(ORDERS[which][phase:])
        copies = []
        for by in (2, 1, 3):
            index = [slice(None)] * len(left_dims)
            index[left_dims.index(dim)] = (here + by) % SIDE
            units = pl.ds(start, count)
            if phase == 0:
                source = blocks.at[(*index, units)]
                target = got1.at[by - 1, :, :, units]
            elif phase == 1:
                source = sum1.at[(*index, units)]
                target = got2.at[by - 1, :, units]
            else:
                source = sum2.at[(*index, units)]
                target = got3.at[by - 1, units]
            copies.append(
                remote(
                    source,
                    target,
                    fold_send.at[which, phase, by - 1],
                    fold_recv.at[which, phase, by - 1],
                    (peer_of(dim, by), tp),
                )
            )
        return copies

    def folded(which, phase):
        start, count = UNIT_CUTS[which]
        units = pl.ds(start, count)
        dim = ORDERS[which][phase]
        left_dims = sorted(ORDERS[which][phase:])
        index = [slice(None)] * len(left_dims)
        index[left_dims.index(dim)] = coordinate(dim)
        source = (blocks, sum1, sum2)[phase]
        total = source[(*index, units)].astype(F32)
        for by in range(3):
            if phase == 0:
                total = total + got1[by, :, :, units].astype(F32)
            elif phase == 1:
                total = total + got2[by, :, units].astype(F32)
            else:
                total = total + got3[by, units].astype(F32)
        return total

    folds = [[fold_copies(which, phase) for phase in range(3)] for which in range(3)]
    for fold in folds:
        start_all(fold[0])

    mixer_grad = (dot(whole[0], w_out[0:1024, :]) + dot(whole[1], w_out[1024:2048, :])).astype(BF)
    mixer_wide = mixer_grad.astype(F32)
    gate_in_grad_ref[...] = (mixer_wide * conv_sum_ref[...]).astype(BF)
    pad_right[pl.ds(0, 256), :] = mixer_wide * gate_in_ref[...].astype(F32)
    right = remote(
        pad_right.at[pl.ds(0, 8)],
        halo.at[1],
        halo_send.at[1],
        halo_recv.at[1],
        ((sp + 63) % 64, tp),
    )
    right.start()
    for which, fold in enumerate(folds):
        start, count = UNIT_CUTS[which]
        for copy in fold[0]:
            copy.wait_recv()
        sum1[:, :, pl.ds(start, count)] = folded(which, 0).astype(BF)
        start_all(fold[1])
    right.wait()
    pad_right[pl.ds(256, 8), :] = jnp.where(sp == 63, 0.0, halo[1])
    prod_grad = jnp.zeros((256, 512), F32)
    for tap in range(3):
        prod_grad = prod_grad + taps_ref[tap : tap + 1, :] * pad_right[pl.ds(2 - tap, 256), :]
    conv_gate_grad_ref[...] = (prod_grad * conv_value_ref[...].astype(F32)).astype(BF)
    conv_value_grad_ref[...] = (prod_grad * conv_gate_ref[...].astype(F32)).astype(BF)
    for which, fold in enumerate(folds):
        start, count = UNIT_CUTS[which]
        for copy in fold[1]:
            copy.wait_recv()
        sum2[:, pl.ds(start, count)] = folded(which, 1).astype(BF)
        start_all(fold[2])
    for which, fold in enumerate(folds):
        start, count = UNIT_CUTS[which]
        for copy in fold[2]:
            copy.wait_recv()
        total = folded(which, 2)
        for unit in range(count):
            tile, row = divmod(start + unit, 2)
            out_block_ref[pl.ds(row * 16, 16), pl.ds(tile * 128, 128)] = total[unit]
    for share in shares:
        share.wait_send()
    for portion in portions:
        for copies in portion[1:]:
            for copy in copies[:-1]:
                copy.wait_send()
    for portion in returns:
        for copies in portion:
            for copy in copies[:-1]:
                copy.wait_send()
    for fold in folds:
        for copies in fold:
            for copy in copies:
                copy.wait_send()
    for copy in saves:
        copy.wait()


def main_call(*operands):
    vmem = pl.BlockSpec(memory_space=pltpu.VMEM)
    hbm = pl.BlockSpec(memory_space=pl.ANY)
    shape = jax.ShapeDtypeStruct
    rows_shape = (4, 4, 4, SLOTS, 1024)
    full_shape = (4, 4, 4, SLOTS, 2048)
    dma = pltpu.SemaphoreType.DMA
    return pl.pallas_call(
        main_kernel,
        out_shape=(
            shape((256, 1024), BF),
            shape((256, 512), BF),
            shape((256, 512), BF),
            shape((256, 512), BF),
            shape((32, 512), F32),
            shape(full_shape, BF),
            shape(full_shape, BF),
            shape((1024, 512), BF),
            shape((1024, 512), BF),
            shape((1024, 512), BF),
        ),
        in_specs=[vmem] * 8 + [hbm] * 4,
        out_specs=(vmem,) * 5 + (hbm,) * 5,
        scratch_shapes=[
            pltpu.VMEM((2, *rows_shape), BF),
            pltpu.VMEM((2, 2, *rows_shape), BF),
            pltpu.VMEM(full_shape, BF),
            pltpu.VMEM(full_shape, BF),
            pltpu.VMEM((2048, 512), BF),
            pltpu.VMEM((2048, 512), BF),
            pltpu.VMEM((512, 2048), BF),
            pltpu.VMEM((2048, 512), BF),
            pltpu.VMEM((1024, 512), F32),
            pltpu.VMEM((1024, 512), F32),
            pltpu.VMEM((1024, 512), BF),
            pltpu.VMEM((1024, 512), BF),
            pltpu.VMEM((1024, 512), BF),
            pltpu.VMEM(rows_shape, BF),
            pltpu.VMEM((3, *rows_shape), BF),
            pltpu.VMEM((1024, 256), BF),
            pltpu.VMEM((2, 256, 1024), BF),
            pltpu.VMEM((4, 4, 4, 8, 16, 128), BF),
            pltpu.VMEM((3, 4, 4, 8, 16, 128), BF),
            pltpu.VMEM((4, 4, 8, 16, 128), BF),
            pltpu.VMEM((3, 4, 8, 16, 128), BF),
            pltpu.VMEM((4, 8, 16, 128), BF),
            pltpu.VMEM((3, 8, 16, 128), BF),
            pltpu.VMEM((264, 512), F32),
            pltpu.VMEM((264, 512), F32),
            pltpu.VMEM((2, 8, 512), F32),
            pltpu.VMEM((256, 512), F32),
            pltpu.VMEM((256, 512), BF),
            dma((4,)),
            dma((5,)),
            dma((9, 3, 3)),
            dma((9, 3, 3)),
            dma((9, 3)),
            dma((12,)),
            dma((12,)),
            dma((2,)),
            dma((2,)),
            dma((3, 3, 3)),
            dma((3, 3, 3)),
        ],
        compiler_params=pltpu.CompilerParams(
            collective_id=0, has_side_effects=True, vmem_limit_bytes=67043328
        ),
    )(*operands)


def shards(
    stream,
    out_grad,
    gate_in,
    conv_gate,
    conv_value,
    taps,
    w_out,
    route_ids,
    route_weights,
    w_gate,
    w_up,
    w_down,
):
    half, gate_in_grad, conv_gate_grad, conv_value_grad, out_block, x, g, hidden, gate, up = main_call(
        route_ids.T,
        route_weights.T,
        stream,
        out_grad,
        gate_in,
        conv_gate,
        conv_value,
        taps,
        w_out,
        w_gate,
        w_up,
        w_down,
    )
    x = x.reshape(1024, 2048)
    g = g.reshape(1024, 2048)
    return (
        half,
        gate_in_grad,
        conv_gate_grad,
        conv_value_grad,
        out_block,
        dot_tn(x, gate)[None],
        dot_tn(x, up)[None],
        dot_tn(hidden, g)[None],
    )


def solution(mesh):
    placed = (
        P("sp", "tp"),
        P("sp", "tp"),
        P("sp", "tp"),
        P("sp", "tp"),
        P("sp", "tp"),
        P(None, "tp"),
        P(None, "tp"),
        P("sp", None),
        P("sp", None),
        P("sp", None, "tp"),
        P("sp", None, "tp"),
        P("sp", "tp", None),
    )
    return jax.shard_map(
        shards,
        mesh=mesh,
        in_specs=placed,
        out_specs=(
            P("sp", "tp"),
            P("sp", "tp"),
            P("sp", "tp"),
            P("sp", "tp"),
            P("sp", "tp"),
            P("sp", None, "tp"),
            P("sp", None, "tp"),
            P("sp", "tp", None),
        ),
        check_vma=False,
    )
```

```python
import functools

import jax
import jax.numpy as jnp
from jax import lax
from jax.experimental import pallas as pl
from jax.experimental.pallas import tpu as pltpu
from jax.sharding import PartitionSpec as P

MESH = pl.DeviceIdType.MESH
BF = jnp.bfloat16
F32 = jnp.float32
SIDE = 4
SLOTS = 16
STRIDE = (16, 4, 1)
ORDERS = ((2, 1, 0), (1, 0, 2), (0, 2, 1))
Z_OFFSETS = (0, 2, 1, 3)
LATE_SHORT = ((0, 384), (384, 384), (768, 256))
EARLY_SHORT = ((0, 256), (256, 384), (640, 384))
MIDDLE_SHORT = ((0, 384), (384, 256), (640, 384))
X_CUTS = (LATE_SHORT, MIDDLE_SHORT)
G_CUTS = (EARLY_SHORT, LATE_SHORT)
BACK_CUTS = (MIDDLE_SHORT, EARLY_SHORT)


def coordinate(dim):
    return (lax.axis_index("sp") // STRIDE[dim]) % SIDE


def peer_of(dim, by):
    here = coordinate(dim)
    return lax.axis_index("sp") + ((here + by) % SIDE - here) * STRIDE[dim]


def piece(spot, index, width):
    ref, start = spot
    return ref.at[(*index, slice(None), pl.ds(start, width))]


def phase_copies(source, target, dim, width, chunk, send_sem, recv_sem, local_sem):
    here = coordinate(dim)
    tp = lax.axis_index("tp")
    moves = []
    if dim == 0:
        every = (slice(None), slice(None))
        if chunk == 0:
            kept = ((0, *every), (0, *every))
            moves.append((2, (1, *every), (1, *every)))
        else:
            kept = None
            moves.append((1, (2, *every), (3, *every)))
            moves.append((3, (3, *every), (2, *every)))
    else:

        def at(place):
            index = [pl.ds(2 * chunk, 2), slice(None), slice(None)]
            index[dim] = place
            return tuple(index)

        kept = (at(here), at(here))
        for by in (2, 1, 3):
            moves.append((by, at((here + by) % SIDE), at(here)))
    sent = [
        pltpu.make_async_remote_copy(
            src_ref=piece(source, from_index, width),
            dst_ref=piece(target, to_index, width),
            send_sem=send_sem.at[by - 1],
            recv_sem=recv_sem.at[by - 1],
            device_id=(peer_of(dim, by), tp),
            device_id_type=MESH,
        )
        for by, from_index, to_index in moves
    ]
    local = []
    if kept is not None:
        local.append(
            pltpu.make_async_copy(
                piece(source, kept[0], width), piece(target, kept[1], width), local_sem
            )
        )
    return sent, local


def start_phase(copies):
    for copy in copies[0] + copies[1]:
        copy.start()


def arrive_phase(copies):
    for copy in copies[0]:
        copy.wait_recv()
    for copy in copies[1]:
        copy.wait()


def sent_phase(copies):
    for copy in copies[0]:
        copy.wait_send()


def start_all(copies):
    for copy in copies:
        copy.start()


def slots_in_lanes(ids):
    tokens = ids.shape[1]
    expert = lax.broadcasted_iota(jnp.int32, (64, tokens), 0)
    first, second = ids[0:1, :], ids[1:2, :]
    named = jnp.where((expert == first) | (expert == second), 1.0, 0.0)
    before = (
        lax.broadcasted_iota(jnp.int32, (tokens, tokens), 0)
        < lax.broadcasted_iota(jnp.int32, (tokens, tokens), 1)
    )
    earlier = jnp.dot(
        named.astype(BF), jnp.where(before, 1.0, 0.0).astype(BF), preferred_element_type=F32
    )
    position = [
        jnp.sum(jnp.where(expert == which, earlier, 0.0), axis=0, keepdims=True).astype(jnp.int32)
        for which in (first, second)
    ]
    return first * SLOTS + position[0], second * SLOTS + position[1]


UNIT_CUTS = ((0, 3), (3, 3), (6, 2))


def greet_all():
    barrier = pltpu.get_barrier_semaphore()
    tp = lax.axis_index("tp")
    sp = lax.axis_index("sp")
    for dim in range(3):
        for by in range(1, SIDE):
            pl.semaphore_signal(
                barrier, inc=1, device_id=(peer_of(dim, by), tp), device_id_type=MESH
            )
    for other in ((sp, 1 - tp), ((sp + 1) % 64, tp), ((sp + 63) % 64, tp)):
        pl.semaphore_signal(barrier, inc=1, device_id=other, device_id_type=MESH)


def all_greeted():
    pl.semaphore_wait(pltpu.get_barrier_semaphore(), 12)


def remote(source, target, send_sem, recv_sem, device):
    return pltpu.make_async_remote_copy(
        src_ref=source,
        dst_ref=target,
        send_sem=send_sem,
        recv_sem=recv_sem,
        device_id=device,
        device_id_type=MESH,
    )


def dot(a, b):
    return jnp.dot(a, b, preferred_element_type=F32)


def dot_tn(a, b):
    return lax.dot_general(a, b, (((0,), (0,)), ((), ())), preferred_element_type=F32)


def dot_nt(a, b):
    return lax.dot_general(a, b, (((1,), (1,)), ((), ())), preferred_element_type=F32)


def main_kernel(
    ids_ref,
    weights_ref,
    stream_ref,
    cot_ref,
    gate_in_ref,
    conv_gate_ref,
    conv_value_ref,
    taps_ref,
    w_out_hbm,
    w_gate_hbm,
    w_up_hbm,
    w_down_hbm,
    half_ref,
    gate_in_grad_ref,
    conv_gate_grad_ref,
    conv_value_grad_ref,
    out_block_ref,
    x_hbm,
    g_hbm,
    hidden_hbm,
    gate_hbm,
    up_hbm,
    send,
    middle,
    full_x,
    full_g,
    wg,
    wu,
    wd,
    w_out,
    silu_keep,
    slope_keep,
    hidden,
    gate_grad,
    up_grad,
    shared,
    arrived,
    rows_out,
    back,
    added_ref,
    hot_ref,
    whole,
    blocks,
    got1,
    sum1,
    got2,
    sum2,
    got3,
    pad_left,
    pad_right,
    halo,
    conv_sum_ref,
    mixer_out,
    load_sems,
    save_sems,
    send_sems,
    recv_sems,
    local_sems,
    tp_send,
    tp_recv,
    halo_send,
    halo_recv,
    fold_send,
    fold_recv,
):
    tp = lax.axis_index("tp")
    sp = lax.axis_index("sp")
    partner = (sp, 1 - tp)
    greet_all()
    loads = [
        pltpu.make_async_copy(source, target, load_sems.at[k])
        for k, (source, target) in enumerate(
            ((w_gate_hbm.at[0], wg), (w_up_hbm.at[0], wu), (w_down_hbm.at[0], wd), (w_out_hbm, w_out))
        )
    ]
    start_all(loads)

    slot0, slot1 = slots_in_lanes(ids_ref[...])
    weight0, weight1 = weights_ref[0:1, :], weights_ref[1:2, :]

    def row_numbers(place):
        z = (coordinate(0) + Z_OFFSETS[place]) % SIDE
        return lax.broadcasted_iota(jnp.int32, (256, 256), 0) + z * 256

    def gather_x(chunk):
        for place in (2 * chunk, 2 * chunk + 1):
            row = row_numbers(place)
            hot = jnp.where((row == slot0) | (row == slot1), 1.0, 0.0).astype(BF)
            hot_ref[pl.ds(place * 256, 256), :] = hot
            send[0, place] = dot(hot, stream_ref[...]).astype(BF).reshape(4, 4, SLOTS, 1024)

    def gather_g(chunk):
        for place in (2 * chunk, 2 * chunk + 1):
            row = row_numbers(place)
            scale = jnp.sum(
                jnp.where(row == slot0, weight0, 0.0) + jnp.where(row == slot1, weight1, 0.0),
                axis=1,
                keepdims=True,
            )
            hot = hot_ref[pl.ds(place * 256, 256), :]
            send[1, place] = (
                (scale * dot(hot, cot_ref[...])).astype(BF).reshape(4, 4, SLOTS, 1024)
            )

    full = (full_x, full_g)

    def stream_of(number, spots_of, cuts, chunk):
        portions = []
        for which, cut in enumerate(cuts):
            spots = spots_of(cut)
            portions.append(
                [
                    phase_copies(
                        spots[phase],
                        spots[phase + 1],
                        ORDERS[which][phase],
                        cut[1],
                        chunk,
                        send_sems.at[number * 3 + which, phase],
                        recv_sems.at[number * 3 + which, phase],
                        local_sems.at[number * 3 + which, phase],
                    )
                    for phase in range(3)
                ]
            )
        return portions

    def outward(tensor, chunk):
        return stream_of(
            chunk * 2 + tensor,
            lambda cut: (
                (send.at[tensor], cut[0]),
                (middle.at[0, tensor], cut[0]),
                (middle.at[1, tensor], cut[0]),
                (full[tensor], pl.multiple_of(tp * 1024 + cut[0], 128)),
            ),
            (X_CUTS, G_CUTS)[tensor][chunk],
            chunk,
        )

    def homeward(chunk):
        return stream_of(
            4 + chunk,
            lambda cut: (
                (rows_out, cut[0]),
                (back.at[0], cut[0]),
                (back.at[1], cut[0]),
                (back.at[2], cut[0]),
            ),
            BACK_CUTS[chunk],
            chunk,
        )

    xs = [outward(0, chunk) for chunk in range(2)]
    gs = [outward(1, chunk) for chunk in range(2)]
    backs = [homeward(chunk) for chunk in range(2)]

    def begin(portions):
        for portion in portions:
            start_phase(portion[0])

    def advance(portions, phase):
        for portion in portions:
            arrive_phase(portion[phase - 1])
            start_phase(portion[phase])

    crossings = {}
    saves = []

    def cross(tensor, chunk):
        crossings[tensor, chunk] = []
        portions = (xs, gs)[tensor][chunk]
        for which, cut in enumerate((X_CUTS, G_CUTS)[tensor][chunk]):
            number = (chunk * 2 + tensor) * 3 + which
            arrive_phase(portions[which][2])
            start = pl.multiple_of(tp * 1024 + cut[0], 128)
            part = full[tensor].at[pl.ds(2 * chunk, 2), :, :, :, pl.ds(start, cut[1])]
            crossing = remote(part, part, tp_send.at[number], tp_recv.at[number], partner)
            crossing.start()
            crossings[tensor, chunk].append(crossing)

    def crossed(tensor, chunk):
        for crossing in crossings[tensor, chunk]:
            crossing.wait()

    def save(source, target):
        copy = pltpu.make_async_copy(source, target, save_sems.at[len(saves)])
        copy.start()
        saves.append(copy)

    def activate(chunk):
        rows = full_x[pl.ds(chunk * 2, 2)].reshape(512, 2048)
        at = pl.ds(chunk * 512, 512)
        pre_gate = dot(rows, wg[...])
        pre_up = dot(rows, wu[...])
        sigmoid = jax.nn.sigmoid(pre_gate)
        silu = pre_gate * sigmoid
        silu_keep[at, :] = silu
        slope_keep[at, :] = pre_up * sigmoid * (1.0 + pre_gate * (1.0 - sigmoid))
        hidden[at, :] = (silu * pre_up).astype(BF)

    def differentiate(chunk):
        rows = full_g[pl.ds(chunk * 2, 2)].reshape(512, 2048)
        at = pl.ds(chunk * 512, 512)
        hidden_grad = dot_nt(rows, wd[...])
        up_grad[at, :] = (hidden_grad * silu_keep[at, :]).astype(BF)
        gate_grad[at, :] = (hidden_grad * slope_keep[at, :]).astype(BF)

    def partial_of(side, cut, chunk):
        at = pl.ds(pl.multiple_of(side * 1024 + cut[0], 128), cut[1])
        rows = pl.ds(chunk * 512, 512)
        return dot_nt(gate_grad[rows, :], wg[at, :]) + dot_nt(up_grad[rows, :], wu[at, :])

    shares = {}

    def part(chunk, cut):
        return (pl.ds(2 * chunk, 2), slice(None), slice(None), slice(None), pl.ds(*cut))

    def share_theirs(chunk):
        shares[chunk] = []
        for which, cut in enumerate(BACK_CUTS[chunk]):
            index = part(chunk, cut)
            shared[index] = (
                partial_of(1 - tp, cut, chunk).astype(BF).reshape(2, 4, 4, SLOTS, cut[1])
            )
            number = 12 + chunk * 3 + which
            share = remote(
                shared.at[index],
                arrived.at[index],
                tp_send.at[number],
                tp_recv.at[number],
                partner,
            )
            share.start()
            shares[chunk].append(share)

    def add_mine(chunk, begin_return):
        for which, cut in enumerate(BACK_CUTS[chunk]):
            index = part(chunk, cut)
            mine = partial_of(tp, cut, chunk).astype(BF).astype(F32)
            shares[chunk][which].wait_recv()
            theirs = arrived[index].reshape(512, cut[1]).astype(F32)
            rows_out[index] = (mine + theirs).astype(BF).reshape(2, 4, 4, SLOTS, cut[1])
            if begin_return:
                start_phase(backs[chunk][which][0])

    gather_x(0)
    all_greeted()
    begin(xs[0])
    gather_g(0)
    begin(gs[0])
    gather_x(1)
    gather_g(1)
    pad_left[pl.ds(8, 256), :] = conv_gate_ref[...].astype(F32) * conv_value_ref[...].astype(F32)
    left = remote(
        pad_left.at[pl.ds(256, 8)],
        halo.at[0],
        halo_send.at[0],
        halo_recv.at[0],
        ((sp + 1) % 64, tp),
    )
    left.start()
    advance(xs[0], 1)
    advance(gs[0], 1)
    left.wait()
    pad_left[pl.ds(0, 8), :] = jnp.where(sp == 0, 0.0, halo[0])
    conv_sum = jnp.zeros((256, 512), F32)
    for tap in range(3):
        conv_sum = conv_sum + taps_ref[tap : tap + 1, :] * pad_left[pl.ds(6 + tap, 256), :]
    conv_sum_ref[...] = conv_sum
    mixer_out[...] = (gate_in_ref[...].astype(F32) * conv_sum).astype(BF)
    advance(xs[0], 2)
    advance(gs[0], 2)
    begin(xs[1])
    cross(0, 0)
    begin(gs[1])
    cross(1, 0)
    for load in loads:
        load.wait()
    crossed(0, 0)
    activate(0)
    advance(xs[1], 1)
    crossed(1, 0)
    differentiate(0)
    advance(gs[1], 1)
    share_theirs(0)
    advance(xs[1], 2)
    add_mine(0, False)
    advance(gs[1], 2)
    begin(backs[0])
    cross(0, 1)
    crossed(0, 1)
    activate(1)
    save(full_x, x_hbm)
    save(hidden, hidden_hbm)
    advance(backs[0], 1)
    cross(1, 1)
    crossed(1, 1)
    differentiate(1)
    save(full_g, g_hbm)
    save(gate_grad, gate_hbm)
    save(up_grad, up_hbm)
    share_theirs(1)
    advance(backs[0], 2)
    add_mine(1, True)
    for portion in backs[0]:
        arrive_phase(portion[2])
    added_ref[...] = dot_tn(
        hot_ref[pl.ds(0, 512), :], back[2, pl.ds(0, 2)].reshape(512, 1024)
    ) + cot_ref[...].astype(F32)
    advance(backs[1], 1)
    advance(backs[1], 2)

    swaps = []
    for which, portion in enumerate(backs[1]):
        arrive_phase(portion[2])
        cut = BACK_CUTS[1][which]
        columns = pl.ds(*cut)
        rows = back[2, pl.ds(2, 2), :, :, :, columns].reshape(512, cut[1])
        total = (added_ref[:, columns] + dot_tn(hot_ref[pl.ds(512, 512), :], rows)).astype(BF)
        half_ref[:, columns] = total
        whole[tp, :, columns] = total
        swap = remote(
            whole.at[tp, :, columns],
            whole.at[tp, :, columns],
            tp_send.at[18 + which],
            tp_recv.at[18 + which],
            partner,
        )
        swap.start()
        swaps.append(swap)

    def block_of(half):
        for part in range(2):
            product = dot_tn(whole[half, :, pl.ds(part * 512, 512)], mixer_out[...])
            for tile in range(4):
                blocks[half * 2 + part, :, :, pl.ds(tile * 2, 2)] = (
                    product[:, tile * 128 : (tile + 1) * 128].astype(BF).reshape(4, 4, 2, 16, 128)
                )

    block_of(tp)
    for swap in swaps:
        swap.wait()
    block_of(1 - tp)

    def fold_copies(which, phase):
        start, count = UNIT_CUTS[which]
        dim = ORDERS[which][phase]
        here = coordinate(dim)
        left_dims = sorted(ORDERS[which][phase:])
        copies = []
        for by in (2, 1, 3):
            index = [slice(None)] * len(left_dims)
            index[left_dims.index(dim)] = (here + by) % SIDE
            units = pl.ds(start, count)
            if phase == 0:
                source = blocks.at[(*index, units)]
                target = got1.at[by - 1, :, :, units]
            elif phase == 1:
                source = sum1.at[(*index, units)]
                target = got2.at[by - 1, :, units]
            else:
                source = sum2.at[(*index, units)]
                target = got3.at[by - 1, units]
            copies.append(
                remote(
                    source,
                    target,
                    fold_send.at[which, phase, by - 1],
                    fold_recv.at[which, phase, by - 1],
                    (peer_of(dim, by), tp),
                )
            )
        return copies

    def folded(which, phase):
        start, count = UNIT_CUTS[which]
        units = pl.ds(start, count)
        dim = ORDERS[which][phase]
        left_dims = sorted(ORDERS[which][phase:])
        index = [slice(None)] * len(left_dims)
        index[left_dims.index(dim)] = coordinate(dim)
        source = (blocks, sum1, sum2)[phase]
        total = source[(*index, units)].astype(F32)
        for by in range(3):
            if phase == 0:
                total = total + got1[by, :, :, units].astype(F32)
            elif phase == 1:
                total = total + got2[by, :, units].astype(F32)
            else:
                total = total + got3[by, units].astype(F32)
        return total

    folds = [[fold_copies(which, phase) for phase in range(3)] for which in range(3)]
    for fold in folds:
        start_all(fold[0])

    mixer_grad = (dot(whole[0], w_out[0:1024, :]) + dot(whole[1], w_out[1024:2048, :])).astype(BF)
    mixer_wide = mixer_grad.astype(F32)
    gate_in_grad_ref[...] = (mixer_wide * conv_sum_ref[...]).astype(BF)
    pad_right[pl.ds(0, 256), :] = mixer_wide * gate_in_ref[...].astype(F32)
    right = remote(
        pad_right.at[pl.ds(0, 8)],
        halo.at[1],
        halo_send.at[1],
        halo_recv.at[1],
        ((sp + 63) % 64, tp),
    )
    right.start()
    for which, fold in enumerate(folds):
        start, count = UNIT_CUTS[which]
        for copy in fold[0]:
            copy.wait_recv()
        sum1[:, :, pl.ds(start, count)] = folded(which, 0).astype(BF)
        start_all(fold[1])
    right.wait()
    pad_right[pl.ds(256, 8), :] = jnp.where(sp == 63, 0.0, halo[1])
    prod_grad = jnp.zeros((256, 512), F32)
    for tap in range(3):
        prod_grad = prod_grad + taps_ref[tap : tap + 1, :] * pad_right[pl.ds(2 - tap, 256), :]
    conv_gate_grad_ref[...] = (prod_grad * conv_value_ref[...].astype(F32)).astype(BF)
    conv_value_grad_ref[...] = (prod_grad * conv_gate_ref[...].astype(F32)).astype(BF)
    for which, fold in enumerate(folds):
        start, count = UNIT_CUTS[which]
        for copy in fold[1]:
            copy.wait_recv()
        sum2[:, pl.ds(start, count)] = folded(which, 1).astype(BF)
        start_all(fold[2])
    for which, fold in enumerate(folds):
        start, count = UNIT_CUTS[which]
        for copy in fold[2]:
            copy.wait_recv()
        total = folded(which, 2)
        for unit in range(count):
            tile, row = divmod(start + unit, 2)
            out_block_ref[pl.ds(row * 16, 16), pl.ds(tile * 128, 128)] = total[unit]
    for chunk in range(2):
        for share in shares[chunk]:
            share.wait_send()
        for stream in (xs[chunk], gs[chunk], backs[chunk]):
            for portion in stream:
                for copies in portion:
                    sent_phase(copies)
    for fold in folds:
        for copies in fold:
            for copy in copies:
                copy.wait_send()
    for copy in saves:
        copy.wait()


def main_call(*operands):
    vmem = pl.BlockSpec(memory_space=pltpu.VMEM)
    hbm = pl.BlockSpec(memory_space=pl.ANY)
    shape = jax.ShapeDtypeStruct
    rows_shape = (4, 4, 4, SLOTS, 1024)
    full_shape = (4, 4, 4, SLOTS, 2048)
    dma = pltpu.SemaphoreType.DMA
    return pl.pallas_call(
        main_kernel,
        out_shape=(
            shape((256, 1024), BF),
            shape((256, 512), BF),
            shape((256, 512), BF),
            shape((256, 512), BF),
            shape((32, 512), F32),
            shape(full_shape, BF),
            shape(full_shape, BF),
            shape((1024, 512), BF),
            shape((1024, 512), BF),
            shape((1024, 512), BF),
        ),
        in_specs=[vmem] * 8 + [hbm] * 4,
        out_specs=(vmem,) * 5 + (hbm,) * 5,
        scratch_shapes=[
            pltpu.VMEM((2, *rows_shape), BF),
            pltpu.VMEM((2, 2, *rows_shape), BF),
            pltpu.VMEM(full_shape, BF),
            pltpu.VMEM(full_shape, BF),
            pltpu.VMEM((2048, 512), BF),
            pltpu.VMEM((2048, 512), BF),
            pltpu.VMEM((512, 2048), BF),
            pltpu.VMEM((2048, 512), BF),
            pltpu.VMEM((1024, 512), F32),
            pltpu.VMEM((1024, 512), F32),
            pltpu.VMEM((1024, 512), BF),
            pltpu.VMEM((1024, 512), BF),
            pltpu.VMEM((1024, 512), BF),
            pltpu.VMEM(rows_shape, BF),
            pltpu.VMEM(rows_shape, BF),
            pltpu.VMEM(rows_shape, BF),
            pltpu.VMEM((3, *rows_shape), BF),
            pltpu.VMEM((256, 1024), F32),
            pltpu.VMEM((1024, 256), BF),
            pltpu.VMEM((2, 256, 1024), BF),
            pltpu.VMEM((4, 4, 4, 8, 16, 128), BF),
            pltpu.VMEM((3, 4, 4, 8, 16, 128), BF),
            pltpu.VMEM((4, 4, 8, 16, 128), BF),
            pltpu.VMEM((3, 4, 8, 16, 128), BF),
            pltpu.VMEM((4, 8, 16, 128), BF),
            pltpu.VMEM((3, 8, 16, 128), BF),
            pltpu.VMEM((264, 512), F32),
            pltpu.VMEM((264, 512), F32),
            pltpu.VMEM((2, 8, 512), F32),
            pltpu.VMEM((256, 512), F32),
            pltpu.VMEM((256, 512), BF),
            dma((4,)),
            dma((5,)),
            dma((18, 3, 3)),
            dma((18, 3, 3)),
            dma((18, 3)),
            dma((21,)),
            dma((21,)),
            dma((2,)),
            dma((2,)),
            dma((3, 3, 3)),
            dma((3, 3, 3)),
        ],
        compiler_params=pltpu.CompilerParams(
            collective_id=0, has_side_effects=True, vmem_limit_bytes=67043328
        ),
    )(*operands)


def shards(
    stream,
    out_grad,
    gate_in,
    conv_gate,
    conv_value,
    taps,
    w_out,
    route_ids,
    route_weights,
    w_gate,
    w_up,
    w_down,
):
    half, gate_in_grad, conv_gate_grad, conv_value_grad, out_block, x, g, hidden, gate, up = main_call(
        route_ids.T,
        route_weights.T,
        stream,
        out_grad,
        gate_in,
        conv_gate,
        conv_value,
        taps,
        w_out,
        w_gate,
        w_up,
        w_down,
    )
    x = x.reshape(1024, 2048)
    g = g.reshape(1024, 2048)
    return (
        half,
        gate_in_grad,
        conv_gate_grad,
        conv_value_grad,
        out_block,
        dot_tn(x, gate)[None],
        dot_tn(x, up)[None],
        dot_tn(hidden, g)[None],
    )


def solution(mesh):
    placed = (
        P("sp", "tp"),
        P("sp", "tp"),
        P("sp", "tp"),
        P("sp", "tp"),
        P("sp", "tp"),
        P(None, "tp"),
        P(None, "tp"),
        P("sp", None),
        P("sp", None),
        P("sp", None, "tp"),
        P("sp", None, "tp"),
        P("sp", "tp", None),
    )
    return jax.shard_map(
        shards,
        mesh=mesh,
        in_specs=placed,
        out_specs=(
            P("sp", "tp"),
            P("sp", "tp"),
            P("sp", "tp"),
            P("sp", "tp"),
            P("sp", "tp"),
            P("sp", None, "tp"),
            P("sp", None, "tp"),
            P("sp", "tp", None),
        ),
        check_vma=False,
    )
```

```python
import functools

import jax
import jax.numpy as jnp
from jax import lax
from jax.experimental import pallas as pl
from jax.experimental.pallas import tpu as pltpu
from jax.sharding import PartitionSpec as P

MESH = pl.DeviceIdType.MESH
BF = jnp.bfloat16
F32 = jnp.float32
SIDE = 4
SLOTS = 16
STRIDE = (16, 4, 1)
ORDERS = ((2, 1, 0), (1, 0, 2), (0, 2, 1))
Z_OFFSETS = (0, 2, 1, 3)
LATE_SHORT = ((0, 384), (384, 384), (768, 256))
EARLY_SHORT = ((0, 256), (256, 384), (640, 384))
MIDDLE_SHORT = ((0, 384), (384, 256), (640, 384))
X_CUTS = (LATE_SHORT, MIDDLE_SHORT)
G_CUTS = (EARLY_SHORT, LATE_SHORT)
BACK_CUTS = (
    MIDDLE_SHORT,
    ((0, 128), (128, 128), (256, 256)),
    ((512, 256), (768, 128), (896, 128)),
)
HALVES = ((0, 512), (512, 512))


def coordinate(dim):
    return (lax.axis_index("sp") // STRIDE[dim]) % SIDE


def peer_of(dim, by):
    here = coordinate(dim)
    return lax.axis_index("sp") + ((here + by) % SIDE - here) * STRIDE[dim]


def piece(spot, index, width):
    ref, start = spot
    return ref.at[(*index, slice(None), pl.ds(start, width))]


def phase_copies(source, target, dim, width, chunk, send_sem, recv_sem, local_sem):
    here = coordinate(dim)
    tp = lax.axis_index("tp")
    moves = []
    if dim == 0:
        every = (slice(None), slice(None))
        if chunk == 0:
            kept = ((0, *every), (0, *every))
            moves.append((2, (1, *every), (1, *every)))
        else:
            kept = None
            moves.append((1, (2, *every), (3, *every)))
            moves.append((3, (3, *every), (2, *every)))
    else:

        def at(place):
            index = [pl.ds(2 * chunk, 2), slice(None), slice(None)]
            index[dim] = place
            return tuple(index)

        kept = (at(here), at(here))
        for by in (2, 1, 3):
            moves.append((by, at((here + by) % SIDE), at(here)))
    sent = [
        pltpu.make_async_remote_copy(
            src_ref=piece(source, from_index, width),
            dst_ref=piece(target, to_index, width),
            send_sem=send_sem.at[by - 1],
            recv_sem=recv_sem.at[by - 1],
            device_id=(peer_of(dim, by), tp),
            device_id_type=MESH,
        )
        for by, from_index, to_index in moves
    ]
    local = []
    if kept is not None:
        local.append(
            pltpu.make_async_copy(
                piece(source, kept[0], width), piece(target, kept[1], width), local_sem
            )
        )
    return sent, local


def start_phase(copies):
    for copy in copies[0] + copies[1]:
        copy.start()


def arrive_phase(copies):
    for copy in copies[0]:
        copy.wait_recv()
    for copy in copies[1]:
        copy.wait()


def sent_phase(copies):
    for copy in copies[0]:
        copy.wait_send()


def start_all(copies):
    for copy in copies:
        copy.start()


def slots_in_lanes(ids):
    tokens = ids.shape[1]
    expert = lax.broadcasted_iota(jnp.int32, (64, tokens), 0)
    first, second = ids[0:1, :], ids[1:2, :]
    named = jnp.where((expert == first) | (expert == second), 1.0, 0.0)
    before = (
        lax.broadcasted_iota(jnp.int32, (tokens, tokens), 0)
        < lax.broadcasted_iota(jnp.int32, (tokens, tokens), 1)
    )
    earlier = jnp.dot(
        named.astype(BF), jnp.where(before, 1.0, 0.0).astype(BF), preferred_element_type=F32
    )
    position = [
        jnp.sum(jnp.where(expert == which, earlier, 0.0), axis=0, keepdims=True).astype(jnp.int32)
        for which in (first, second)
    ]
    return first * SLOTS + position[0], second * SLOTS + position[1]


UNIT_CUTS = ((0, 3), (3, 3), (6, 2))


def greet_all():
    barrier = pltpu.get_barrier_semaphore()
    tp = lax.axis_index("tp")
    sp = lax.axis_index("sp")
    for dim in range(3):
        for by in range(1, SIDE):
            pl.semaphore_signal(
                barrier, inc=1, device_id=(peer_of(dim, by), tp), device_id_type=MESH
            )
    for other in ((sp, 1 - tp), ((sp + 1) % 64, tp), ((sp + 63) % 64, tp)):
        pl.semaphore_signal(barrier, inc=1, device_id=other, device_id_type=MESH)


def all_greeted():
    pl.semaphore_wait(pltpu.get_barrier_semaphore(), 12)


def remote(source, target, send_sem, recv_sem, device):
    return pltpu.make_async_remote_copy(
        src_ref=source,
        dst_ref=target,
        send_sem=send_sem,
        recv_sem=recv_sem,
        device_id=device,
        device_id_type=MESH,
    )


def dot(a, b):
    return jnp.dot(a, b, preferred_element_type=F32)


def dot_tn(a, b):
    return lax.dot_general(a, b, (((0,), (0,)), ((), ())), preferred_element_type=F32)


def dot_nt(a, b):
    return lax.dot_general(a, b, (((1,), (1,)), ((), ())), preferred_element_type=F32)


def main_kernel(
    ids_hbm,
    weights_hbm,
    stream_hbm,
    cot_hbm,
    gate_in_hbm,
    conv_gate_hbm,
    conv_value_hbm,
    taps_hbm,
    w_out_hbm,
    w_gate_hbm,
    w_up_hbm,
    w_down_hbm,
    half_hbm,
    gate_in_grad_hbm,
    conv_gate_grad_hbm,
    conv_value_grad_hbm,
    out_block_hbm,
    gate_w_hbm,
    up_w_hbm,
    down_w_hbm,
    ids_ref,
    weights_ref,
    stream_ref,
    cot_ref,
    gate_in_ref,
    conv_gate_ref,
    conv_value_ref,
    taps_ref,
    send,
    middle,
    full_x,
    full_g,
    wgu,
    wd,
    w_out,
    silu_keep,
    slope_keep,
    hidden,
    both_grad,
    arrived,
    staged,
    back,
    added_ref,
    hot_ref,
    whole,
    blocks,
    got1,
    sum1,
    got2,
    sum2,
    got3,
    pad_left,
    pad_right,
    halo,
    conv_sum_ref,
    mixer_out,
    small,
    out_block_ref,
    input_sems,
    load_sems,
    save_sems,
    small_sems,
    send_sems,
    recv_sems,
    local_sems,
    tp_send,
    tp_recv,
    halo_send,
    halo_recv,
    fold_send,
    fold_recv,
):
    tp = lax.axis_index("tp")
    sp = lax.axis_index("sp")
    partner = (sp, 1 - tp)
    greet_all()
    inputs = [
        pltpu.make_async_copy(source, target, input_sems.at[k])
        for k, (source, target) in enumerate(
            (
                (ids_hbm, ids_ref),
                (weights_hbm, weights_ref),
                (stream_hbm, stream_ref),
                (cot_hbm, cot_ref),
                (gate_in_hbm, gate_in_ref),
                (conv_gate_hbm, conv_gate_ref),
                (conv_value_hbm, conv_value_ref),
                (taps_hbm, taps_ref),
            )
        )
    ]
    start_all(inputs)
    loads = [
        pltpu.make_async_copy(source, target, load_sems.at[k])
        for k, (source, target) in enumerate(
            (
                (w_gate_hbm.at[0], wgu.at[:, pl.ds(0, 512)]),
                (w_up_hbm.at[0], wgu.at[:, pl.ds(512, 512)]),
                (w_down_hbm.at[0], wd),
                (w_out_hbm, w_out),
            )
        )
    ]
    start_all(loads)
    inputs[0].wait()

    slot0, slot1 = slots_in_lanes(ids_ref[...])
    for copy in inputs[1:]:
        copy.wait()
    weight0, weight1 = weights_ref[0:1, :], weights_ref[1:2, :]

    def row_numbers(place):
        z = (coordinate(0) + Z_OFFSETS[place]) % SIDE
        return lax.broadcasted_iota(jnp.int32, (256, 256), 0) + z * 256

    def gather_x(chunk):
        for place in (2 * chunk, 2 * chunk + 1):
            row = row_numbers(place)
            hot = jnp.where((row == slot0) | (row == slot1), 1.0, 0.0).astype(BF)
            hot_ref[pl.ds(place * 256, 256), :] = hot
            send[0, place] = dot(hot, stream_ref[...]).astype(BF).reshape(4, 4, SLOTS, 1024)

    def gather_g(chunk):
        for place in (2 * chunk, 2 * chunk + 1):
            row = row_numbers(place)
            scale = jnp.sum(
                jnp.where(row == slot0, weight0, 0.0) + jnp.where(row == slot1, weight1, 0.0),
                axis=1,
                keepdims=True,
            )
            hot = hot_ref[pl.ds(place * 256, 256), :]
            send[1, place] = (
                (scale * dot(hot, cot_ref[...])).astype(BF).reshape(4, 4, SLOTS, 1024)
            )

    full = (full_x, full_g)
    shared, rows_out = send.at[0], send.at[1]

    def stream_of(number, spots_of, cuts, chunk):
        portions = []
        for which, cut in enumerate(cuts):
            spots = spots_of(cut)
            portions.append(
                [
                    phase_copies(
                        spots[phase],
                        spots[phase + 1],
                        ORDERS[which][phase],
                        cut[1],
                        chunk,
                        send_sems.at[number * 3 + which, phase],
                        recv_sems.at[number * 3 + which, phase],
                        local_sems.at[number * 3 + which, phase],
                    )
                    for phase in range(3)
                ]
            )
        return portions

    def outward(tensor, chunk):
        return stream_of(
            chunk * 2 + tensor,
            lambda cut: (
                (send.at[tensor], cut[0]),
                (middle.at[0, tensor], cut[0]),
                (middle.at[1, tensor], cut[0]),
                (full[tensor], pl.multiple_of(tp * 1024 + cut[0], 128)),
            ),
            (X_CUTS, G_CUTS)[tensor][chunk],
            chunk,
        )

    def homeward(number):
        return stream_of(
            4 + number,
            lambda cut: (
                (rows_out, cut[0]),
                (back.at[0], cut[0]),
                (back.at[1], cut[0]),
                (back.at[2], cut[0]),
            ),
            BACK_CUTS[number],
            min(number, 1),
        )

    xs = [outward(0, chunk) for chunk in range(2)]
    gs = [outward(1, chunk) for chunk in range(2)]
    backs = [homeward(number) for number in range(3)]

    def begin(portions):
        for portion in portions:
            start_phase(portion[0])

    def advance(portions, phase):
        for portion in portions:
            arrive_phase(portion[phase - 1])
            start_phase(portion[phase])

    crossings = {}
    saves = []

    def cross(tensor, chunk):
        crossings[tensor, chunk] = []
        portions = (xs, gs)[tensor][chunk]
        for which, cut in enumerate((X_CUTS, G_CUTS)[tensor][chunk]):
            number = (chunk * 2 + tensor) * 3 + which
            arrive_phase(portions[which][2])
            start = pl.multiple_of(tp * 1024 + cut[0], 128)
            part = full[tensor].at[pl.ds(2 * chunk, 2), :, :, :, pl.ds(start, cut[1])]
            crossing = remote(part, part, tp_send.at[number], tp_recv.at[number], partner)
            crossing.start()
            crossings[tensor, chunk].append(crossing)

    def crossed(tensor, chunk):
        for crossing in crossings[tensor, chunk]:
            crossing.wait()

    def weight_tile(number):
        slot = number % 2
        if number >= 2:
            for copy in saves[number - 2]:
                copy.wait()
        if number < 4:
            at = pl.ds(number * 512, 512)
            columns = full_x[:, :, :, :, at].reshape(1024, 512)
            staged[slot] = dot_tn(columns, both_grad[...]).astype(BF)
            pairs = (
                (staged.at[slot, :, pl.ds(0, 512)], gate_w_hbm.at[at]),
                (staged.at[slot, :, pl.ds(512, 512)], up_w_hbm.at[at]),
            )
        else:
            at = pl.ds((number - 4) * 1024, 1024)
            columns = full_g[:, :, :, :, at].reshape(1024, 1024)
            staged[slot] = dot_tn(hidden[...], columns).astype(BF)
            pairs = ((staged.at[slot], down_w_hbm.at[:, at]),)
        copies = [
            pltpu.make_async_copy(source, target, save_sems.at[number, k])
            for k, (source, target) in enumerate(pairs)
        ]
        start_all(copies)
        saves.append(copies)

    def activate(chunk):
        rows = full_x[pl.ds(chunk * 2, 2)].reshape(512, 2048)
        at = pl.ds(chunk * 512, 512)
        pre_gate = dot(rows, wgu[:, 0:512])
        pre_up = dot(rows, wgu[:, 512:1024])
        sigmoid = jax.nn.sigmoid(pre_gate)
        silu = pre_gate * sigmoid
        silu_keep[at, :] = silu
        slope_keep[at, :] = pre_up * sigmoid * (1.0 + pre_gate * (1.0 - sigmoid))
        hidden[at, :] = (silu * pre_up).astype(BF)

    def differentiate(chunk):
        rows = full_g[pl.ds(chunk * 2, 2)].reshape(512, 2048)
        at = pl.ds(chunk * 512, 512)
        hidden_grad = dot_nt(rows, wd[...])
        both_grad[at, 512:1024] = (hidden_grad * silu_keep[at, :]).astype(BF)
        both_grad[at, 0:512] = (hidden_grad * slope_keep[at, :]).astype(BF)

    def partial_of(side, cut, chunk):
        at = pl.ds(pl.multiple_of(side * 1024 + cut[0], 128), cut[1])
        rows = pl.ds(chunk * 512, 512)
        return dot_nt(both_grad[rows, :], wgu[at, :])

    shares = {}

    def part(chunk, cut):
        return (pl.ds(2 * chunk, 2), slice(None), slice(None), slice(None), pl.ds(*cut))

    def share_theirs(chunk):
        shares[chunk] = []
        for which, cut in enumerate(HALVES):
            index = part(chunk, cut)
            shared[index] = (
                partial_of(1 - tp, cut, chunk).astype(BF).reshape(2, 4, 4, SLOTS, cut[1])
            )
            number = 12 + chunk * 2 + which
            share = remote(
                shared.at[index],
                arrived.at[index],
                tp_send.at[number],
                tp_recv.at[number],
                partner,
            )
            share.start()
            shares[chunk].append(share)

    def add_mine(chunk):
        for which, cut in enumerate(HALVES):
            index = part(chunk, cut)
            mine = partial_of(tp, cut, chunk).astype(BF).astype(F32)
            shares[chunk][which].wait_recv()
            theirs = arrived[index].reshape(512, cut[1]).astype(F32)
            rows_out[index] = (mine + theirs).astype(BF).reshape(2, 4, 4, SLOTS, cut[1])
            if chunk == 1:
                begin(backs[1 + which])

    gather_x(0)
    all_greeted()
    begin(xs[0])
    gather_g(0)
    begin(gs[0])
    gather_x(1)
    begin(xs[1])
    gather_g(1)
    pad_left[pl.ds(8, 256), :] = conv_gate_ref[...].astype(F32) * conv_value_ref[...].astype(F32)
    left = remote(
        pad_left.at[pl.ds(256, 8)],
        halo.at[0],
        halo_send.at[0],
        halo_recv.at[0],
        ((sp + 1) % 64, tp),
    )
    left.start()
    advance(xs[0], 1)
    advance(gs[0], 1)
    begin(gs[1])
    left.wait()
    pad_left[pl.ds(0, 8), :] = jnp.where(sp == 0, 0.0, halo[0])
    conv_sum = jnp.zeros((256, 512), F32)
    for tap in range(3):
        conv_sum = conv_sum + taps_ref[tap : tap + 1, :] * pad_left[pl.ds(6 + tap, 256), :]
    conv_sum_ref[...] = conv_sum
    mixer_out[...] = (gate_in_ref[...].astype(F32) * conv_sum).astype(BF)
    advance(xs[0], 2)
    advance(gs[0], 2)
    advance(xs[1], 1)
    advance(gs[1], 1)
    cross(0, 0)
    for load in loads:
        load.wait()
    crossed(0, 0)
    cross(1, 0)
    advance(xs[1], 2)
    activate(0)
    crossed(1, 0)
    advance(gs[1], 2)
    differentiate(0)
    for stream in (*xs, *gs):
        for portion in stream:
            sent_phase(portion[0])
    share_theirs(0)
    add_mine(0)
    begin(backs[0])
    cross(0, 1)
    crossed(0, 1)
    activate(1)
    cross(1, 1)
    advance(backs[0], 1)
    crossed(1, 1)
    differentiate(1)
    share_theirs(1)
    add_mine(1)
    advance(backs[0], 2)
    weight_tile(0)
    for portion in backs[0]:
        arrive_phase(portion[2])
    added_ref[...] = dot_tn(
        hot_ref[pl.ds(0, 512), :], back[2, pl.ds(0, 2)].reshape(512, 1024)
    ) + cot_ref[...].astype(F32)
    advance(backs[1], 1)
    weight_tile(1)
    advance(backs[2], 1)
    weight_tile(2)
    advance(backs[1], 2)
    weight_tile(3)
    advance(backs[2], 2)
    weight_tile(4)
    swaps = []

    def combine(which):
        for portion in backs[1 + which]:
            arrive_phase(portion[2])
        columns = pl.ds(*HALVES[which])
        rows = back[2, pl.ds(2, 2), :, :, :, columns].reshape(512, 512)
        total = added_ref[:, columns] + dot_tn(hot_ref[pl.ds(512, 512), :], rows)
        whole[tp, :, columns] = total.astype(BF)
        swap = remote(
            whole.at[tp, :, columns],
            whole.at[tp, :, columns],
            tp_send.at[16 + which],
            tp_recv.at[16 + which],
            partner,
        )
        swap.start()
        swaps.append(swap)

    combine(0)
    combine(1)

    def block_of(half):
        for part in range(2):
            product = dot_tn(whole[half, :, pl.ds(part * 512, 512)], mixer_out[...])
            for tile in range(4):
                blocks[half * 2 + part, :, :, pl.ds(tile * 2, 2)] = (
                    product[:, tile * 128 : (tile + 1) * 128].astype(BF).reshape(4, 4, 2, 16, 128)
                )

    def fold_copies(which, phase, half=None, late=0):
        start, count = UNIT_CUTS[which]
        dim = ORDERS[which][phase]
        here = coordinate(dim)
        left_dims = sorted(ORDERS[which][phase:])
        copies = []
        for by in (2, 1, 3):
            index = [slice(None)] * len(left_dims)
            index[left_dims.index(dim)] = (here + by) % SIDE
            kept = slice(None)
            if half is not None:
                kept = pl.ds(2 * half, 2)
                index[0] = kept
            units = pl.ds(start, count)
            if phase == 0:
                source = blocks.at[(*index, units)]
                target = got1.at[by - 1, kept, :, units]
            elif phase == 1:
                source = sum1.at[(*index, units)]
                target = got2.at[by - 1, :, units]
            else:
                source = sum2.at[(*index, units)]
                target = got3.at[by - 1, units]
            copies.append(
                remote(
                    source,
                    target,
                    fold_send.at[which, phase + 3 * late, by - 1],
                    fold_recv.at[which, phase + 3 * late, by - 1],
                    (peer_of(dim, by), tp),
                )
            )
        return copies

    def folded(which, phase):
        start, count = UNIT_CUTS[which]
        units = pl.ds(start, count)
        dim = ORDERS[which][phase]
        left_dims = sorted(ORDERS[which][phase:])
        index = [slice(None)] * len(left_dims)
        index[left_dims.index(dim)] = coordinate(dim)
        source = (blocks, sum1, sum2)[phase]
        total = source[(*index, units)].astype(F32)
        for by in range(3):
            if phase == 0:
                total = total + got1[by, :, :, units].astype(F32)
            elif phase == 1:
                total = total + got2[by, :, units].astype(F32)
            else:
                total = total + got3[by, units].astype(F32)
        return total

    folds = [[[], fold_copies(which, 1), fold_copies(which, 2)] for which in range(3)]

    def fold_first(which, half, late):
        copies = fold_copies(which, 0, half, late)
        start_all(copies)
        folds[which][0] += copies

    block_of(tp)
    fold_first(0, tp, 0)
    fold_first(1, tp, 0)
    for swap in swaps:
        swap.wait()
    block_of(1 - tp)
    fold_first(2, None, 0)
    fold_first(0, 1 - tp, 1)
    fold_first(1, 1 - tp, 1)
    results = []

    def deliver(source, target):
        copy = pltpu.make_async_copy(source, target, small_sems.at[len(results)])
        copy.start()
        results.append(copy)

    deliver(whole.at[tp], half_hbm)

    mixer_grad = (dot(whole[0], w_out[0:1024, :]) + dot(whole[1], w_out[1024:2048, :])).astype(BF)
    mixer_wide = mixer_grad.astype(F32)
    small[0] = (mixer_wide * conv_sum_ref[...]).astype(BF)
    pad_right[pl.ds(0, 256), :] = mixer_wide * gate_in_ref[...].astype(F32)
    right = remote(
        pad_right.at[pl.ds(0, 8)],
        halo.at[1],
        halo_send.at[1],
        halo_recv.at[1],
        ((sp + 63) % 64, tp),
    )
    right.start()
    deliver(small.at[0], gate_in_grad_hbm)
    weight_tile(5)
    for which, fold in enumerate(folds):
        start, count = UNIT_CUTS[which]
        for copy in fold[0]:
            copy.wait_recv()
        sum1[:, :, pl.ds(start, count)] = folded(which, 0).astype(BF)
        start_all(fold[1])
    right.wait()
    pad_right[pl.ds(256, 8), :] = jnp.where(sp == 63, 0.0, halo[1])
    prod_grad = jnp.zeros((256, 512), F32)
    for tap in range(3):
        prod_grad = prod_grad + taps_ref[tap : tap + 1, :] * pad_right[pl.ds(2 - tap, 256), :]
    small[1] = (prod_grad * conv_value_ref[...].astype(F32)).astype(BF)
    small[2] = (prod_grad * conv_gate_ref[...].astype(F32)).astype(BF)
    deliver(small.at[1], conv_gate_grad_hbm)
    deliver(small.at[2], conv_value_grad_hbm)
    for which, fold in enumerate(folds):
        start, count = UNIT_CUTS[which]
        for copy in fold[1]:
            copy.wait_recv()
        sum2[:, pl.ds(start, count)] = folded(which, 1).astype(BF)
        start_all(fold[2])
    for which, fold in enumerate(folds):
        start, count = UNIT_CUTS[which]
        for copy in fold[2]:
            copy.wait_recv()
        total = folded(which, 2)
        for unit in range(count):
            tile, row = divmod(start + unit, 2)
            out_block_ref[pl.ds(row * 16, 16), pl.ds(tile * 128, 128)] = total[unit]
    deliver(out_block_ref, out_block_hbm)
    for chunk in range(2):
        for share in shares[chunk]:
            share.wait_send()
        for stream in (xs[chunk], gs[chunk]):
            for portion in stream:
                for copies in portion[1:]:
                    sent_phase(copies)
    for stream in backs:
        for portion in stream:
            for copies in portion:
                sent_phase(copies)
    for fold in folds:
        for copies in fold:
            for copy in copies:
                copy.wait_send()
    for copy in results:
        copy.wait()
    for copies in saves[4:]:
        for copy in copies:
            copy.wait()


def main_call(*operands):
    hbm = pl.BlockSpec(memory_space=pl.ANY)
    shape = jax.ShapeDtypeStruct
    rows_shape = (4, 4, 4, SLOTS, 1024)
    full_shape = (4, 4, 4, SLOTS, 2048)
    dma = pltpu.SemaphoreType.DMA
    return pl.pallas_call(
        main_kernel,
        out_shape=(
            shape((256, 1024), BF),
            shape((256, 512), BF),
            shape((256, 512), BF),
            shape((256, 512), BF),
            shape((32, 512), F32),
            shape((2048, 512), BF),
            shape((2048, 512), BF),
            shape((512, 2048), BF),
        ),
        in_specs=[hbm] * 12,
        out_specs=(hbm,) * 8,
        scratch_shapes=[
            pltpu.VMEM((2, 256), jnp.int32),
            pltpu.VMEM((2, 256), F32),
            pltpu.VMEM((256, 1024), BF),
            pltpu.VMEM((256, 1024), BF),
            pltpu.VMEM((256, 512), BF),
            pltpu.VMEM((256, 512), BF),
            pltpu.VMEM((256, 512), BF),
            pltpu.VMEM((3, 512), F32),
            pltpu.VMEM((2, *rows_shape), BF),
            pltpu.VMEM((2, 2, *rows_shape), BF),
            pltpu.VMEM(full_shape, BF),
            pltpu.VMEM(full_shape, BF),
            pltpu.VMEM((2048, 1024), BF),
            pltpu.VMEM((512, 2048), BF),
            pltpu.VMEM((2048, 512), BF),
            pltpu.VMEM((1024, 512), F32),
            pltpu.VMEM((1024, 512), F32),
            pltpu.VMEM((1024, 512), BF),
            pltpu.VMEM((1024, 1024), BF),
            pltpu.VMEM(rows_shape, BF),
            pltpu.VMEM((2, 512, 1024), BF),
            pltpu.VMEM((3, *rows_shape), BF),
            pltpu.VMEM((256, 1024), F32),
            pltpu.VMEM((1024, 256), BF),
            pltpu.VMEM((2, 256, 1024), BF),
            pltpu.VMEM((4, 4, 4, 8, 16, 128), BF),
            pltpu.VMEM((3, 4, 4, 8, 16, 128), BF),
            pltpu.VMEM((4, 4, 8, 16, 128), BF),
            pltpu.VMEM((3, 4, 8, 16, 128), BF),
            pltpu.VMEM((4, 8, 16, 128), BF),
            pltpu.VMEM((3, 8, 16, 128), BF),
            pltpu.VMEM((264, 512), F32),
            pltpu.VMEM((264, 512), F32),
            pltpu.VMEM((2, 8, 512), F32),
            pltpu.VMEM((256, 512), F32),
            pltpu.VMEM((256, 512), BF),
            pltpu.VMEM((3, 256, 512), BF),
            pltpu.VMEM((32, 512), F32),
            dma((8,)),
            dma((4,)),
            dma((6, 2)),
            dma((5,)),
            dma((21, 3, 3)),
            dma((21, 3, 3)),
            dma((21, 3)),
            dma((18,)),
            dma((18,)),
            dma((2,)),
            dma((2,)),
            dma((3, 4, 3)),
            dma((3, 4, 3)),
        ],
        compiler_params=pltpu.CompilerParams(
            collective_id=0, has_side_effects=True, vmem_limit_bytes=67043328
        ),
    )(*operands)


def finish_kernel(*refs):
    sources, targets = refs[:8], refs[8:16]
    passing, held, narrow, wide, in_sems, out_sems, big_in, big_out = (
        refs[16:20],
        refs[20],
        refs[21:24],
        refs[24:27],
        *refs[27:31],
    )
    passing = (*passing, held)

    def rows_of(which, step):
        rows = narrow[which].shape[1]
        return pl.ds(pl.multiple_of(step * rows, rows), rows)

    def taken(which, step):
        return pltpu.make_async_copy(
            sources[5 + which].at[rows_of(which, step)],
            narrow[which].at[step],
            big_in.at[which, step],
        )

    def given(which, step):
        return pltpu.make_async_copy(
            wide[which].at[step],
            targets[5 + which].at[0, rows_of(which, step)],
            big_out.at[which, step],
        )

    ins = [
        pltpu.make_async_copy(sources[k], passing[k], in_sems.at[k]) for k in range(5)
    ]
    outs = [
        pltpu.make_async_copy(passing[k], targets[k], out_sems.at[k]) for k in range(5)
    ]
    for step in range(4):
        for which in range(3):
            taken(which, step).start()
    start_all(ins)

    def widen(step, carry):
        for which in range(3):
            taken(which, step).wait()
            wide[which][step] = narrow[which][step].astype(F32)
            given(which, step).start()
        return carry

    lax.fori_loop(0, 4, widen, 0)
    for k in range(5):
        ins[k].wait()
        outs[k].start()
    for step in range(4):
        for which in range(3):
            given(which, step).wait()
    for copy in outs:
        copy.wait()


def finished(produced):
    hbm = pl.BlockSpec(memory_space=pl.ANY)
    dma = pltpu.SemaphoreType.DMA
    shape = jax.ShapeDtypeStruct
    tiles = ((4, 512, 512), (4, 512, 512), (4, 128, 2048))
    return pl.pallas_call(
        finish_kernel,
        out_shape=tuple(shape(array.shape, array.dtype) for array in produced[:5])
        + tuple(shape((1, *array.shape), F32) for array in produced[5:]),
        in_specs=[hbm] * 8,
        out_specs=(hbm,) * 8,
        scratch_shapes=[pltpu.VMEM(array.shape, array.dtype) for array in produced[:5]]
        + [pltpu.VMEM(tile, BF) for tile in tiles]
        + [pltpu.VMEM(tile, F32) for tile in tiles]
        + [dma((5,)), dma((5,)), dma((3, 4)), dma((3, 4))],
        compiler_params=pltpu.CompilerParams(vmem_limit_bytes=67043328),
    )(*produced)


def shards(
    stream,
    out_grad,
    gate_in,
    conv_gate,
    conv_value,
    taps,
    w_out,
    route_ids,
    route_weights,
    w_gate,
    w_up,
    w_down,
):
    produced = main_call(
        route_ids.T,
        route_weights.T,
        stream,
        out_grad,
        gate_in,
        conv_gate,
        conv_value,
        taps,
        w_out,
        w_gate,
        w_up,
        w_down,
    )
    return finished(produced)


def solution(mesh):
    placed = (
        P("sp", "tp"),
        P("sp", "tp"),
        P("sp", "tp"),
        P("sp", "tp"),
        P("sp", "tp"),
        P(None, "tp"),
        P(None, "tp"),
        P("sp", None),
        P("sp", None),
        P("sp", None, "tp"),
        P("sp", None, "tp"),
        P("sp", "tp", None),
    )
    return jax.shard_map(
        shards,
        mesh=mesh,
        in_specs=placed,
        out_specs=(
            P("sp", "tp"),
            P("sp", "tp"),
            P("sp", "tp"),
            P("sp", "tp"),
            P("sp", "tp"),
            P("sp", None, "tp"),
            P("sp", None, "tp"),
            P("sp", "tp", None),
        ),
        check_vma=False,
    )
```

```python
import functools

import jax
import jax.numpy as jnp
from jax import lax
from jax.experimental import pallas as pl
from jax.experimental.pallas import tpu as pltpu
from jax.sharding import PartitionSpec as P

MESH = pl.DeviceIdType.MESH
BF = jnp.bfloat16
F32 = jnp.float32
SIDE = 4
SLOTS = 16
STRIDE = (16, 4, 1)
ORDERS = ((2, 1, 0), (1, 0, 2), (0, 2, 1))
Z_OFFSETS = (0, 2, 1, 3)
LATE_SHORT = ((0, 384), (384, 384), (768, 256))
EARLY_SHORT = ((0, 256), (256, 384), (640, 384))
MIDDLE_SHORT = ((0, 384), (384, 256), (640, 384))
X_CUTS = (LATE_SHORT, MIDDLE_SHORT)
G_CUTS = (EARLY_SHORT, LATE_SHORT)
BACK_CUTS = (
    MIDDLE_SHORT,
    ((0, 128), (128, 128), (256, 256)),
    ((512, 256), (768, 128), (896, 128)),
)
HALVES = ((0, 512), (512, 512))


def coordinate(dim):
    return (lax.axis_index("sp") // STRIDE[dim]) % SIDE


def peer_of(dim, by):
    here = coordinate(dim)
    return lax.axis_index("sp") + ((here + by) % SIDE - here) * STRIDE[dim]


def piece(spot, index, width):
    ref, start = spot
    return ref.at[(*index, slice(None), pl.ds(start, width))]


class Phase:
    def __init__(self, source, target, dim, width, chunk, send_sem, recv_sem):
        here = coordinate(dim)
        tp = lax.axis_index("tp")
        every = (slice(None), slice(None))
        both = pl.ds(2 * chunk, 2)
        moves = []
        if dim == 0:
            kept = None
            if chunk == 0:
                kept = (0, *every)
                moves.append((2, (1, *every), (1, *every)))
                gone = (1, *every)
            else:
                moves.append((1, (2, *every), (3, *every)))
                moves.append((3, (3, *every), (2, *every)))
                gone = (both, *every)
        else:

            def at(place):
                index = [both, slice(None), slice(None)]
                index[dim] = place
                return tuple(index)

            kept = at(here)
            for by in (2, 1, 3):
                moves.append((by, at((here + by) % SIDE), at(here)))
            gone = at(pl.ds(0, 3))
        self.copies = [
            pltpu.make_async_remote_copy(
                src_ref=piece(source, from_index, width),
                dst_ref=piece(target, to_index, width),
                send_sem=send_sem,
                recv_sem=recv_sem,
                device_id=(peer_of(dim, by), tp),
                device_id_type=MESH,
            )
            for by, from_index, to_index in moves
        ]
        if kept is not None:
            self.copies.append(
                pltpu.make_async_copy(
                    piece(source, kept, width), piece(target, kept, width), recv_sem
                )
            )
        filled = piece(target, (both, *every), width)
        self.filled = pltpu.make_async_copy(filled, filled, recv_sem)
        left = piece(source, gone, width)
        self.left = pltpu.make_async_copy(left, left, send_sem)


def start_phase(phase):
    start_all(phase.copies)


def arrive_phase(phase):
    phase.filled.wait()


def sent_phase(phase):
    phase.left.wait()


def start_all(copies):
    for copy in copies:
        copy.start()


def slots_in_lanes(ids):
    tokens = ids.shape[1]
    expert = lax.broadcasted_iota(jnp.int32, (64, tokens), 0)
    first, second = ids[0:1, :], ids[1:2, :]
    named = jnp.where((expert == first) | (expert == second), 1.0, 0.0)
    before = (
        lax.broadcasted_iota(jnp.int32, (tokens, tokens), 0)
        < lax.broadcasted_iota(jnp.int32, (tokens, tokens), 1)
    )
    earlier = jnp.dot(
        named.astype(BF), jnp.where(before, 1.0, 0.0).astype(BF), preferred_element_type=F32
    )
    position = [
        jnp.sum(jnp.where(expert == which, earlier, 0.0), axis=0, keepdims=True).astype(jnp.int32)
        for which in (first, second)
    ]
    return first * SLOTS + position[0], second * SLOTS + position[1]


UNIT_CUTS = ((0, 3), (3, 3), (6, 2))


def greet_all():
    barrier = pltpu.get_barrier_semaphore()
    tp = lax.axis_index("tp")
    sp = lax.axis_index("sp")
    for dim in range(3):
        for by in range(1, SIDE):
            pl.semaphore_signal(
                barrier, inc=1, device_id=(peer_of(dim, by), tp), device_id_type=MESH
            )
    for other in ((sp, 1 - tp), ((sp + 1) % 64, tp), ((sp + 63) % 64, tp)):
        pl.semaphore_signal(barrier, inc=1, device_id=other, device_id_type=MESH)


def all_greeted():
    pl.semaphore_wait(pltpu.get_barrier_semaphore(), 12)


def remote(source, target, send_sem, recv_sem, device):
    return pltpu.make_async_remote_copy(
        src_ref=source,
        dst_ref=target,
        send_sem=send_sem,
        recv_sem=recv_sem,
        device_id=device,
        device_id_type=MESH,
    )


def dot(a, b):
    return jnp.dot(a, b, preferred_element_type=F32)


def dot_tn(a, b):
    return lax.dot_general(a, b, (((0,), (0,)), ((), ())), preferred_element_type=F32)


def dot_nt(a, b):
    return lax.dot_general(a, b, (((1,), (1,)), ((), ())), preferred_element_type=F32)


def main_kernel(
    ids_hbm,
    weights_hbm,
    stream_hbm,
    cot_hbm,
    gate_in_hbm,
    conv_gate_hbm,
    conv_value_hbm,
    taps_hbm,
    w_out_hbm,
    w_gate_hbm,
    w_up_hbm,
    w_down_hbm,
    half_hbm,
    gate_in_grad_hbm,
    conv_gate_grad_hbm,
    conv_value_grad_hbm,
    out_block_hbm,
    gate_w_hbm,
    up_w_hbm,
    down_w_hbm,
    ids_ref,
    weights_ref,
    stream_ref,
    cot_ref,
    gate_in_ref,
    conv_gate_ref,
    conv_value_ref,
    taps_ref,
    send,
    middle,
    full_x,
    full_g,
    wgu,
    wd,
    w_out,
    silu_keep,
    slope_keep,
    hidden,
    both_grad,
    arrived,
    staged,
    back,
    added_ref,
    hot_ref,
    whole,
    blocks,
    got1,
    sum1,
    got2,
    sum2,
    got3,
    pad_left,
    pad_right,
    halo,
    conv_sum_ref,
    mixer_out,
    small,
    out_block_ref,
    input_sems,
    load_sems,
    save_sems,
    small_sems,
    send_sems,
    recv_sems,
    tp_send,
    tp_recv,
    halo_send,
    halo_recv,
    fold_send,
    fold_recv,
):
    tp = lax.axis_index("tp")
    sp = lax.axis_index("sp")
    partner = (sp, 1 - tp)
    greet_all()
    inputs = [
        pltpu.make_async_copy(source, target, input_sems.at[k])
        for k, (source, target) in enumerate(
            (
                (ids_hbm, ids_ref),
                (weights_hbm, weights_ref),
                (stream_hbm, stream_ref),
                (cot_hbm, cot_ref),
                (gate_in_hbm, gate_in_ref),
                (conv_gate_hbm, conv_gate_ref),
                (conv_value_hbm, conv_value_ref),
                (taps_hbm, taps_ref),
            )
        )
    ]
    start_all(inputs)
    loads = [
        pltpu.make_async_copy(source, target, load_sems.at[k])
        for k, (source, target) in enumerate(
            (
                (w_gate_hbm.at[0], wgu.at[:, pl.ds(0, 512)]),
                (w_up_hbm.at[0], wgu.at[:, pl.ds(512, 512)]),
                (w_down_hbm.at[0], wd),
                (w_out_hbm, w_out),
            )
        )
    ]
    start_all(loads)
    inputs[0].wait()

    slot0, slot1 = slots_in_lanes(ids_ref[...])
    for copy in inputs[1:]:
        copy.wait()
    weight0, weight1 = weights_ref[0:1, :], weights_ref[1:2, :]

    def row_numbers(place):
        z = (coordinate(0) + Z_OFFSETS[place]) % SIDE
        return lax.broadcasted_iota(jnp.int32, (256, 256), 0) + z * 256

    def gather_x(chunk):
        for place in (2 * chunk, 2 * chunk + 1):
            row = row_numbers(place)
            hot = jnp.where((row == slot0) | (row == slot1), 1.0, 0.0).astype(BF)
            hot_ref[pl.ds(place * 256, 256), :] = hot
            send[0, place] = dot(hot, stream_ref[...]).astype(BF).reshape(4, 4, SLOTS, 1024)

    def gather_g(chunk):
        for place in (2 * chunk, 2 * chunk + 1):
            row = row_numbers(place)
            scale = jnp.sum(
                jnp.where(row == slot0, weight0, 0.0) + jnp.where(row == slot1, weight1, 0.0),
                axis=1,
                keepdims=True,
            )
            hot = hot_ref[pl.ds(place * 256, 256), :]
            send[1, place] = (
                (scale * dot(hot, cot_ref[...])).astype(BF).reshape(4, 4, SLOTS, 1024)
            )

    full = (full_x, full_g)
    shared, rows_out = send.at[0], send.at[1]

    def stream_of(number, spots_of, cuts, chunk):
        portions = []
        for which, cut in enumerate(cuts):
            spots = spots_of(cut)
            portions.append(
                [
                    Phase(
                        spots[phase],
                        spots[phase + 1],
                        ORDERS[which][phase],
                        cut[1],
                        chunk,
                        send_sems.at[number * 3 + which, phase],
                        recv_sems.at[number * 3 + which, phase],
                    )
                    for phase in range(3)
                ]
            )
        return portions

    def outward(tensor, chunk):
        return stream_of(
            chunk * 2 + tensor,
            lambda cut: (
                (send.at[tensor], cut[0]),
                (middle.at[0, tensor], cut[0]),
                (middle.at[1, tensor], cut[0]),
                (full[tensor], pl.multiple_of(tp * 1024 + cut[0], 128)),
            ),
            (X_CUTS, G_CUTS)[tensor][chunk],
            chunk,
        )

    def homeward(number):
        return stream_of(
            4 + number,
            lambda cut: (
                (rows_out, cut[0]),
                (back.at[0], cut[0]),
                (back.at[1], cut[0]),
                (back.at[2], cut[0]),
            ),
            BACK_CUTS[number],
            min(number, 1),
        )

    xs = [outward(0, chunk) for chunk in range(2)]
    gs = [outward(1, chunk) for chunk in range(2)]
    backs = [homeward(number) for number in range(3)]

    def begin(portions):
        for portion in portions:
            start_phase(portion[0])

    def advance(portions, phase):
        for portion in portions:
            arrive_phase(portion[phase - 1])
            start_phase(portion[phase])

    saves = []

    def half_of(tensor, chunk, cut):
        start = pl.multiple_of(tp * 1024 + cut[0], 128)
        return full[tensor].at[pl.ds(2 * chunk, 2), :, :, :, pl.ds(start, cut[1])]

    def crossing(tensor, chunk, cut):
        part = half_of(tensor, chunk, cut)
        number = chunk * 2 + tensor
        return remote(part, part, tp_send.at[number], tp_recv.at[number], partner)

    def cross(tensor, chunk):
        portions = (xs, gs)[tensor][chunk]
        for which, cut in enumerate((X_CUTS, G_CUTS)[tensor][chunk]):
            arrive_phase(portions[which][2])
            crossing(tensor, chunk, cut).start()

    def crossed(tensor, chunk):
        crossing(tensor, chunk, (0, 1024)).wait()

    def weight_tile(number):
        slot = number % 2
        if number >= 2:
            for copy in saves[number - 2]:
                copy.wait()
        if number < 4:
            at = pl.ds(number * 512, 512)
            columns = full_x[:, :, :, :, at].reshape(1024, 512)
            staged[slot] = dot_tn(columns, both_grad[...]).astype(BF)
            pairs = (
                (staged.at[slot, :, pl.ds(0, 512)], gate_w_hbm.at[at]),
                (staged.at[slot, :, pl.ds(512, 512)], up_w_hbm.at[at]),
            )
        else:
            at = pl.ds((number - 4) * 1024, 1024)
            columns = full_g[:, :, :, :, at].reshape(1024, 1024)
            staged[slot] = dot_tn(hidden[...], columns).astype(BF)
            pairs = ((staged.at[slot], down_w_hbm.at[:, at]),)
        copies = [
            pltpu.make_async_copy(source, target, save_sems.at[number, k])
            for k, (source, target) in enumerate(pairs)
        ]
        start_all(copies)
        saves.append(copies)

    def activate(chunk):
        rows = full_x[pl.ds(chunk * 2, 2)].reshape(512, 2048)
        at = pl.ds(chunk * 512, 512)
        pre_gate = dot(rows, wgu[:, 0:512])
        pre_up = dot(rows, wgu[:, 512:1024])
        sigmoid = jax.nn.sigmoid(pre_gate)
        silu = pre_gate * sigmoid
        silu_keep[at, :] = silu
        slope_keep[at, :] = pre_up * sigmoid * (1.0 + pre_gate * (1.0 - sigmoid))
        hidden[at, :] = (silu * pre_up).astype(BF)

    def differentiate(chunk):
        rows = full_g[pl.ds(chunk * 2, 2)].reshape(512, 2048)
        at = pl.ds(chunk * 512, 512)
        hidden_grad = dot_nt(rows, wd[...])
        both_grad[at, 512:1024] = (hidden_grad * silu_keep[at, :]).astype(BF)
        both_grad[at, 0:512] = (hidden_grad * slope_keep[at, :]).astype(BF)

    def partial_of(side, cut, chunk):
        at = pl.ds(pl.multiple_of(side * 1024 + cut[0], 128), cut[1])
        rows = pl.ds(chunk * 512, 512)
        return dot_nt(both_grad[rows, :], wgu[at, :])

    shares = {}

    def part(chunk, cut):
        return (pl.ds(2 * chunk, 2), slice(None), slice(None), slice(None), pl.ds(*cut))

    def share_theirs(chunk):
        shares[chunk] = []
        for which, cut in enumerate(HALVES):
            index = part(chunk, cut)
            shared[index] = (
                partial_of(1 - tp, cut, chunk).astype(BF).reshape(2, 4, 4, SLOTS, cut[1])
            )
            number = 4 + chunk * 2 + which
            share = remote(
                shared.at[index],
                arrived.at[index],
                tp_send.at[number],
                tp_recv.at[number],
                partner,
            )
            share.start()
            shares[chunk].append(share)

    def add_mine(chunk):
        for which, cut in enumerate(HALVES):
            index = part(chunk, cut)
            mine = partial_of(tp, cut, chunk).astype(BF).astype(F32)
            shares[chunk][which].wait_recv()
            theirs = arrived[index].reshape(512, cut[1]).astype(F32)
            rows_out[index] = (mine + theirs).astype(BF).reshape(2, 4, 4, SLOTS, cut[1])
            if chunk == 1:
                begin(backs[1 + which])

    gather_x(0)
    all_greeted()
    begin(xs[0])
    gather_g(0)
    begin(gs[0])
    gather_x(1)
    begin(xs[1])
    gather_g(1)
    pad_left[pl.ds(8, 256), :] = conv_gate_ref[...].astype(F32) * conv_value_ref[...].astype(F32)
    left = remote(
        pad_left.at[pl.ds(256, 8)],
        halo.at[0],
        halo_send.at[0],
        halo_recv.at[0],
        ((sp + 1) % 64, tp),
    )
    left.start()
    advance(xs[0], 1)
    advance(gs[0], 1)
    begin(gs[1])
    left.wait()
    pad_left[pl.ds(0, 8), :] = jnp.where(sp == 0, 0.0, halo[0])
    conv_sum = jnp.zeros((256, 512), F32)
    for tap in range(3):
        conv_sum = conv_sum + taps_ref[tap : tap + 1, :] * pad_left[pl.ds(6 + tap, 256), :]
    conv_sum_ref[...] = conv_sum
    mixer_out[...] = (gate_in_ref[...].astype(F32) * conv_sum).astype(BF)
    advance(xs[0], 2)
    advance(gs[0], 2)
    advance(xs[1], 1)
    advance(gs[1], 1)
    cross(0, 0)
    for load in loads:
        load.wait()
    crossed(0, 0)
    cross(1, 0)
    advance(xs[1], 2)
    activate(0)
    crossed(1, 0)
    advance(gs[1], 2)
    differentiate(0)
    for stream in (*xs, *gs):
        for portion in stream:
            sent_phase(portion[0])
    share_theirs(0)
    add_mine(0)
    begin(backs[0])
    cross(0, 1)
    crossed(0, 1)
    cross(1, 1)
    activate(1)
    crossed(1, 1)
    differentiate(1)
    advance(backs[0], 1)
    share_theirs(1)
    add_mine(1)
    advance(backs[0], 2)
    weight_tile(0)
    advance(backs[1], 1)
    weight_tile(1)
    advance(backs[2], 1)
    for portion in backs[0]:
        arrive_phase(portion[2])
    added_ref[...] = dot_tn(
        hot_ref[pl.ds(0, 512), :], back[2, pl.ds(0, 2)].reshape(512, 1024)
    ) + cot_ref[...].astype(F32)
    weight_tile(2)
    advance(backs[1], 2)
    weight_tile(3)
    advance(backs[2], 2)
    weight_tile(4)
    swaps = []

    def combine(which):
        for portion in backs[1 + which]:
            arrive_phase(portion[2])
        columns = pl.ds(*HALVES[which])
        rows = back[2, pl.ds(2, 2), :, :, :, columns].reshape(512, 512)
        total = added_ref[:, columns] + dot_tn(hot_ref[pl.ds(512, 512), :], rows)
        whole[tp, :, columns] = total.astype(BF)
        swap = remote(
            whole.at[tp, :, columns],
            whole.at[tp, :, columns],
            tp_send.at[8 + which],
            tp_recv.at[8 + which],
            partner,
        )
        swap.start()
        swaps.append(swap)

    combine(0)
    combine(1)

    def block_of(half):
        for part in range(2):
            product = dot_tn(whole[half, :, pl.ds(part * 512, 512)], mixer_out[...])
            for tile in range(4):
                blocks[half * 2 + part, :, :, pl.ds(tile * 2, 2)] = (
                    product[:, tile * 128 : (tile + 1) * 128].astype(BF).reshape(4, 4, 2, 16, 128)
                )

    def fold_copies(which, phase, half=None, late=0):
        start, count = UNIT_CUTS[which]
        dim = ORDERS[which][phase]
        here = coordinate(dim)
        left_dims = sorted(ORDERS[which][phase:])
        copies = []
        for by in (2, 1, 3):
            index = [slice(None)] * len(left_dims)
            index[left_dims.index(dim)] = (here + by) % SIDE
            kept = slice(None)
            if half is not None:
                kept = pl.ds(2 * half, 2)
                index[0] = kept
            units = pl.ds(start, count)
            if phase == 0:
                source = blocks.at[(*index, units)]
                target = got1.at[by - 1, kept, :, units]
            elif phase == 1:
                source = sum1.at[(*index, units)]
                target = got2.at[by - 1, :, units]
            else:
                source = sum2.at[(*index, units)]
                target = got3.at[by - 1, units]
            copies.append(
                remote(
                    source,
                    target,
                    fold_send.at[which, phase + 3 * late],
                    fold_recv.at[which, phase + 3 * late],
                    (peer_of(dim, by), tp),
                )
            )
        index = [slice(None)] * len(left_dims)
        index[left_dims.index(dim)] = pl.ds(0, 3)
        kept = slice(None)
        if half is not None:
            kept = pl.ds(2 * half, 2)
            index[0] = kept
        if phase == 0:
            source, target = blocks.at[(*index, units)], got1.at[:, kept, :, units]
        elif phase == 1:
            source, target = sum1.at[(*index, units)], got2.at[:, :, units]
        else:
            source, target = sum2.at[(*index, units)], got3.at[:, units]
        ended = (
            pltpu.make_async_copy(target, target, fold_recv.at[which, phase + 3 * late]),
            pltpu.make_async_copy(source, source, fold_send.at[which, phase + 3 * late]),
        )
        return copies, ended

    def folded(which, phase):
        start, count = UNIT_CUTS[which]
        units = pl.ds(start, count)
        dim = ORDERS[which][phase]
        left_dims = sorted(ORDERS[which][phase:])
        index = [slice(None)] * len(left_dims)
        index[left_dims.index(dim)] = coordinate(dim)
        source = (blocks, sum1, sum2)[phase]
        total = source[(*index, units)].astype(F32)
        for by in range(3):
            if phase == 0:
                total = total + got1[by, :, :, units].astype(F32)
            elif phase == 1:
                total = total + got2[by, :, units].astype(F32)
            else:
                total = total + got3[by, units].astype(F32)
        return total

    folds = [[[], [], []] for which in range(3)]

    def fold_first(which, half, late):
        copies, ended = fold_copies(which, 0, half, late)
        start_all(copies)
        folds[which][0].append(ended)

    def fold_next(which, phase):
        copies, ended = fold_copies(which, phase)
        start_all(copies)
        folds[which][phase].append(ended)

    block_of(tp)
    fold_first(0, tp, 0)
    fold_first(1, tp, 0)
    for swap in swaps:
        swap.wait()
    block_of(1 - tp)
    fold_first(2, None, 0)
    fold_first(0, 1 - tp, 1)
    fold_first(1, 1 - tp, 1)
    results = []

    def deliver(source, target):
        copy = pltpu.make_async_copy(source, target, small_sems.at[len(results)])
        copy.start()
        results.append(copy)

    deliver(whole.at[tp], half_hbm)

    mixer_grad = (dot(whole[0], w_out[0:1024, :]) + dot(whole[1], w_out[1024:2048, :])).astype(BF)
    mixer_wide = mixer_grad.astype(F32)
    small[0] = (mixer_wide * conv_sum_ref[...]).astype(BF)
    pad_right[pl.ds(0, 256), :] = mixer_wide * gate_in_ref[...].astype(F32)
    right = remote(
        pad_right.at[pl.ds(0, 8)],
        halo.at[1],
        halo_send.at[1],
        halo_recv.at[1],
        ((sp + 63) % 64, tp),
    )
    right.start()
    deliver(small.at[0], gate_in_grad_hbm)
    weight_tile(5)
    for which, fold in enumerate(folds):
        start, count = UNIT_CUTS[which]
        for ended in fold[0]:
            ended[0].wait()
        sum1[:, :, pl.ds(start, count)] = folded(which, 0).astype(BF)
        fold_next(which, 1)
    right.wait()
    pad_right[pl.ds(256, 8), :] = jnp.where(sp == 63, 0.0, halo[1])
    prod_grad = jnp.zeros((256, 512), F32)
    for tap in range(3):
        prod_grad = prod_grad + taps_ref[tap : tap + 1, :] * pad_right[pl.ds(2 - tap, 256), :]
    small[1] = (prod_grad * conv_value_ref[...].astype(F32)).astype(BF)
    small[2] = (prod_grad * conv_gate_ref[...].astype(F32)).astype(BF)
    deliver(small.at[1], conv_gate_grad_hbm)
    deliver(small.at[2], conv_value_grad_hbm)
    for which, fold in enumerate(folds):
        start, count = UNIT_CUTS[which]
        for ended in fold[1]:
            ended[0].wait()
        sum2[:, pl.ds(start, count)] = folded(which, 1).astype(BF)
        fold_next(which, 2)
    for which, fold in enumerate(folds):
        start, count = UNIT_CUTS[which]
        for ended in fold[2]:
            ended[0].wait()
        total = folded(which, 2)
        for unit in range(count):
            tile, row = divmod(start + unit, 2)
            out_block_ref[pl.ds(row * 16, 16), pl.ds(tile * 128, 128)] = total[unit]
    deliver(out_block_ref, out_block_hbm)
    for chunk in range(2):
        for share in shares[chunk]:
            share.wait_send()
        for stream in (xs[chunk], gs[chunk]):
            for portion in stream:
                for copies in portion[1:]:
                    sent_phase(copies)
    for stream in backs:
        for portion in stream:
            for copies in portion:
                sent_phase(copies)
    for fold in folds:
        for phase in fold:
            for ended in phase:
                ended[1].wait()
    for copy in results:
        copy.wait()
    for copies in saves[4:]:
        for copy in copies:
            copy.wait()


def main_call(*operands):
    hbm = pl.BlockSpec(memory_space=pl.ANY)
    shape = jax.ShapeDtypeStruct
    rows_shape = (4, 4, 4, SLOTS, 1024)
    full_shape = (4, 4, 4, SLOTS, 2048)
    dma = pltpu.SemaphoreType.DMA
    return pl.pallas_call(
        main_kernel,
        out_shape=(
            shape((256, 1024), BF),
            shape((256, 512), BF),
            shape((256, 512), BF),
            shape((256, 512), BF),
            shape((32, 512), F32),
            shape((2048, 512), BF),
            shape((2048, 512), BF),
            shape((512, 2048), BF),
        ),
        in_specs=[hbm] * 12,
        out_specs=(hbm,) * 8,
        scratch_shapes=[
            pltpu.VMEM((2, 256), jnp.int32),
            pltpu.VMEM((2, 256), F32),
            pltpu.VMEM((256, 1024), BF),
            pltpu.VMEM((256, 1024), BF),
            pltpu.VMEM((256, 512), BF),
            pltpu.VMEM((256, 512), BF),
            pltpu.VMEM((256, 512), BF),
            pltpu.VMEM((3, 512), F32),
            pltpu.VMEM((2, *rows_shape), BF),
            pltpu.VMEM((2, 2, *rows_shape), BF),
            pltpu.VMEM(full_shape, BF),
            pltpu.VMEM(full_shape, BF),
            pltpu.VMEM((2048, 1024), BF),
            pltpu.VMEM((512, 2048), BF),
            pltpu.VMEM((2048, 512), BF),
            pltpu.VMEM((1024, 512), F32),
            pltpu.VMEM((1024, 512), F32),
            pltpu.VMEM((1024, 512), BF),
            pltpu.VMEM((1024, 1024), BF),
            pltpu.VMEM(rows_shape, BF),
            pltpu.VMEM((2, 512, 1024), BF),
            pltpu.VMEM((3, *rows_shape), BF),
            pltpu.VMEM((256, 1024), F32),
            pltpu.VMEM((1024, 256), BF),
            pltpu.VMEM((2, 256, 1024), BF),
            pltpu.VMEM((4, 4, 4, 8, 16, 128), BF),
            pltpu.VMEM((3, 4, 4, 8, 16, 128), BF),
            pltpu.VMEM((4, 4, 8, 16, 128), BF),
            pltpu.VMEM((3, 4, 8, 16, 128), BF),
            pltpu.VMEM((4, 8, 16, 128), BF),
            pltpu.VMEM((3, 8, 16, 128), BF),
            pltpu.VMEM((264, 512), F32),
            pltpu.VMEM((264, 512), F32),
            pltpu.VMEM((2, 8, 512), F32),
            pltpu.VMEM((256, 512), F32),
            pltpu.VMEM((256, 512), BF),
            pltpu.VMEM((3, 256, 512), BF),
            pltpu.VMEM((32, 512), F32),
            dma((8,)),
            dma((4,)),
            dma((6, 2)),
            dma((5,)),
            dma((21, 3)),
            dma((21, 3)),
            dma((10,)),
            dma((10,)),
            dma((2,)),
            dma((2,)),
            dma((3, 4)),
            dma((3, 4)),
        ],
        compiler_params=pltpu.CompilerParams(
            collective_id=0, has_side_effects=True, vmem_limit_bytes=67043328
        ),
    )(*operands)


def finish_kernel(*refs):
    sources, targets = refs[:8], refs[8:16]
    passing, held, narrow, wide, in_sems, out_sems, big_in, big_out = (
        refs[16:20],
        refs[20],
        refs[21:24],
        refs[24:27],
        *refs[27:31],
    )
    passing = (*passing, held)

    def rows_of(which, step):
        rows = narrow[which].shape[1]
        return pl.ds(pl.multiple_of(step * rows, rows), rows)

    def taken(which, step):
        return pltpu.make_async_copy(
            sources[5 + which].at[rows_of(which, step)],
            narrow[which].at[step],
            big_in.at[which, step],
        )

    def given(which, step):
        return pltpu.make_async_copy(
            wide[which].at[step],
            targets[5 + which].at[0, rows_of(which, step)],
            big_out.at[which, step],
        )

    ins = [
        pltpu.make_async_copy(sources[k], passing[k], in_sems.at[k]) for k in range(5)
    ]
    outs = [
        pltpu.make_async_copy(passing[k], targets[k], out_sems.at[k]) for k in range(5)
    ]
    for step in range(4):
        for which in range(3):
            taken(which, step).start()
    start_all(ins)

    def widen(step, carry):
        for which in range(3):
            taken(which, step).wait()
            wide[which][step] = narrow[which][step].astype(F32)
            given(which, step).start()
        return carry

    lax.fori_loop(0, 4, widen, 0)
    for k in range(5):
        ins[k].wait()
        outs[k].start()
    for step in range(4):
        for which in range(3):
            given(which, step).wait()
    for copy in outs:
        copy.wait()


def finished(produced):
    hbm = pl.BlockSpec(memory_space=pl.ANY)
    dma = pltpu.SemaphoreType.DMA
    shape = jax.ShapeDtypeStruct
    tiles = ((4, 512, 512), (4, 512, 512), (4, 128, 2048))
    return pl.pallas_call(
        finish_kernel,
        out_shape=tuple(shape(array.shape, array.dtype) for array in produced[:5])
        + tuple(shape((1, *array.shape), F32) for array in produced[5:]),
        in_specs=[hbm] * 8,
        out_specs=(hbm,) * 8,
        scratch_shapes=[pltpu.VMEM(array.shape, array.dtype) for array in produced[:5]]
        + [pltpu.VMEM(tile, BF) for tile in tiles]
        + [pltpu.VMEM(tile, F32) for tile in tiles]
        + [dma((5,)), dma((5,)), dma((3, 4)), dma((3, 4))],
        compiler_params=pltpu.CompilerParams(vmem_limit_bytes=67043328),
    )(*produced)


def shards(
    stream,
    out_grad,
    gate_in,
    conv_gate,
    conv_value,
    taps,
    w_out,
    route_ids,
    route_weights,
    w_gate,
    w_up,
    w_down,
):
    produced = main_call(
        route_ids.T,
        route_weights.T,
        stream,
        out_grad,
        gate_in,
        conv_gate,
        conv_value,
        taps,
        w_out,
        w_gate,
        w_up,
        w_down,
    )
    return finished(produced)


def solution(mesh):
    placed = (
        P("sp", "tp"),
        P("sp", "tp"),
        P("sp", "tp"),
        P("sp", "tp"),
        P("sp", "tp"),
        P(None, "tp"),
        P(None, "tp"),
        P("sp", None),
        P("sp", None),
        P("sp", None, "tp"),
        P("sp", None, "tp"),
        P("sp", "tp", None),
    )
    return jax.shard_map(
        shards,
        mesh=mesh,
        in_specs=placed,
        out_specs=(
            P("sp", "tp"),
            P("sp", "tp"),
            P("sp", "tp"),
            P("sp", "tp"),
            P("sp", "tp"),
            P("sp", None, "tp"),
            P("sp", None, "tp"),
            P("sp", "tp", None),
        ),
        check_vma=False,
    )
```

```python
import functools

import jax
import jax.numpy as jnp
from jax import lax
from jax.experimental import pallas as pl
from jax.experimental.pallas import tpu as pltpu
from jax.sharding import PartitionSpec as P

MESH = pl.DeviceIdType.MESH
BF = jnp.bfloat16
F32 = jnp.float32
SIDE = 4
SLOTS = 16
STRIDE = (16, 4, 1)
ORDERS = ((2, 1, 0), (1, 0, 2), (0, 2, 1))
Z_OFFSETS = (0, 2, 1, 3)
LATE_SHORT = ((0, 384), (384, 384), (768, 256))
EARLY_SHORT = ((0, 256), (256, 384), (640, 384))
MIDDLE_SHORT = ((0, 384), (384, 256), (640, 384))
X_CUTS = (LATE_SHORT, MIDDLE_SHORT)
G_CUTS = (EARLY_SHORT, LATE_SHORT)
BACK_CUTS = (
    MIDDLE_SHORT,
    ((0, 128), (128, 128), (256, 256)),
    ((512, 256), (768, 128), (896, 128)),
)
HALVES = ((0, 512), (512, 512))


def coordinate(dim):
    return (lax.axis_index("sp") // STRIDE[dim]) % SIDE


def peer_of(dim, by):
    here = coordinate(dim)
    return lax.axis_index("sp") + ((here + by) % SIDE - here) * STRIDE[dim]


def piece(spot, index, width):
    ref, start = spot
    return ref.at[(*index, slice(None), pl.ds(start, width))]


class Phase:
    def __init__(self, source, target, dim, width, chunk, send_sem, recv_sem):
        here = coordinate(dim)
        tp = lax.axis_index("tp")
        every = (slice(None), slice(None))
        both = pl.ds(2 * chunk, 2)
        moves = []
        if dim == 0:
            kept = None
            if chunk == 0:
                kept = (0, *every)
                moves.append((2, (1, *every), (1, *every)))
                gone = (1, *every)
            else:
                moves.append((1, (2, *every), (3, *every)))
                moves.append((3, (3, *every), (2, *every)))
                gone = (both, *every)
        else:

            def at(place):
                index = [both, slice(None), slice(None)]
                index[dim] = place
                return tuple(index)

            kept = at(here)
            for by in (2, 1, 3):
                moves.append((by, at((here + by) % SIDE), at(here)))
            gone = at(pl.ds(0, 3))
        self.copies = [
            pltpu.make_async_remote_copy(
                src_ref=piece(source, from_index, width),
                dst_ref=piece(target, to_index, width),
                send_sem=send_sem,
                recv_sem=recv_sem,
                device_id=(peer_of(dim, by), tp),
                device_id_type=MESH,
            )
            for by, from_index, to_index in moves
        ]
        if kept is not None:
            self.copies.append(
                pltpu.make_async_copy(
                    piece(source, kept, width), piece(target, kept, width), recv_sem
                )
            )
        filled = piece(target, (both, *every), width)
        self.filled = pltpu.make_async_copy(filled, filled, recv_sem)
        left = piece(source, gone, width)
        self.left = pltpu.make_async_copy(left, left, send_sem)


def start_phase(phase):
    start_all(phase.copies)


def arrive_phase(phase):
    phase.filled.wait()


def sent_phase(phase):
    phase.left.wait()


def start_all(copies):
    for copy in copies:
        copy.start()


def slots_in_lanes(ids):
    tokens = ids.shape[1]
    expert = lax.broadcasted_iota(jnp.int32, (64, tokens), 0)
    first, second = ids[0:1, :], ids[1:2, :]
    named = jnp.where((expert == first) | (expert == second), 1.0, 0.0)
    before = (
        lax.broadcasted_iota(jnp.int32, (tokens, tokens), 0)
        < lax.broadcasted_iota(jnp.int32, (tokens, tokens), 1)
    )
    earlier = jnp.dot(
        named.astype(BF), jnp.where(before, 1.0, 0.0).astype(BF), preferred_element_type=F32
    )
    position = [
        jnp.sum(jnp.where(expert == which, earlier, 0.0), axis=0, keepdims=True).astype(jnp.int32)
        for which in (first, second)
    ]
    return first * SLOTS + position[0], second * SLOTS + position[1]


UNIT_CUTS = ((0, 3), (3, 3), (6, 2))


def greet_all():
    barrier = pltpu.get_barrier_semaphore()
    tp = lax.axis_index("tp")
    sp = lax.axis_index("sp")
    for dim in range(3):
        for by in range(1, SIDE):
            pl.semaphore_signal(
                barrier, inc=1, device_id=(peer_of(dim, by), tp), device_id_type=MESH
            )
    for other in ((sp, 1 - tp), ((sp + 1) % 64, tp), ((sp + 63) % 64, tp)):
        pl.semaphore_signal(barrier, inc=1, device_id=other, device_id_type=MESH)


def all_greeted():
    pl.semaphore_wait(pltpu.get_barrier_semaphore(), 12)


def remote(source, target, send_sem, recv_sem, device):
    return pltpu.make_async_remote_copy(
        src_ref=source,
        dst_ref=target,
        send_sem=send_sem,
        recv_sem=recv_sem,
        device_id=device,
        device_id_type=MESH,
    )


def dot(a, b):
    return jnp.dot(a, b, preferred_element_type=F32)


def dot_tn(a, b):
    return lax.dot_general(a, b, (((0,), (0,)), ((), ())), preferred_element_type=F32)


def dot_nt(a, b):
    return lax.dot_general(a, b, (((1,), (1,)), ((), ())), preferred_element_type=F32)


def main_kernel(
    ids_hbm,
    weights_hbm,
    stream_hbm,
    cot_hbm,
    gate_in_hbm,
    conv_gate_hbm,
    conv_value_hbm,
    taps_hbm,
    w_out_hbm,
    w_gate_hbm,
    w_up_hbm,
    w_down_hbm,
    half_hbm,
    gate_in_grad_hbm,
    conv_gate_grad_hbm,
    conv_value_grad_hbm,
    out_block_hbm,
    gate_w_hbm,
    up_w_hbm,
    down_w_hbm,
    ids_ref,
    weights_ref,
    stream_ref,
    cot_ref,
    gate_in_ref,
    conv_gate_ref,
    conv_value_ref,
    taps_ref,
    send,
    middle,
    full_x,
    full_g,
    wgu,
    wd,
    w_out,
    silu_keep,
    slope_keep,
    hidden,
    both_grad,
    arrived,
    staged,
    back,
    added_ref,
    hot_ref,
    whole,
    blocks,
    got1,
    sum1,
    got2,
    sum2,
    got3,
    pad_left,
    pad_right,
    halo,
    conv_sum_ref,
    mixer_out,
    small,
    out_block_ref,
    input_sems,
    load_sems,
    save_sems,
    small_sems,
    send_sems,
    recv_sems,
    tp_send,
    tp_recv,
    halo_send,
    halo_recv,
    fold_send,
    fold_recv,
):
    tp = lax.axis_index("tp")
    sp = lax.axis_index("sp")
    partner = (sp, 1 - tp)
    greet_all()
    inputs = [
        pltpu.make_async_copy(source, target, input_sems.at[k])
        for k, (source, target) in enumerate(
            (
                (ids_hbm, ids_ref),
                (weights_hbm, weights_ref),
                (stream_hbm, stream_ref),
                (cot_hbm, cot_ref),
                (gate_in_hbm, gate_in_ref),
                (conv_gate_hbm, conv_gate_ref),
                (conv_value_hbm, conv_value_ref),
                (taps_hbm, taps_ref),
            )
        )
    ]
    start_all(inputs)
    loads = [
        pltpu.make_async_copy(source, target, load_sems.at[k])
        for k, (source, target) in enumerate(
            (
                (w_gate_hbm.at[0], wgu.at[:, pl.ds(0, 512)]),
                (w_up_hbm.at[0], wgu.at[:, pl.ds(512, 512)]),
                (w_down_hbm.at[0], wd),
                (w_out_hbm, w_out),
            )
        )
    ]
    inputs[0].wait()

    slot0, slot1 = slots_in_lanes(ids_ref[...])
    for copy in inputs[1:]:
        copy.wait()
    weight0, weight1 = weights_ref[0:1, :], weights_ref[1:2, :]

    def row_numbers(place):
        z = (coordinate(0) + Z_OFFSETS[place]) % SIDE
        return lax.broadcasted_iota(jnp.int32, (256, 256), 0) + z * 256

    def gather_x(chunk):
        for place in (2 * chunk, 2 * chunk + 1):
            row = row_numbers(place)
            hot = jnp.where((row == slot0) | (row == slot1), 1.0, 0.0).astype(BF)
            hot_ref[pl.ds(place * 256, 256), :] = hot
            send[0, place] = dot(hot, stream_ref[...]).astype(BF).reshape(4, 4, SLOTS, 1024)

    def gather_g(chunk):
        for place in (2 * chunk, 2 * chunk + 1):
            row = row_numbers(place)
            scale = jnp.sum(
                jnp.where(row == slot0, weight0, 0.0) + jnp.where(row == slot1, weight1, 0.0),
                axis=1,
                keepdims=True,
            )
            hot = hot_ref[pl.ds(place * 256, 256), :]
            send[1, place] = (
                (scale * dot(hot, cot_ref[...])).astype(BF).reshape(4, 4, SLOTS, 1024)
            )

    full = (full_x, full_g)
    shared, rows_out = send.at[0], send.at[1]

    def stream_of(number, spots_of, cuts, chunk):
        portions = []
        for which, cut in enumerate(cuts):
            spots = spots_of(cut)
            portions.append(
                [
                    Phase(
                        spots[phase],
                        spots[phase + 1],
                        ORDERS[which][phase],
                        cut[1],
                        chunk,
                        send_sems.at[number * 3 + which, phase],
                        recv_sems.at[number * 3 + which, phase],
                    )
                    for phase in range(3)
                ]
            )
        return portions

    def outward(tensor, chunk):
        return stream_of(
            chunk * 2 + tensor,
            lambda cut: (
                (send.at[tensor], cut[0]),
                (middle.at[0, tensor], cut[0]),
                (middle.at[1, tensor], cut[0]),
                (full[tensor], pl.multiple_of(tp * 1024 + cut[0], 128)),
            ),
            (X_CUTS, G_CUTS)[tensor][chunk],
            chunk,
        )

    def homeward(number):
        return stream_of(
            4 + number,
            lambda cut: (
                (rows_out, cut[0]),
                (back.at[0], cut[0]),
                (back.at[1], cut[0]),
                (back.at[2], cut[0]),
            ),
            BACK_CUTS[number],
            min(number, 1),
        )

    xs = [outward(0, chunk) for chunk in range(2)]
    gs = [outward(1, chunk) for chunk in range(2)]
    backs = [homeward(number) for number in range(3)]

    def begin(portions):
        for portion in portions:
            start_phase(portion[0])

    def advance(portions, phase):
        for portion in portions:
            arrive_phase(portion[phase - 1])
            start_phase(portion[phase])

    saves = []

    def half_of(tensor, chunk, cut):
        start = pl.multiple_of(tp * 1024 + cut[0], 128)
        return full[tensor].at[pl.ds(2 * chunk, 2), :, :, :, pl.ds(start, cut[1])]

    def crossing(tensor, chunk, cut):
        part = half_of(tensor, chunk, cut)
        number = chunk * 2 + tensor
        return remote(part, part, tp_send.at[number], tp_recv.at[number], partner)

    def cross(tensor, chunk):
        portions = (xs, gs)[tensor][chunk]
        for which, cut in enumerate((X_CUTS, G_CUTS)[tensor][chunk]):
            arrive_phase(portions[which][2])
            crossing(tensor, chunk, cut).start()

    def crossed(tensor, chunk):
        crossing(tensor, chunk, (0, 1024)).wait()

    def weight_tile(number):
        slot = number % 2
        if number >= 2:
            for copy in saves[number - 2]:
                copy.wait()
        if number < 4:
            at = pl.ds(number * 512, 512)
            columns = full_x[:, :, :, :, at].reshape(1024, 512)
            staged[slot] = dot_tn(columns, both_grad[...]).astype(BF)
            pairs = (
                (staged.at[slot, :, pl.ds(0, 512)], gate_w_hbm.at[at]),
                (staged.at[slot, :, pl.ds(512, 512)], up_w_hbm.at[at]),
            )
        else:
            at = pl.ds((number - 4) * 1024, 1024)
            columns = full_g[:, :, :, :, at].reshape(1024, 1024)
            staged[slot] = dot_tn(hidden[...], columns).astype(BF)
            pairs = ((staged.at[slot], down_w_hbm.at[:, at]),)
        copies = [
            pltpu.make_async_copy(source, target, save_sems.at[number, k])
            for k, (source, target) in enumerate(pairs)
        ]
        start_all(copies)
        saves.append(copies)

    def activate(chunk):
        rows = full_x[pl.ds(chunk * 2, 2)].reshape(512, 2048)
        at = pl.ds(chunk * 512, 512)
        pre_gate = dot(rows, wgu[:, 0:512])
        pre_up = dot(rows, wgu[:, 512:1024])
        sigmoid = jax.nn.sigmoid(pre_gate)
        silu = pre_gate * sigmoid
        silu_keep[at, :] = silu
        slope_keep[at, :] = pre_up * sigmoid * (1.0 + pre_gate * (1.0 - sigmoid))
        hidden[at, :] = (silu * pre_up).astype(BF)

    def differentiate(chunk):
        rows = full_g[pl.ds(chunk * 2, 2)].reshape(512, 2048)
        at = pl.ds(chunk * 512, 512)
        hidden_grad = dot_nt(rows, wd[...])
        both_grad[at, 512:1024] = (hidden_grad * silu_keep[at, :]).astype(BF)
        both_grad[at, 0:512] = (hidden_grad * slope_keep[at, :]).astype(BF)

    def partial_of(side, cut, chunk):
        at = pl.ds(pl.multiple_of(side * 1024 + cut[0], 128), cut[1])
        rows = pl.ds(chunk * 512, 512)
        return dot_nt(both_grad[rows, :], wgu[at, :])

    shares = {}

    def part(chunk, cut):
        return (pl.ds(2 * chunk, 2), slice(None), slice(None), slice(None), pl.ds(*cut))

    def share_theirs(chunk):
        shares[chunk] = []
        for which, cut in enumerate(HALVES):
            index = part(chunk, cut)
            shared[index] = (
                partial_of(1 - tp, cut, chunk).astype(BF).reshape(2, 4, 4, SLOTS, cut[1])
            )
            number = 4 + chunk * 2 + which
            share = remote(
                shared.at[index],
                arrived.at[index],
                tp_send.at[number],
                tp_recv.at[number],
                partner,
            )
            share.start()
            shares[chunk].append(share)

    def add_mine(chunk):
        for which, cut in enumerate(HALVES):
            index = part(chunk, cut)
            mine = partial_of(tp, cut, chunk).astype(BF).astype(F32)
            shares[chunk][which].wait_recv()
            theirs = arrived[index].reshape(512, cut[1]).astype(F32)
            rows_out[index] = (mine + theirs).astype(BF).reshape(2, 4, 4, SLOTS, cut[1])
            if chunk == 1:
                begin(backs[1 + which])

    gather_x(0)
    all_greeted()
    start_all(loads)
    begin(xs[0])
    gather_g(0)
    begin(gs[0])
    gather_x(1)
    begin(xs[1])
    gather_g(1)
    pad_left[pl.ds(8, 256), :] = conv_gate_ref[...].astype(F32) * conv_value_ref[...].astype(F32)
    left = remote(
        pad_left.at[pl.ds(256, 8)],
        halo.at[0],
        halo_send.at[0],
        halo_recv.at[0],
        ((sp + 1) % 64, tp),
    )
    left.start()
    advance(xs[0], 1)
    advance(gs[0], 1)
    begin(gs[1])
    left.wait()
    pad_left[pl.ds(0, 8), :] = jnp.where(sp == 0, 0.0, halo[0])
    conv_sum = jnp.zeros((256, 512), F32)
    for tap in range(3):
        conv_sum = conv_sum + taps_ref[tap : tap + 1, :] * pad_left[pl.ds(6 + tap, 256), :]
    conv_sum_ref[...] = conv_sum
    mixer_out[...] = (gate_in_ref[...].astype(F32) * conv_sum).astype(BF)
    advance(xs[0], 2)
    advance(gs[0], 2)
    advance(xs[1], 1)
    advance(gs[1], 1)
    cross(0, 0)
    for load in loads:
        load.wait()
    crossed(0, 0)
    cross(1, 0)
    advance(xs[1], 2)
    activate(0)
    crossed(1, 0)
    advance(gs[1], 2)
    differentiate(0)
    for stream in (*xs, *gs):
        for portion in stream:
            sent_phase(portion[0])
    share_theirs(0)
    add_mine(0)
    begin(backs[0])
    cross(0, 1)
    crossed(0, 1)
    cross(1, 1)
    activate(1)
    crossed(1, 1)
    differentiate(1)
    advance(backs[0], 1)
    share_theirs(1)
    add_mine(1)
    advance(backs[0], 2)
    weight_tile(0)
    advance(backs[1], 1)
    weight_tile(1)
    advance(backs[2], 1)
    for portion in backs[0]:
        arrive_phase(portion[2])
    added_ref[...] = dot_tn(
        hot_ref[pl.ds(0, 512), :], back[2, pl.ds(0, 2)].reshape(512, 1024)
    ) + cot_ref[...].astype(F32)
    weight_tile(2)
    advance(backs[1], 2)
    weight_tile(3)
    advance(backs[2], 2)
    weight_tile(4)
    swaps = []

    def combine(which):
        for portion in backs[1 + which]:
            arrive_phase(portion[2])
        columns = pl.ds(*HALVES[which])
        rows = back[2, pl.ds(2, 2), :, :, :, columns].reshape(512, 512)
        total = added_ref[:, columns] + dot_tn(hot_ref[pl.ds(512, 512), :], rows)
        whole[tp, :, columns] = total.astype(BF)
        swap = remote(
            whole.at[tp, :, columns],
            whole.at[tp, :, columns],
            tp_send.at[8 + which],
            tp_recv.at[8 + which],
            partner,
        )
        swap.start()
        swaps.append(swap)

    combine(0)
    combine(1)

    def block_of(half):
        for part in range(2):
            product = dot_tn(whole[half, :, pl.ds(part * 512, 512)], mixer_out[...])
            for tile in range(4):
                blocks[half * 2 + part, :, :, pl.ds(tile * 2, 2)] = (
                    product[:, tile * 128 : (tile + 1) * 128].astype(BF).reshape(4, 4, 2, 16, 128)
                )

    def fold_copies(which, phase, half=None, late=0):
        start, count = UNIT_CUTS[which]
        dim = ORDERS[which][phase]
        here = coordinate(dim)
        left_dims = sorted(ORDERS[which][phase:])
        copies = []
        for by in (2, 1, 3):
            index = [slice(None)] * len(left_dims)
            index[left_dims.index(dim)] = (here + by) % SIDE
            kept = slice(None)
            if half is not None:
                kept = pl.ds(2 * half, 2)
                index[0] = kept
            units = pl.ds(start, count)
            if phase == 0:
                source = blocks.at[(*index, units)]
                target = got1.at[by - 1, kept, :, units]
            elif phase == 1:
                source = sum1.at[(*index, units)]
                target = got2.at[by - 1, :, units]
            else:
                source = sum2.at[(*index, units)]
                target = got3.at[by - 1, units]
            copies.append(
                remote(
                    source,
                    target,
                    fold_send.at[which, phase + 3 * late],
                    fold_recv.at[which, phase + 3 * late],
                    (peer_of(dim, by), tp),
                )
            )
        index = [slice(None)] * len(left_dims)
        index[left_dims.index(dim)] = pl.ds(0, 3)
        kept = slice(None)
        if half is not None:
            kept = pl.ds(2 * half, 2)
            index[0] = kept
        if phase == 0:
            source, target = blocks.at[(*index, units)], got1.at[:, kept, :, units]
        elif phase == 1:
            source, target = sum1.at[(*index, units)], got2.at[:, :, units]
        else:
            source, target = sum2.at[(*index, units)], got3.at[:, units]
        ended = (
            pltpu.make_async_copy(target, target, fold_recv.at[which, phase + 3 * late]),
            pltpu.make_async_copy(source, source, fold_send.at[which, phase + 3 * late]),
        )
        return copies, ended

    def folded(which, phase):
        start, count = UNIT_CUTS[which]
        units = pl.ds(start, count)
        dim = ORDERS[which][phase]
        left_dims = sorted(ORDERS[which][phase:])
        index = [slice(None)] * len(left_dims)
        index[left_dims.index(dim)] = coordinate(dim)
        source = (blocks, sum1, sum2)[phase]
        total = source[(*index, units)].astype(F32)
        for by in range(3):
            if phase == 0:
                total = total + got1[by, :, :, units].astype(F32)
            elif phase == 1:
                total = total + got2[by, :, units].astype(F32)
            else:
                total = total + got3[by, units].astype(F32)
        return total

    folds = [[[], [], []] for which in range(3)]

    def fold_first(which, half, late):
        copies, ended = fold_copies(which, 0, half, late)
        start_all(copies)
        folds[which][0].append(ended)

    def fold_next(which, phase):
        copies, ended = fold_copies(which, phase)
        start_all(copies)
        folds[which][phase].append(ended)

    block_of(tp)
    fold_first(0, tp, 0)
    fold_first(1, tp, 0)
    for swap in swaps:
        swap.wait()
    block_of(1 - tp)
    fold_first(2, None, 0)
    fold_first(0, 1 - tp, 1)
    fold_first(1, 1 - tp, 1)
    results = []

    def deliver(source, target):
        copy = pltpu.make_async_copy(source, target, small_sems.at[len(results)])
        copy.start()
        results.append(copy)

    deliver(whole.at[tp], half_hbm)

    mixer_grad = (dot(whole[0], w_out[0:1024, :]) + dot(whole[1], w_out[1024:2048, :])).astype(BF)
    mixer_wide = mixer_grad.astype(F32)
    small[0] = (mixer_wide * conv_sum_ref[...]).astype(BF)
    pad_right[pl.ds(0, 256), :] = mixer_wide * gate_in_ref[...].astype(F32)
    right = remote(
        pad_right.at[pl.ds(0, 8)],
        halo.at[1],
        halo_send.at[1],
        halo_recv.at[1],
        ((sp + 63) % 64, tp),
    )
    right.start()
    deliver(small.at[0], gate_in_grad_hbm)
    weight_tile(5)
    for which, fold in enumerate(folds):
        start, count = UNIT_CUTS[which]
        for ended in fold[0]:
            ended[0].wait()
        sum1[:, :, pl.ds(start, count)] = folded(which, 0).astype(BF)
        fold_next(which, 1)
    right.wait()
    pad_right[pl.ds(256, 8), :] = jnp.where(sp == 63, 0.0, halo[1])
    prod_grad = jnp.zeros((256, 512), F32)
    for tap in range(3):
        prod_grad = prod_grad + taps_ref[tap : tap + 1, :] * pad_right[pl.ds(2 - tap, 256), :]
    small[1] = (prod_grad * conv_value_ref[...].astype(F32)).astype(BF)
    small[2] = (prod_grad * conv_gate_ref[...].astype(F32)).astype(BF)
    deliver(small.at[1], conv_gate_grad_hbm)
    deliver(small.at[2], conv_value_grad_hbm)
    for which, fold in enumerate(folds):
        start, count = UNIT_CUTS[which]
        for ended in fold[1]:
            ended[0].wait()
        sum2[:, pl.ds(start, count)] = folded(which, 1).astype(BF)
        fold_next(which, 2)
    for which, fold in enumerate(folds):
        start, count = UNIT_CUTS[which]
        for ended in fold[2]:
            ended[0].wait()
        total = folded(which, 2)
        for unit in range(count):
            tile, row = divmod(start + unit, 2)
            out_block_ref[pl.ds(row * 16, 16), pl.ds(tile * 128, 128)] = total[unit]
    deliver(out_block_ref, out_block_hbm)
    for chunk in range(2):
        for share in shares[chunk]:
            share.wait_send()
        for stream in (xs[chunk], gs[chunk]):
            for portion in stream:
                for copies in portion[1:]:
                    sent_phase(copies)
    for stream in backs:
        for portion in stream:
            for copies in portion:
                sent_phase(copies)
    for fold in folds:
        for phase in fold:
            for ended in phase:
                ended[1].wait()
    for copy in results:
        copy.wait()
    for copies in saves[4:]:
        for copy in copies:
            copy.wait()


def main_call(*operands):
    hbm = pl.BlockSpec(memory_space=pl.ANY)
    shape = jax.ShapeDtypeStruct
    rows_shape = (4, 4, 4, SLOTS, 1024)
    full_shape = (4, 4, 4, SLOTS, 2048)
    dma = pltpu.SemaphoreType.DMA
    return pl.pallas_call(
        main_kernel,
        out_shape=(
            shape((256, 1024), BF),
            shape((256, 512), BF),
            shape((256, 512), BF),
            shape((256, 512), BF),
            shape((32, 512), F32),
            shape((2048, 512), BF),
            shape((2048, 512), BF),
            shape((512, 2048), BF),
        ),
        in_specs=[hbm] * 12,
        out_specs=(hbm,) * 8,
        scratch_shapes=[
            pltpu.VMEM((2, 256), jnp.int32),
            pltpu.VMEM((2, 256), F32),
            pltpu.VMEM((256, 1024), BF),
            pltpu.VMEM((256, 1024), BF),
            pltpu.VMEM((256, 512), BF),
            pltpu.VMEM((256, 512), BF),
            pltpu.VMEM((256, 512), BF),
            pltpu.VMEM((3, 512), F32),
            pltpu.VMEM((2, *rows_shape), BF),
            pltpu.VMEM((2, 2, *rows_shape), BF),
            pltpu.VMEM(full_shape, BF),
            pltpu.VMEM(full_shape, BF),
            pltpu.VMEM((2048, 1024), BF),
            pltpu.VMEM((512, 2048), BF),
            pltpu.VMEM((2048, 512), BF),
            pltpu.VMEM((1024, 512), F32),
            pltpu.VMEM((1024, 512), F32),
            pltpu.VMEM((1024, 512), BF),
            pltpu.VMEM((1024, 1024), BF),
            pltpu.VMEM(rows_shape, BF),
            pltpu.VMEM((2, 512, 1024), BF),
            pltpu.VMEM((3, *rows_shape), BF),
            pltpu.VMEM((256, 1024), F32),
            pltpu.VMEM((1024, 256), BF),
            pltpu.VMEM((2, 256, 1024), BF),
            pltpu.VMEM((4, 4, 4, 8, 16, 128), BF),
            pltpu.VMEM((3, 4, 4, 8, 16, 128), BF),
            pltpu.VMEM((4, 4, 8, 16, 128), BF),
            pltpu.VMEM((3, 4, 8, 16, 128), BF),
            pltpu.VMEM((4, 8, 16, 128), BF),
            pltpu.VMEM((3, 8, 16, 128), BF),
            pltpu.VMEM((264, 512), F32),
            pltpu.VMEM((264, 512), F32),
            pltpu.VMEM((2, 8, 512), F32),
            pltpu.VMEM((256, 512), F32),
            pltpu.VMEM((256, 512), BF),
            pltpu.VMEM((3, 256, 512), BF),
            pltpu.VMEM((32, 512), F32),
            dma((8,)),
            dma((4,)),
            dma((6, 2)),
            dma((5,)),
            dma((21, 3)),
            dma((21, 3)),
            dma((10,)),
            dma((10,)),
            dma((2,)),
            dma((2,)),
            dma((3, 4)),
            dma((3, 4)),
        ],
        compiler_params=pltpu.CompilerParams(
            collective_id=0, has_side_effects=True, vmem_limit_bytes=67043328
        ),
    )(*operands)


def finish_kernel(*refs):
    sources, targets = refs[:8], refs[8:16]
    passing, held, narrow, wide, in_sems, out_sems, big_in, big_out = (
        refs[16:20],
        refs[20],
        refs[21:24],
        refs[24:27],
        *refs[27:31],
    )
    passing = (*passing, held)

    def rows_of(which, step):
        rows = narrow[which].shape[1]
        return pl.ds(pl.multiple_of(step * rows, rows), rows)

    def taken(which, step):
        return pltpu.make_async_copy(
            sources[5 + which].at[rows_of(which, step)],
            narrow[which].at[step],
            big_in.at[which, step],
        )

    def given(which, step):
        return pltpu.make_async_copy(
            wide[which].at[step],
            targets[5 + which].at[0, rows_of(which, step)],
            big_out.at[which, step],
        )

    ins = [
        pltpu.make_async_copy(sources[k], passing[k], in_sems.at[k]) for k in range(5)
    ]
    outs = [
        pltpu.make_async_copy(passing[k], targets[k], out_sems.at[k]) for k in range(5)
    ]
    for step in range(4):
        for which in range(3):
            taken(which, step).start()
    start_all(ins)

    def widen(step, carry):
        for which in range(3):
            taken(which, step).wait()
            wide[which][step] = narrow[which][step].astype(F32)
            given(which, step).start()
        return carry

    lax.fori_loop(0, 4, widen, 0)
    for k in range(5):
        ins[k].wait()
        outs[k].start()
    for step in range(4):
        for which in range(3):
            given(which, step).wait()
    for copy in outs:
        copy.wait()


def finished(produced):
    hbm = pl.BlockSpec(memory_space=pl.ANY)
    dma = pltpu.SemaphoreType.DMA
    shape = jax.ShapeDtypeStruct
    tiles = ((4, 512, 512), (4, 512, 512), (4, 128, 2048))
    return pl.pallas_call(
        finish_kernel,
        out_shape=tuple(shape(array.shape, array.dtype) for array in produced[:5])
        + tuple(shape((1, *array.shape), F32) for array in produced[5:]),
        in_specs=[hbm] * 8,
        out_specs=(hbm,) * 8,
        scratch_shapes=[pltpu.VMEM(array.shape, array.dtype) for array in produced[:5]]
        + [pltpu.VMEM(tile, BF) for tile in tiles]
        + [pltpu.VMEM(tile, F32) for tile in tiles]
        + [dma((5,)), dma((5,)), dma((3, 4)), dma((3, 4))],
        compiler_params=pltpu.CompilerParams(vmem_limit_bytes=67043328),
    )(*produced)


def shards(
    stream,
    out_grad,
    gate_in,
    conv_gate,
    conv_value,
    taps,
    w_out,
    route_ids,
    route_weights,
    w_gate,
    w_up,
    w_down,
):
    produced = main_call(
        route_ids.T,
        route_weights.T,
        stream,
        out_grad,
        gate_in,
        conv_gate,
        conv_value,
        taps,
        w_out,
        w_gate,
        w_up,
        w_down,
    )
    return finished(produced)


def solution(mesh):
    placed = (
        P("sp", "tp"),
        P("sp", "tp"),
        P("sp", "tp"),
        P("sp", "tp"),
        P("sp", "tp"),
        P(None, "tp"),
        P(None, "tp"),
        P("sp", None),
        P("sp", None),
        P("sp", None, "tp"),
        P("sp", None, "tp"),
        P("sp", "tp", None),
    )
    return jax.shard_map(
        shards,
        mesh=mesh,
        in_specs=placed,
        out_specs=(
            P("sp", "tp"),
            P("sp", "tp"),
            P("sp", "tp"),
            P("sp", "tp"),
            P("sp", "tp"),
            P("sp", None, "tp"),
            P("sp", None, "tp"),
            P("sp", "tp", None),
        ),
        check_vma=False,
    )
```

```python
import functools

import jax
import jax.numpy as jnp
from jax import lax
from jax.experimental import pallas as pl
from jax.experimental.pallas import tpu as pltpu
from jax.sharding import PartitionSpec as P

MESH = pl.DeviceIdType.MESH
BF = jnp.bfloat16
F32 = jnp.float32
SIDE = 4
SLOTS = 16
STRIDE = (16, 4, 1)
ORDERS = ((2, 1, 0), (1, 0, 2), (0, 2, 1))
Z_OFFSETS = (0, 2, 1, 3)
LATE_SHORT = ((0, 384), (384, 384), (768, 256))
EARLY_SHORT = ((0, 256), (256, 384), (640, 384))
MIDDLE_SHORT = ((0, 384), (384, 256), (640, 384))
X_CUTS = (LATE_SHORT, MIDDLE_SHORT)
G_CUTS = (EARLY_SHORT, LATE_SHORT)
BACK_CUTS = (
    MIDDLE_SHORT,
    ((0, 128), (128, 128), (256, 256)),
    ((512, 256), (768, 128), (896, 128)),
)
HALVES = ((0, 512), (512, 512))


def coordinate(dim):
    return (lax.axis_index("sp") // STRIDE[dim]) % SIDE


def peer_of(dim, by):
    here = coordinate(dim)
    return lax.axis_index("sp") + ((here + by) % SIDE - here) * STRIDE[dim]


def piece(spot, index, width):
    ref, start = spot
    return ref.at[(*index, slice(None), pl.ds(start, width))]


class Phase:
    def __init__(self, source, target, dim, width, chunk, send_sem, recv_sem):
        here = coordinate(dim)
        tp = lax.axis_index("tp")
        every = (slice(None), slice(None))
        both = pl.ds(2 * chunk, 2)
        moves = []
        if dim == 0:
            kept = None
            if chunk == 0:
                kept = (0, *every)
                moves.append((2, (1, *every), (1, *every)))
                gone = (1, *every)
            else:
                moves.append((1, (2, *every), (3, *every)))
                moves.append((3, (3, *every), (2, *every)))
                gone = (both, *every)
        else:

            def at(place):
                index = [both, slice(None), slice(None)]
                index[dim] = place
                return tuple(index)

            kept = at(here)
            for by in (2, 1, 3):
                moves.append((by, at((here + by) % SIDE), at(here)))
            gone = at(pl.ds(0, 3))
        self.copies = [
            pltpu.make_async_remote_copy(
                src_ref=piece(source, from_index, width),
                dst_ref=piece(target, to_index, width),
                send_sem=send_sem,
                recv_sem=recv_sem,
                device_id=(peer_of(dim, by), tp),
                device_id_type=MESH,
            )
            for by, from_index, to_index in moves
        ]
        if kept is not None:
            self.copies.append(
                pltpu.make_async_copy(
                    piece(source, kept, width), piece(target, kept, width), recv_sem
                )
            )
        filled = piece(target, (both, *every), width)
        self.filled = pltpu.make_async_copy(filled, filled, recv_sem)
        left = piece(source, gone, width)
        self.left = pltpu.make_async_copy(left, left, send_sem)


def start_phase(phase):
    start_all(phase.copies)


def arrive_phase(phase):
    phase.filled.wait()


def sent_phase(phase):
    phase.left.wait()


def start_all(copies):
    for copy in copies:
        copy.start()


def slots_in_lanes(ids):
    tokens = ids.shape[1]
    expert = lax.broadcasted_iota(jnp.int32, (64, tokens), 0)
    first, second = ids[0:1, :], ids[1:2, :]
    named = jnp.where((expert == first) | (expert == second), 1.0, 0.0)
    before = (
        lax.broadcasted_iota(jnp.int32, (tokens, tokens), 0)
        < lax.broadcasted_iota(jnp.int32, (tokens, tokens), 1)
    )
    earlier = jnp.dot(
        named.astype(BF), jnp.where(before, 1.0, 0.0).astype(BF), preferred_element_type=F32
    )
    position = [
        jnp.sum(jnp.where(expert == which, earlier, 0.0), axis=0, keepdims=True).astype(jnp.int32)
        for which in (first, second)
    ]
    return first * SLOTS + position[0], second * SLOTS + position[1]


UNIT_CUTS = ((0, 3), (3, 3), (6, 2))


def greet_all():
    barrier = pltpu.get_barrier_semaphore()
    tp = lax.axis_index("tp")
    sp = lax.axis_index("sp")
    for dim in range(3):
        for by in range(1, SIDE):
            pl.semaphore_signal(
                barrier, inc=1, device_id=(peer_of(dim, by), tp), device_id_type=MESH
            )
    for other in ((sp, 1 - tp), ((sp + 1) % 64, tp), ((sp + 63) % 64, tp)):
        pl.semaphore_signal(barrier, inc=1, device_id=other, device_id_type=MESH)


def all_greeted():
    pl.semaphore_wait(pltpu.get_barrier_semaphore(), 12)


def remote(source, target, send_sem, recv_sem, device):
    return pltpu.make_async_remote_copy(
        src_ref=source,
        dst_ref=target,
        send_sem=send_sem,
        recv_sem=recv_sem,
        device_id=device,
        device_id_type=MESH,
    )


def dot(a, b):
    return jnp.dot(a, b, preferred_element_type=F32)


def dot_tn(a, b):
    return lax.dot_general(a, b, (((0,), (0,)), ((), ())), preferred_element_type=F32)


def dot_nt(a, b):
    return lax.dot_general(a, b, (((1,), (1,)), ((), ())), preferred_element_type=F32)


def main_kernel(
    ids_hbm,
    weights_hbm,
    stream_hbm,
    cot_hbm,
    gate_in_hbm,
    conv_gate_hbm,
    conv_value_hbm,
    taps_hbm,
    w_out_hbm,
    w_gate_hbm,
    w_up_hbm,
    w_down_hbm,
    half_hbm,
    gate_in_grad_hbm,
    conv_gate_grad_hbm,
    conv_value_grad_hbm,
    out_block_hbm,
    gate_w_hbm,
    up_w_hbm,
    down_w_hbm,
    ids_ref,
    weights_ref,
    stream_ref,
    cot_ref,
    gate_in_ref,
    conv_gate_ref,
    conv_value_ref,
    taps_ref,
    send,
    middle,
    full_x,
    full_g,
    wgu,
    wd,
    w_out,
    silu_keep,
    slope_keep,
    hidden,
    both_grad,
    arrived,
    staged,
    back,
    added_ref,
    hot_ref,
    whole,
    blocks,
    got1,
    sum1,
    got2,
    sum2,
    got3,
    pad_left,
    pad_right,
    halo,
    conv_sum_ref,
    mixer_out,
    small,
    out_block_ref,
    input_sems,
    load_sems,
    save_sems,
    small_sems,
    send_sems,
    recv_sems,
    tp_send,
    tp_recv,
    halo_send,
    halo_recv,
    fold_send,
    fold_recv,
):
    tp = lax.axis_index("tp")
    sp = lax.axis_index("sp")
    partner = (sp, 1 - tp)
    greet_all()
    inputs = [
        pltpu.make_async_copy(source, target, input_sems.at[k])
        for k, (source, target) in enumerate(
            (
                (ids_hbm, ids_ref),
                (weights_hbm, weights_ref),
                (stream_hbm, stream_ref),
                (cot_hbm, cot_ref),
                (gate_in_hbm, gate_in_ref),
                (conv_gate_hbm, conv_gate_ref),
                (conv_value_hbm, conv_value_ref),
                (taps_hbm, taps_ref),
            )
        )
    ]
    start_all(inputs)
    loads = [
        pltpu.make_async_copy(source, target, load_sems.at[k])
        for k, (source, target) in enumerate(
            (
                (w_gate_hbm.at[0], wgu.at[:, pl.ds(0, 512)]),
                (w_up_hbm.at[0], wgu.at[:, pl.ds(512, 512)]),
                (w_down_hbm.at[0], wd),
                (w_out_hbm, w_out),
            )
        )
    ]
    inputs[0].wait()

    slot0, slot1 = slots_in_lanes(ids_ref[...])
    for copy in inputs[1:]:
        copy.wait()
    weight0, weight1 = weights_ref[0:1, :], weights_ref[1:2, :]

    def row_numbers(place):
        z = (coordinate(0) + Z_OFFSETS[place]) % SIDE
        return lax.broadcasted_iota(jnp.int32, (256, 256), 0) + z * 256

    def gather_x(chunk):
        for place in (2 * chunk, 2 * chunk + 1):
            row = row_numbers(place)
            hot = jnp.where((row == slot0) | (row == slot1), 1.0, 0.0).astype(BF)
            hot_ref[pl.ds(place * 256, 256), :] = hot
            send[0, place] = dot(hot, stream_ref[...]).astype(BF).reshape(4, 4, SLOTS, 1024)

    def gather_g(chunk):
        for place in (2 * chunk, 2 * chunk + 1):
            row = row_numbers(place)
            scale = jnp.sum(
                jnp.where(row == slot0, weight0, 0.0) + jnp.where(row == slot1, weight1, 0.0),
                axis=1,
                keepdims=True,
            )
            hot = hot_ref[pl.ds(place * 256, 256), :]
            send[1, place] = (
                (scale * dot(hot, cot_ref[...])).astype(BF).reshape(4, 4, SLOTS, 1024)
            )

    full = (full_x, full_g)
    shared, rows_out = send.at[0], send.at[1]

    def stream_of(number, spots_of, cuts, chunk):
        portions = []
        for which, cut in enumerate(cuts):
            spots = spots_of(cut)
            portions.append(
                [
                    Phase(
                        spots[phase],
                        spots[phase + 1],
                        ORDERS[which][phase],
                        cut[1],
                        chunk,
                        send_sems.at[number * 3 + which, phase],
                        recv_sems.at[number * 3 + which, phase],
                    )
                    for phase in range(3)
                ]
            )
        return portions

    def outward(tensor, chunk):
        return stream_of(
            chunk * 2 + tensor,
            lambda cut: (
                (send.at[tensor], cut[0]),
                (middle.at[0, tensor], cut[0]),
                (middle.at[1, tensor], cut[0]),
                (full[tensor], pl.multiple_of(tp * 1024 + cut[0], 128)),
            ),
            (X_CUTS, G_CUTS)[tensor][chunk],
            chunk,
        )

    def homeward(number):
        return stream_of(
            4 + number,
            lambda cut: (
                (rows_out, cut[0]),
                (back.at[0], cut[0]),
                (back.at[1], cut[0]),
                (back.at[2], cut[0]),
            ),
            BACK_CUTS[number],
            min(number, 1),
        )

    xs = [outward(0, chunk) for chunk in range(2)]
    gs = [outward(1, chunk) for chunk in range(2)]
    backs = [homeward(number) for number in range(3)]

    def begin(portions):
        for portion in portions:
            start_phase(portion[0])

    def advance(portions, phase):
        for portion in portions:
            arrive_phase(portion[phase - 1])
            start_phase(portion[phase])

    saves = []

    def half_of(tensor, chunk, cut):
        start = pl.multiple_of(tp * 1024 + cut[0], 128)
        return full[tensor].at[pl.ds(2 * chunk, 2), :, :, :, pl.ds(start, cut[1])]

    def crossing(tensor, chunk, cut):
        part = half_of(tensor, chunk, cut)
        number = chunk * 2 + tensor
        return remote(part, part, tp_send.at[number], tp_recv.at[number], partner)

    def cross(tensor, chunk):
        portions = (xs, gs)[tensor][chunk]
        for which, cut in enumerate((X_CUTS, G_CUTS)[tensor][chunk]):
            arrive_phase(portions[which][2])
            crossing(tensor, chunk, cut).start()

    def crossed(tensor, chunk):
        crossing(tensor, chunk, (0, 1024)).wait()

    def weight_tile(number):
        slot = number % 2
        if number >= 2:
            for copy in saves[number - 2]:
                copy.wait()
        if number < 4:
            at = pl.ds(number * 512, 512)
            columns = full_x[:, :, :, :, at].reshape(1024, 512)
            staged[slot] = dot_tn(columns, both_grad[...]).astype(BF)
            pairs = (
                (staged.at[slot, :, pl.ds(0, 512)], gate_w_hbm.at[at]),
                (staged.at[slot, :, pl.ds(512, 512)], up_w_hbm.at[at]),
            )
        else:
            at = pl.ds((number - 4) * 1024, 1024)
            columns = full_g[:, :, :, :, at].reshape(1024, 1024)
            staged[slot] = dot_tn(hidden[...], columns).astype(BF)
            pairs = ((staged.at[slot], down_w_hbm.at[:, at]),)
        copies = [
            pltpu.make_async_copy(source, target, save_sems.at[number, k])
            for k, (source, target) in enumerate(pairs)
        ]
        start_all(copies)
        saves.append(copies)

    def activate(chunk):
        rows = full_x[pl.ds(chunk * 2, 2)].reshape(512, 2048)
        at = pl.ds(chunk * 512, 512)
        pre_gate = dot(rows, wgu[:, 0:512])
        pre_up = dot(rows, wgu[:, 512:1024])
        sigmoid = jax.nn.sigmoid(pre_gate)
        silu = pre_gate * sigmoid
        silu_keep[at, :] = silu
        slope_keep[at, :] = pre_up * sigmoid * (1.0 + pre_gate * (1.0 - sigmoid))
        hidden[at, :] = (silu * pre_up).astype(BF)

    def differentiate(chunk):
        rows = full_g[pl.ds(chunk * 2, 2)].reshape(512, 2048)
        at = pl.ds(chunk * 512, 512)
        hidden_grad = dot_nt(rows, wd[...])
        both_grad[at, 512:1024] = (hidden_grad * silu_keep[at, :]).astype(BF)
        both_grad[at, 0:512] = (hidden_grad * slope_keep[at, :]).astype(BF)

    def partial_of(side, cut, chunk):
        at = pl.ds(pl.multiple_of(side * 1024 + cut[0], 128), cut[1])
        rows = pl.ds(chunk * 512, 512)
        return dot_nt(both_grad[rows, :], wgu[at, :])

    shares = {}

    def part(chunk, cut):
        return (pl.ds(2 * chunk, 2), slice(None), slice(None), slice(None), pl.ds(*cut))

    def share_theirs(chunk):
        shares[chunk] = []
        for which, cut in enumerate(HALVES):
            index = part(chunk, cut)
            shared[index] = (
                partial_of(1 - tp, cut, chunk).astype(BF).reshape(2, 4, 4, SLOTS, cut[1])
            )
            number = 4 + chunk * 2 + which
            share = remote(
                shared.at[index],
                arrived.at[index],
                tp_send.at[number],
                tp_recv.at[number],
                partner,
            )
            share.start()
            shares[chunk].append(share)

    def add_mine(chunk):
        for which, cut in enumerate(HALVES):
            index = part(chunk, cut)
            mine = partial_of(tp, cut, chunk).astype(BF).astype(F32)
            shares[chunk][which].wait_recv()
            theirs = arrived[index].reshape(512, cut[1]).astype(F32)
            rows_out[index] = (mine + theirs).astype(BF).reshape(2, 4, 4, SLOTS, cut[1])
            if chunk == 1:
                begin(backs[1 + which])

    gather_x(0)
    all_greeted()
    start_all(loads)
    begin(xs[0])
    gather_g(0)
    begin(gs[0])
    gather_x(1)
    begin(xs[1])
    gather_g(1)
    pad_left[pl.ds(8, 256), :] = conv_gate_ref[...].astype(F32) * conv_value_ref[...].astype(F32)
    left = remote(
        pad_left.at[pl.ds(256, 8)],
        halo.at[0],
        halo_send.at[0],
        halo_recv.at[0],
        ((sp + 1) % 64, tp),
    )
    left.start()
    advance(xs[0], 1)
    advance(gs[0], 1)
    begin(gs[1])
    left.wait()
    pad_left[pl.ds(0, 8), :] = jnp.where(sp == 0, 0.0, halo[0])
    conv_sum = jnp.zeros((256, 512), F32)
    for tap in range(3):
        conv_sum = conv_sum + taps_ref[tap : tap + 1, :] * pad_left[pl.ds(6 + tap, 256), :]
    conv_sum_ref[...] = conv_sum
    mixer_out[...] = (gate_in_ref[...].astype(F32) * conv_sum).astype(BF)
    advance(xs[0], 2)
    advance(gs[0], 2)
    advance(xs[1], 1)
    advance(gs[1], 1)
    cross(0, 0)
    for load in loads:
        load.wait()
    crossed(0, 0)
    cross(1, 0)
    advance(xs[1], 2)
    activate(0)
    crossed(1, 0)
    advance(gs[1], 2)
    differentiate(0)
    for stream in (*xs, *gs):
        for portion in stream:
            sent_phase(portion[0])
    share_theirs(0)
    add_mine(0)
    begin(backs[0])
    cross(0, 1)
    crossed(0, 1)
    cross(1, 1)
    activate(1)
    crossed(1, 1)
    differentiate(1)
    advance(backs[0], 1)
    share_theirs(1)
    add_mine(1)
    advance(backs[0], 2)
    weight_tile(0)
    advance(backs[1], 1)
    weight_tile(1)
    advance(backs[2], 1)
    weight_tile(2)
    weight_tile(3)
    advance(backs[1], 2)
    for portion in backs[0]:
        arrive_phase(portion[2])
    added_ref[...] = dot_tn(
        hot_ref[pl.ds(0, 512), :], back[2, pl.ds(0, 2)].reshape(512, 1024)
    ) + cot_ref[...].astype(F32)
    advance(backs[2], 2)
    weight_tile(4)
    swaps = []

    def combine(which):
        for portion in backs[1 + which]:
            arrive_phase(portion[2])
        columns = pl.ds(*HALVES[which])
        rows = back[2, pl.ds(2, 2), :, :, :, columns].reshape(512, 512)
        total = added_ref[:, columns] + dot_tn(hot_ref[pl.ds(512, 512), :], rows)
        whole[tp, :, columns] = total.astype(BF)
        swap = remote(
            whole.at[tp, :, columns],
            whole.at[tp, :, columns],
            tp_send.at[8 + which],
            tp_recv.at[8 + which],
            partner,
        )
        swap.start()
        swaps.append(swap)

    combine(0)
    combine(1)

    def block_of(half):
        for part in range(2):
            product = dot_tn(whole[half, :, pl.ds(part * 512, 512)], mixer_out[...])
            for tile in range(4):
                blocks[half * 2 + part, :, :, pl.ds(tile * 2, 2)] = (
                    product[:, tile * 128 : (tile + 1) * 128].astype(BF).reshape(4, 4, 2, 16, 128)
                )

    def fold_copies(which, phase, half=None, late=0):
        start, count = UNIT_CUTS[which]
        dim = ORDERS[which][phase]
        here = coordinate(dim)
        left_dims = sorted(ORDERS[which][phase:])
        copies = []
        for by in (2, 1, 3):
            index = [slice(None)] * len(left_dims)
            index[left_dims.index(dim)] = (here + by) % SIDE
            kept = slice(None)
            if half is not None:
                kept = pl.ds(2 * half, 2)
                index[0] = kept
            units = pl.ds(start, count)
            if phase == 0:
                source = blocks.at[(*index, units)]
                target = got1.at[by - 1, kept, :, units]
            elif phase == 1:
                source = sum1.at[(*index, units)]
                target = got2.at[by - 1, :, units]
            else:
                source = sum2.at[(*index, units)]
                target = got3.at[by - 1, units]
            copies.append(
                remote(
                    source,
                    target,
                    fold_send.at[which, phase + 3 * late],
                    fold_recv.at[which, phase + 3 * late],
                    (peer_of(dim, by), tp),
                )
            )
        index = [slice(None)] * len(left_dims)
        index[left_dims.index(dim)] = pl.ds(0, 3)
        kept = slice(None)
        if half is not None:
            kept = pl.ds(2 * half, 2)
            index[0] = kept
        if phase == 0:
            source, target = blocks.at[(*index, units)], got1.at[:, kept, :, units]
        elif phase == 1:
            source, target = sum1.at[(*index, units)], got2.at[:, :, units]
        else:
            source, target = sum2.at[(*index, units)], got3.at[:, units]
        ended = (
            pltpu.make_async_copy(target, target, fold_recv.at[which, phase + 3 * late]),
            pltpu.make_async_copy(source, source, fold_send.at[which, phase + 3 * late]),
        )
        return copies, ended

    def folded(which, phase):
        start, count = UNIT_CUTS[which]
        units = pl.ds(start, count)
        dim = ORDERS[which][phase]
        left_dims = sorted(ORDERS[which][phase:])
        index = [slice(None)] * len(left_dims)
        index[left_dims.index(dim)] = coordinate(dim)
        source = (blocks, sum1, sum2)[phase]
        total = source[(*index, units)].astype(F32)
        for by in range(3):
            if phase == 0:
                total = total + got1[by, :, :, units].astype(F32)
            elif phase == 1:
                total = total + got2[by, :, units].astype(F32)
            else:
                total = total + got3[by, units].astype(F32)
        return total

    folds = [[[], [], []] for which in range(3)]

    def fold_first(which, half, late):
        copies, ended = fold_copies(which, 0, half, late)
        start_all(copies)
        folds[which][0].append(ended)

    def fold_next(which, phase):
        copies, ended = fold_copies(which, phase)
        start_all(copies)
        folds[which][phase].append(ended)

    block_of(tp)
    fold_first(0, tp, 0)
    fold_first(1, tp, 0)
    for swap in swaps:
        swap.wait()
    block_of(1 - tp)
    fold_first(2, None, 0)
    fold_first(0, 1 - tp, 1)
    fold_first(1, 1 - tp, 1)
    results = []

    def deliver(source, target):
        copy = pltpu.make_async_copy(source, target, small_sems.at[len(results)])
        copy.start()
        results.append(copy)

    deliver(whole.at[tp], half_hbm)

    mixer_grad = (dot(whole[0], w_out[0:1024, :]) + dot(whole[1], w_out[1024:2048, :])).astype(BF)
    mixer_wide = mixer_grad.astype(F32)
    small[0] = (mixer_wide * conv_sum_ref[...]).astype(BF)
    pad_right[pl.ds(0, 256), :] = mixer_wide * gate_in_ref[...].astype(F32)
    right = remote(
        pad_right.at[pl.ds(0, 8)],
        halo.at[1],
        halo_send.at[1],
        halo_recv.at[1],
        ((sp + 63) % 64, tp),
    )
    right.start()
    deliver(small.at[0], gate_in_grad_hbm)
    weight_tile(5)
    for which, fold in enumerate(folds):
        start, count = UNIT_CUTS[which]
        for ended in fold[0]:
            ended[0].wait()
        sum1[:, :, pl.ds(start, count)] = folded(which, 0).astype(BF)
        fold_next(which, 1)
    right.wait()
    pad_right[pl.ds(256, 8), :] = jnp.where(sp == 63, 0.0, halo[1])
    prod_grad = jnp.zeros((256, 512), F32)
    for tap in range(3):
        prod_grad = prod_grad + taps_ref[tap : tap + 1, :] * pad_right[pl.ds(2 - tap, 256), :]
    small[1] = (prod_grad * conv_value_ref[...].astype(F32)).astype(BF)
    small[2] = (prod_grad * conv_gate_ref[...].astype(F32)).astype(BF)
    deliver(small.at[1], conv_gate_grad_hbm)
    deliver(small.at[2], conv_value_grad_hbm)
    for which, fold in enumerate(folds):
        start, count = UNIT_CUTS[which]
        for ended in fold[1]:
            ended[0].wait()
        sum2[:, pl.ds(start, count)] = folded(which, 1).astype(BF)
        fold_next(which, 2)
    for which, fold in enumerate(folds):
        start, count = UNIT_CUTS[which]
        for ended in fold[2]:
            ended[0].wait()
        total = folded(which, 2)
        for unit in range(count):
            tile, row = divmod(start + unit, 2)
            out_block_ref[pl.ds(row * 16, 16), pl.ds(tile * 128, 128)] = total[unit]
    deliver(out_block_ref, out_block_hbm)
    for chunk in range(2):
        for share in shares[chunk]:
            share.wait_send()
        for stream in (xs[chunk], gs[chunk]):
            for portion in stream:
                for copies in portion[1:]:
                    sent_phase(copies)
    for stream in backs:
        for portion in stream:
            for copies in portion:
                sent_phase(copies)
    for fold in folds:
        for phase in fold:
            for ended in phase:
                ended[1].wait()
    for copy in results:
        copy.wait()
    for copies in saves[4:]:
        for copy in copies:
            copy.wait()


def main_call(*operands):
    hbm = pl.BlockSpec(memory_space=pl.ANY)
    shape = jax.ShapeDtypeStruct
    rows_shape = (4, 4, 4, SLOTS, 1024)
    full_shape = (4, 4, 4, SLOTS, 2048)
    dma = pltpu.SemaphoreType.DMA
    return pl.pallas_call(
        main_kernel,
        out_shape=(
            shape((256, 1024), BF),
            shape((256, 512), BF),
            shape((256, 512), BF),
            shape((256, 512), BF),
            shape((32, 512), F32),
            shape((2048, 512), BF),
            shape((2048, 512), BF),
            shape((512, 2048), BF),
        ),
        in_specs=[hbm] * 12,
        out_specs=(hbm,) * 8,
        scratch_shapes=[
            pltpu.VMEM((2, 256), jnp.int32),
            pltpu.VMEM((2, 256), F32),
            pltpu.VMEM((256, 1024), BF),
            pltpu.VMEM((256, 1024), BF),
            pltpu.VMEM((256, 512), BF),
            pltpu.VMEM((256, 512), BF),
            pltpu.VMEM((256, 512), BF),
            pltpu.VMEM((3, 512), F32),
            pltpu.VMEM((2, *rows_shape), BF),
            pltpu.VMEM((2, 2, *rows_shape), BF),
            pltpu.VMEM(full_shape, BF),
            pltpu.VMEM(full_shape, BF),
            pltpu.VMEM((2048, 1024), BF),
            pltpu.VMEM((512, 2048), BF),
            pltpu.VMEM((2048, 512), BF),
            pltpu.VMEM((1024, 512), F32),
            pltpu.VMEM((1024, 512), F32),
            pltpu.VMEM((1024, 512), BF),
            pltpu.VMEM((1024, 1024), BF),
            pltpu.VMEM(rows_shape, BF),
            pltpu.VMEM((2, 512, 1024), BF),
            pltpu.VMEM((3, *rows_shape), BF),
            pltpu.VMEM((256, 1024), F32),
            pltpu.VMEM((1024, 256), BF),
            pltpu.VMEM((2, 256, 1024), BF),
            pltpu.VMEM((4, 4, 4, 8, 16, 128), BF),
            pltpu.VMEM((3, 4, 4, 8, 16, 128), BF),
            pltpu.VMEM((4, 4, 8, 16, 128), BF),
            pltpu.VMEM((3, 4, 8, 16, 128), BF),
            pltpu.VMEM((4, 8, 16, 128), BF),
            pltpu.VMEM((3, 8, 16, 128), BF),
            pltpu.VMEM((264, 512), F32),
            pltpu.VMEM((264, 512), F32),
            pltpu.VMEM((2, 8, 512), F32),
            pltpu.VMEM((256, 512), F32),
            pltpu.VMEM((256, 512), BF),
            pltpu.VMEM((3, 256, 512), BF),
            pltpu.VMEM((32, 512), F32),
            dma((8,)),
            dma((4,)),
            dma((6, 2)),
            dma((5,)),
            dma((21, 3)),
            dma((21, 3)),
            dma((10,)),
            dma((10,)),
            dma((2,)),
            dma((2,)),
            dma((3, 4)),
            dma((3, 4)),
        ],
        compiler_params=pltpu.CompilerParams(
            collective_id=0, has_side_effects=True, vmem_limit_bytes=67043328
        ),
    )(*operands)


def finish_kernel(*refs):
    sources, targets = refs[:8], refs[8:16]
    passing, held, narrow, wide, in_sems, out_sems, big_in, big_out = (
        refs[16:20],
        refs[20],
        refs[21:24],
        refs[24:27],
        *refs[27:31],
    )
    passing = (*passing, held)

    def rows_of(which, step):
        rows = narrow[which].shape[1]
        return pl.ds(pl.multiple_of(step * rows, rows), rows)

    def taken(which, step):
        return pltpu.make_async_copy(
            sources[5 + which].at[rows_of(which, step)],
            narrow[which].at[step],
            big_in.at[which, step],
        )

    def given(which, step):
        return pltpu.make_async_copy(
            wide[which].at[step],
            targets[5 + which].at[0, rows_of(which, step)],
            big_out.at[which, step],
        )

    ins = [
        pltpu.make_async_copy(sources[k], passing[k], in_sems.at[k]) for k in range(5)
    ]
    outs = [
        pltpu.make_async_copy(passing[k], targets[k], out_sems.at[k]) for k in range(5)
    ]
    for step in range(2):
        for which in range(3):
            taken(which, step).start()
    start_all(ins)

    def widen(step, carry):
        for which in range(3):
            taken(which, step).wait()
            wide[which][step] = narrow[which][step].astype(F32)
            given(which, step).start()
        return carry

    lax.fori_loop(0, 2, widen, 0)
    for k in range(5):
        ins[k].wait()
        outs[k].start()
    for step in range(2):
        for which in range(3):
            given(which, step).wait()
    for copy in outs:
        copy.wait()


def finished(produced):
    hbm = pl.BlockSpec(memory_space=pl.ANY)
    dma = pltpu.SemaphoreType.DMA
    shape = jax.ShapeDtypeStruct
    tiles = ((2, 1024, 512), (2, 1024, 512), (2, 256, 2048))
    return pl.pallas_call(
        finish_kernel,
        out_shape=tuple(shape(array.shape, array.dtype) for array in produced[:5])
        + tuple(shape((1, *array.shape), F32) for array in produced[5:]),
        in_specs=[hbm] * 8,
        out_specs=(hbm,) * 8,
        scratch_shapes=[pltpu.VMEM(array.shape, array.dtype) for array in produced[:5]]
        + [pltpu.VMEM(tile, BF) for tile in tiles]
        + [pltpu.VMEM(tile, F32) for tile in tiles]
        + [dma((5,)), dma((5,)), dma((3, 4)), dma((3, 4))],
        compiler_params=pltpu.CompilerParams(vmem_limit_bytes=67043328),
    )(*produced)


def shards(
    stream,
    out_grad,
    gate_in,
    conv_gate,
    conv_value,
    taps,
    w_out,
    route_ids,
    route_weights,
    w_gate,
    w_up,
    w_down,
):
    produced = main_call(
        route_ids.T,
        route_weights.T,
        stream,
        out_grad,
        gate_in,
        conv_gate,
        conv_value,
        taps,
        w_out,
        w_gate,
        w_up,
        w_down,
    )
    return finished(produced)


def solution(mesh):
    placed = (
        P("sp", "tp"),
        P("sp", "tp"),
        P("sp", "tp"),
        P("sp", "tp"),
        P("sp", "tp"),
        P(None, "tp"),
        P(None, "tp"),
        P("sp", None),
        P("sp", None),
        P("sp", None, "tp"),
        P("sp", None, "tp"),
        P("sp", "tp", None),
    )
    return jax.shard_map(
        shards,
        mesh=mesh,
        in_specs=placed,
        out_specs=(
            P("sp", "tp"),
            P("sp", "tp"),
            P("sp", "tp"),
            P("sp", "tp"),
            P("sp", "tp"),
            P("sp", None, "tp"),
            P("sp", None, "tp"),
            P("sp", "tp", None),
        ),
        check_vma=False,
    )
```
